128 devices in a mesh: dp: 4 (over x), kv: 16 (over z, y), tp: 2 (over core).
Axes of the slice: x: 4, y: 4, z: 4, core: 2. Of those that a mesh axis runs over, the one named last changes fastest.
Arguments:
- tokens: bfloat16 [1024, 4096], P('dp', 'kv'), may hold values from -24 to 24
- state: float32 [1024, 64, 64, 64], P(('dp', 'kv'), 'tp'), may hold values from -4 to 4
- w_query: bfloat16 [4096, 4096], P('kv', 'tp'), may hold values from -0.09375 to 0.09375
- w_forget: bfloat16 [4096, 4096], P('kv', 'tp'), may hold values from -0.09375 to 0.09375
- w_input: bfloat16 [4096, 4096], P('kv', 'tp'), may hold values from -0.09375 to 0.09375
- w_gate: bfloat16 [4096, 4096], P('kv', 'tp'), may hold values from -0.09375 to 0.09375
- lower_bound: float32 [4096], P('tp'), may hold values from 0 to 0.9
- head_gain: float32 [64], replicated, may hold values from 0.1 to 1.9
- w_out: bfloat16 [4096, 4096], P('tp', 'kv'), may hold values from -0.09375 to 0.09375
- gain_one: float32 [4096], P(('kv', 'tp')), may hold values from 0.1 to 1.9
- bias_one: float32 [4096], P(('kv', 'tp')), may hold values from -2 to 2
- w_up: bfloat16 [4096, 16384], P(None, ('kv', 'tp')), may hold values from -0.09375 to 0.09375
- w_down: bfloat16 [16384, 4096], P(('kv', 'tp')), may hold values from -0.09375 to 0.09375
- gain_two: float32 [4096], P(('kv', 'tp')), may hold values from 0.1 to 1.9
- bias_two: float32 [4096], P(('kv', 'tp')), may hold values from -2 to 2
Outputs:
- result: bfloat16 [1024, 4096], P('dp', ('kv', 'tp'))
- new_state: float32 [1024, 64, 64, 64], P(('dp', 'kv'), 'tp')
The draws below stay inside these ranges and needn't reach their ends.
All inputs are finite; a program needn't handle non-finite values.
Results may differ from the reference program's by a relative error of at most 0.014.
Values may be sent and summed in bfloat16 or wider, within the bound.
No kernel may reach another device: no remote copies, remote signals or barrier semaphores. Data moves between devices by JAX's collectives and lax.ppermute only.
A program may use at most 128 MiB of HBM per device.

```python
import math
import jax
import jax.numpy as jnp
from jax import lax

D = 4096
HEADS = 64
DK = 64
FF = 16384
HW = 4096
BATCH = 1024


def draw_tokens(key, part):
    key_base = jax.random.fold_in(key, 11)
    key_scale = jax.random.fold_in(key, 12)
    base = jnp.clip(jax.random.normal(key_base, (BATCH, D), jnp.float32), -8.0, 8.0)
    scales = jnp.exp(jax.random.uniform(key_scale, (16,), jnp.float32, math.log(0.3), math.log(3.0)))
    column_scale = jnp.repeat(scales, D // 16)
    return (base * column_scale[None, :]).astype(jnp.bfloat16)


def spiked(drawn, key, source, target, parts, factor):
    def block_of(dim):
        return (jnp.arange(drawn.shape[dim]) // (drawn.shape[dim] // parts)).reshape((-1,) + (1,) * (drawn.ndim - 1 - dim))

    one_side = jax.random.permutation(key, parts)[block_of(target)]
    far = (block_of(target) + parts // 2) % parts
    return jnp.where((block_of(source) == one_side) | (block_of(source) == far), factor * drawn, drawn)


def shard_levels(rng, shape, shards, smallest, high):
    def one(axis_at, shards_of):
        draws = jax.random.uniform(jax.random.fold_in(jax.random.fold_in(rng, 6), axis_at), (shards_of,), jnp.float32, smallest / len(shards), high / len(shards))
        return jnp.repeat(jnp.exp(draws), shape[axis_at] // shards_of).reshape((-1,) + (1,) * (len(shape) - axis_at - 1))

    loudness = one(*shards[0])
    for cut in shards[1:]:
        loudness = loudness * one(*cut)
    return loudness


def bell_draw(key, dims, scale, most, shards=(), held_as=jnp.bfloat16):
    entries = scale * jax.random.normal(key, dims, jnp.float32)
    if shards:
        entries = entries * shard_levels(key, dims, shards, -0.22, 0.18)
    return jnp.clip(entries, -most, most).astype(held_as)


def heavy_noise(rng, extent, deviation, reach, shards, heavy, kind=jnp.bfloat16):
    values = deviation * jax.random.normal(rng, extent, jnp.float32)
    if shards:
        values = values * shard_levels(rng, extent, shards, -0.22, 0.18)
    return jnp.clip(spiked(values, jax.random.fold_in(rng, 3), *heavy), -reach, reach).astype(kind)


def setup_inputs(seed: int = 0) -> dict:
    splits = jax.random.split(jax.random.key(seed), 16)
    return {
        "tokens": draw_tokens(jax.random.fold_in(splits[15], 71), 0),
        "state": bell_draw(splits[1], (BATCH, HEADS, DK, DK), 0.3, 4.0, ((0, 64), (1, 2)), jnp.float32),
        "w_query": bell_draw(splits[2], (D, HW), D ** -0.5, 0.09375, ((0, 16), (1, 2))),
        "w_forget": bell_draw(splits[3], (D, HW), D ** -0.5, 0.09375, ((0, 16), (1, 2))),
        "w_input": bell_draw(splits[4], (D, HW), D ** -0.5, 0.09375, ((0, 16), (1, 2))),
        "w_gate": bell_draw(splits[5], (D, HW), D ** -0.5, 0.09375, ((0, 16), (1, 2))),
        "lower_bound": jnp.clip(0.9 * jax.random.uniform(splits[6], (HW,), jnp.float32) ** shard_levels(splits[6], (HW,), ((0, 2),), -0.2, 0.2), 0.0, 0.9),
        "head_gain": jnp.clip(1.0 + 0.18 * jax.random.normal(splits[7], (DK,), jnp.float32), 0.1, 1.9),
        "w_out": bell_draw(splits[8], (HW, D), HW ** -0.5, 0.09375, ((0, 2), (1, 16))),
        "gain_one": jnp.clip(1.0 + 0.18 * jax.random.normal(splits[9], (D,), jnp.float32), 0.1, 1.9),
        "bias_one": bell_draw(splits[10], (D,), 0.3, 2.0, ((0, 32),), jnp.float32),
        "w_up": bell_draw(splits[11], (D, FF), D ** -0.5, 0.09375, ((1, 32),)),
        "w_down": heavy_noise(splits[12], (FF, D), FF ** -0.5, 0.09375, ((0, 32),), (0, 1, 32, 2.75)),
        "gain_two": jnp.clip(1.0 + 0.18 * jax.random.normal(splits[13], (D,), jnp.float32), 0.1, 1.9),
        "bias_two": bell_draw(splits[14], (D,), 0.3, 2.0, ((0, 32),), jnp.float32),
    }


epsilon = 0.1
residual_scale = 1.68

def layer_norm(values, gain, bias):
    center = lax.optimization_barrier(jnp.mean(values, axis=-1, keepdims=True))
    spread = lax.optimization_barrier(jnp.mean(jnp.square(values - center), axis=-1, keepdims=True))
    return (values - center) * lax.rsqrt(spread + epsilon) * gain + bias

def project(tokens, weight):
    rounded = jnp.dot(tokens, weight, preferred_element_type=jnp.float32).astype(jnp.bfloat16)
    rounded = lax.optimization_barrier(rounded)
    return rounded.astype(jnp.float32)

def reference(tokens, state, w_query, w_forget, w_input, w_gate, lower_bound, head_gain, w_out, gain_one, bias_one, w_up, w_down, gain_two, bias_two):
    batch = tokens.shape[0]
    shape = (batch, HEADS, DK)
    query_raw = project(tokens, w_query).reshape(shape)
    forget_raw = project(tokens, w_forget).reshape(shape)
    value_raw = project(tokens, w_input).reshape(shape)
    gate_raw = project(tokens, w_gate).reshape(shape)
    bound = lower_bound.reshape(HEADS, DK)
    forget = bound + (1.0 - bound) * jax.nn.sigmoid(forget_raw)
    keyvec = (1.0 - bound) * jax.nn.sigmoid(-forget_raw)
    query = jax.nn.silu(query_raw)
    new_state = forget[..., None] * state + keyvec[..., None] * value_raw[:, :, None, :]
    read = jnp.einsum('bhij,bhi->bhj', new_state, query, precision=lax.Precision.HIGHEST)
    read = read * lax.rsqrt(lax.optimization_barrier(jnp.mean(jnp.square(read), axis=-1, keepdims=True)) + epsilon)
    mixout = (read * head_gain * jax.nn.silu(gate_raw)).reshape(batch, HEADS * DK).astype(jnp.bfloat16)
    mixed = jnp.dot(mixout, w_out, preferred_element_type=jnp.float32)
    first = residual_scale * tokens.astype(jnp.float32) + mixed
    normed = layer_norm(first, gain_one, bias_one).astype(jnp.bfloat16)
    upper = jnp.dot(normed, w_up, preferred_element_type=jnp.float32)
    hidden = jnp.square(jax.nn.relu(upper)).astype(jnp.bfloat16)
    mlp = jnp.dot(hidden, w_down, preferred_element_type=jnp.float32)
    second = residual_scale * normed.astype(jnp.float32) + mlp
    result = layer_norm(second, gain_two, bias_two).astype(jnp.bfloat16)
    return (result, new_state)
```

```python
import jax
import jax.numpy as jnp
from jax import lax
from jax.sharding import Mesh
from jax.sharding import PartitionSpec as P

D = 4096
epsilon = 0.1
residual_scale = 1.68
f32 = jnp.float32
bf16 = jnp.bfloat16


def dot(a, b):
    return jnp.dot(a, b, preferred_element_type=f32)


def flipped(value, axis, bits):
    return lax.ppermute(value, axis, [(i, i ^ bits) for i in range(lax.axis_size(axis))])


def exchanged(tiles, axis):
    return lax.all_to_all(tiles, axis, split_axis=0, concat_axis=0, tiled=True)


def of_all(value, axis):
    return exchanged(jnp.broadcast_to(value, (lax.axis_size(axis), *value.shape)), axis)


def relative(flip):
    return (0, 4 - flip, flip, 2)


def row_order(rows, outer, outer_flip, inner, inner_flip, outer_stride, inner_stride):
    own = rows // 16
    p = lax.broadcasted_iota(jnp.int32, (rows, rows), 0)
    c = lax.broadcasted_iota(jnp.int32, (rows, rows), 1)
    block = p // own

    def flip_of(i, flip):
        r = relative(flip)
        return jnp.where(i == 0, r[0], jnp.where(i == 1, r[1], jnp.where(i == 2, r[2], r[3])))

    o = jnp.bitwise_xor(outer, flip_of(block // 4, outer_flip))
    i = jnp.bitwise_xor(inner, flip_of(block % 4, inner_flip))
    source = (o * outer_stride + i * inner_stride) * own + p % own
    return (c == source).astype(bf16)


def halved(kept, received):
    return kept + received.astype(f32)


def scattered_sum(tokens, weight, first, flip_first, second, flip_second):
    rows = tokens.shape[0]
    sent = dot(tokens[rows // 2 :], weight).astype(bf16)
    arrived = flipped(sent, first, flip_first)
    total = halved(dot(tokens[: rows // 2], weight), arrived)
    for axis, flip in ((first, 4 - flip_first), (second, flip_second), (second, 4 - flip_second)):
        rows = total.shape[0]
        arrived = flipped(total[rows // 2 :].astype(bf16), axis, flip)
        total = halved(total[: rows // 2], arrived)
    return total


def packed_total(arrays, axis):
    line = jnp.stack(arrays)
    got = of_all(line[None], axis).sum(axis=0)[0]
    return got[0], got[1]


def finish_norm(values, total, squares, width, gain, bias):
    center = total[:, None] / width
    spread = squares[:, None] / width - center * center
    return (values - center) * lax.rsqrt(spread + epsilon) * gain + bias


def per_device(
    tokens,
    state,
    w_query,
    w_forget,
    w_input,
    w_gate,
    lower_bound,
    head_gain,
    w_out,
    gain_one,
    bias_one,
    w_up,
    w_down,
    gain_two,
    bias_two,
):
    z, y, t = lax.axis_index("z"), lax.axis_index("y"), lax.axis_index("tp")
    rows = tokens.shape[0]
    rows_own = rows // 16
    width = w_query.shape[1]
    key_size = head_gain.shape[0]
    heads_here = width // key_size

    streams = []
    for weight, z_first, flip in (
        (w_query, True, 1),
        (w_forget, True, 3),
        (w_input, False, 1),
        (w_gate, False, 3),
    ):
        if z_first:
            order = row_order(rows, z, flip, y, flip, 4, 1)
            axes = ("z", flip, "y", flip)
        else:
            order = row_order(rows, y, flip, z, flip, 1, 4)
            axes = ("y", flip, "z", flip)
        streams.append(scattered_sum(dot(order, tokens).astype(bf16), weight, *axes))
    shape = (rows_own, heads_here, key_size)
    query_raw, forget_raw, value_raw, gate_raw = (
        s.astype(bf16).astype(f32).reshape(shape) for s in streams
    )
    bound = lower_bound.reshape(heads_here, key_size)
    forget = bound + (1.0 - bound) * jax.nn.sigmoid(forget_raw)
    keyvec = (1.0 - bound) * jax.nn.sigmoid(-forget_raw)
    query = jax.nn.silu(query_raw)
    new_state = forget[..., None] * state + keyvec[..., None] * value_raw[:, :, None, :]
    read = jnp.einsum("bhij,bhi->bhj", new_state, query, precision=lax.Precision.HIGHEST)
    read = read * lax.rsqrt(jnp.mean(jnp.square(read), axis=-1, keepdims=True) + epsilon)
    mixout = (read * head_gain * jax.nn.silu(gate_raw)).reshape(rows_own, width).astype(bf16)

    mixout = of_all(of_all(mixout[None], "y").reshape(1, 4 * rows_own, width), "z").reshape(rows, width)
    columns = w_out.shape[1] // 2
    w_out = w_out.reshape(width, 2, columns)
    theirs = dot(mixout, lax.dynamic_index_in_dim(w_out, 1 - t, 1, False))
    arrived = flipped(theirs, "tp", 1)
    mixed = dot(mixout, lax.dynamic_index_in_dim(w_out, t, 1, False)) + arrived
    own_tokens = lax.dynamic_slice_in_dim(tokens, t * columns, columns, 1)
    first = residual_scale * own_tokens.astype(f32) + mixed
    total, squares = packed_total(
        (jnp.sum(first, axis=1), jnp.sum(first * first, axis=1)), ("z", "y", "tp")
    )
    normed_own = finish_norm(first, total, squares, D, gain_one, bias_one).astype(bf16)

    half = D // 2
    hidden_width = w_up.shape[1]
    w_up = w_up.reshape(16, 2, columns, hidden_width)
    w_up_ours = lax.dynamic_index_in_dim(w_up, t, 1, False).reshape(half, hidden_width)
    w_up_theirs = lax.dynamic_index_in_dim(w_up, 1 - t, 1, False).reshape(half, hidden_width)
    w_down = w_down.reshape(hidden_width, 16, 2, columns)
    w_down_ours = lax.dynamic_index_in_dim(w_down, t, 2, False).reshape(hidden_width, half)
    w_down_theirs = lax.dynamic_index_in_dim(w_down, 1 - t, 2, False).reshape(hidden_width, half)

    gathered = of_all(of_all(normed_own[None], "y").reshape(1, 4, rows, columns), "z")
    ours = jnp.moveaxis(gathered.reshape(16, rows, columns), 0, 1).reshape(rows, half)
    other = flipped(ours, "tp", 1)
    upper = dot(ours, w_up_ours) + dot(other, w_up_theirs)
    hidden = jnp.square(jax.nn.relu(upper)).astype(bf16)
    arrived = flipped(dot(hidden, w_down_theirs).astype(bf16), "tp", 1)
    mlp = halved(dot(hidden, w_down_ours), arrived).astype(bf16)
    tiles = jnp.moveaxis(mlp.reshape(rows, 4, 4 * columns), 1, 0)
    mlp = exchanged(tiles, "z").astype(f32).sum(axis=0).astype(bf16)
    tiles = jnp.moveaxis(mlp.reshape(rows, 4, columns), 1, 0)
    mlp = exchanged(tiles, "y").astype(f32).sum(axis=0)
    second = residual_scale * normed_own.astype(f32) + mlp
    total, squares = packed_total(
        (jnp.sum(second, axis=1), jnp.sum(second * second, axis=1)), ("z", "y", "tp")
    )
    result = finish_norm(second, total, squares, D, gain_two, bias_two).astype(bf16)
    return (result, new_state)


def solution(mesh):
    fine = Mesh(mesh.devices.reshape(4, 4, 4, 2), ("dp", "z", "y", "tp"))
    kv = ("z", "y")
    every = ("z", "y", "tp")
    placed = (
        P("dp", kv),
        P(("dp", "z", "y"), "tp", None, None),
        P(kv, "tp"),
        P(kv, "tp"),
        P(kv, "tp"),
        P(kv, "tp"),
        P("tp"),
        P(),
        P("tp", kv),
        P(every),
        P(every),
        P(None, every),
        P(every, None),
        P(every),
        P(every),
    )
    return jax.shard_map(
        per_device,
        mesh=fine,
        in_specs=placed,
        out_specs=(P("dp", every), P(("dp", "z", "y"), "tp", None, None)),
        check_vma=False,
    )
```

```python
import jax
import jax.numpy as jnp
from jax import lax
from jax.experimental import pallas as pl
from jax.experimental.pallas import tpu as pltpu
from jax.sharding import Mesh
from jax.sharding import PartitionSpec as P

D = 4096
epsilon = 0.1
residual_scale = 1.68
f32 = jnp.float32
bf16 = jnp.bfloat16


def dot(a, b):
    return jnp.dot(a, b, preferred_element_type=f32)


def flipped(value, axis, bits):
    return lax.ppermute(value, axis, [(i, i ^ bits) for i in range(lax.axis_size(axis))])


def exchanged(tiles, axis):
    return lax.all_to_all(tiles, axis, split_axis=0, concat_axis=0, tiled=True)


def of_all(value, axis):
    return exchanged(jnp.broadcast_to(value, (lax.axis_size(axis), *value.shape)), axis)


def relative(flip):
    return (0, 4 - flip, flip, 2)


def row_order(rows, outer, outer_flip, inner, inner_flip, outer_stride, inner_stride):
    own = rows // 16
    p = lax.broadcasted_iota(jnp.int32, (rows, rows), 0)
    c = lax.broadcasted_iota(jnp.int32, (rows, rows), 1)
    block = p // own

    def flip_of(i, flip):
        r = relative(flip)
        return jnp.where(i == 0, r[0], jnp.where(i == 1, r[1], jnp.where(i == 2, r[2], r[3])))

    o = jnp.bitwise_xor(outer, flip_of(block // 4, outer_flip))
    i = jnp.bitwise_xor(inner, flip_of(block % 4, inner_flip))
    source = (o * outer_stride + i * inner_stride) * own + p % own
    return (c == source).astype(bf16)


def halved(kept, received):
    return kept + received.astype(f32)


def scattered_sum(tokens, weight, first, flip_first, second, flip_second):
    rows = tokens.shape[0]
    sent = dot(tokens[rows // 2 :], weight).astype(bf16)
    arrived = flipped(sent, first, flip_first)
    total = halved(dot(tokens[: rows // 2], weight), arrived)
    for axis, flip in ((first, 4 - flip_first), (second, flip_second), (second, 4 - flip_second)):
        rows = total.shape[0]
        arrived = flipped(total[rows // 2 :].astype(bf16), axis, flip)
        total = halved(total[: rows // 2], arrived)
    return total


def packed_total(arrays, axis):
    line = jnp.stack(arrays)
    got = of_all(line[None], axis).sum(axis=0)[0]
    return got[0], got[1]


def finish_norm(values, total, squares, width, gain, bias):
    center = total[:, None] / width
    spread = squares[:, None] / width - center * center
    return (values - center) * lax.rsqrt(spread + epsilon) * gain + bias


def rounded(ref):
    return ref[...].astype(bf16).astype(f32)


def gates(forget_raw, bound):
    rest = 1.0 - bound
    return bound + rest * jax.nn.sigmoid(forget_raw), rest * jax.nn.sigmoid(-forget_raw)


def read_kernel(q_ref, f_ref, v_ref, g_ref, bound_ref, gain_ref, state_ref, mix_ref, columns, reads):
    rows, heads, size = state_ref.shape[:3]
    wide = 2 * size
    query = rounded(q_ref)
    query = query * jax.nn.sigmoid(query)
    forget, keyvec = gates(rounded(f_ref), bound_ref[...])
    value = rounded(v_ref)
    gate = rounded(g_ref)
    scaled = forget * query
    for pair in range(heads // 2):
        columns[pair] = jnp.transpose(scaled[:, pair * wide : (pair + 1) * wide])

    def body(pair, carry):
        for b in range(rows):
            for half in range(2):
                column = columns[pair, half * size : (half + 1) * size, b : b + 1]
                product = state_ref[b, 2 * pair + half] * column
                reads[2 * pair + half, b : b + 1, :] = jnp.sum(product, axis=0, keepdims=True)
        return carry

    lax.fori_loop(0, heads // 2, body, 0)
    agreement = keyvec * query
    gate = gate * jax.nn.sigmoid(gate)
    for pair in range(heads // 2):
        done = []
        for head in (2 * pair, 2 * pair + 1):
            own = slice(head * size, (head + 1) * size)
            read = reads[head] + jnp.sum(agreement[:, own], axis=1, keepdims=True) * value[:, own]
            power = jnp.mean(read * read, axis=1, keepdims=True)
            done.append(read * lax.rsqrt(power + epsilon) * gain_ref[...] * gate[:, own])
        mix_ref[:, pair * wide : (pair + 1) * wide] = jnp.concatenate(done, axis=1).astype(bf16)


def state_kernel(f_ref, v_ref, bound_ref, state_ref, out_ref, forgets, keys, values, ready, sems):
    rows, heads, size = state_ref.shape[:3]
    wide = 2 * size
    forget, keyvec = gates(rounded(f_ref), bound_ref[...])
    value = rounded(v_ref)
    for pair in range(heads // 2):
        own = slice(pair * wide, (pair + 1) * wide)
        forgets[pair] = jnp.transpose(forget[:, own])
        keys[pair] = jnp.transpose(keyvec[:, own])
    for head in range(heads):
        values[head] = value[:, head * size : (head + 1) * size]

    def copied(pair):
        slot = pair % 2
        return pltpu.make_async_copy(ready.at[slot], out_ref.at[:, pl.ds(2 * pair, 2)], sems.at[slot])

    def body(pair, carry):
        @pl.when(pair >= 2)
        def _():
            copied(pair - 2).wait()

        slot = pair % 2
        for b in range(rows):
            for half in range(2):
                own = slice(half * size, (half + 1) * size)
                kept = forgets[pair, own, b : b + 1] * state_ref[b, 2 * pair + half]
                added = keys[pair, own, b : b + 1] * values[2 * pair + half, b : b + 1, :]
                ready[slot, b, half] = kept + added
        copied(pair).start()
        return carry

    pairs = heads // 2
    lax.fori_loop(0, pairs, body, 0)
    copied(pairs - 2).wait()
    copied(pairs - 1).wait()


def mlp_kernel(t_ref, ours_ref, other_ref, up_ref, down_ref, theirs_ref, mine_ref, joined):
    t = t_ref[0]
    blocks, _, size = ours_ref.shape
    for k in range(blocks):
        joined[:, pl.ds(pl.multiple_of((2 * k + t) * size, size), size)] = ours_ref[k]
        joined[:, pl.ds(pl.multiple_of((2 * k + 1 - t) * size, size), size)] = other_ref[k]
    upper = dot(joined[...], up_ref[...])
    hidden = jnp.square(jnp.maximum(upper, 0.0)).astype(bf16)
    for k in range(blocks):
        both = dot(hidden, down_ref[:, 2 * k * size : 2 * (k + 1) * size])
        left, right = both[:, :size], both[:, size:]
        at = slice((k % 4) * size, (k % 4 + 1) * size)
        theirs_ref[k // 4, :, at] = jnp.where(t == 0, right, left).astype(bf16)
        mine_ref[k // 4, :, at] = jnp.where(t == 0, left, right)


def in_vmem(n):
    return [pl.BlockSpec(memory_space=pltpu.VMEM)] * n


def mixed_heads(query, forget, value, gate, bound, head_gain, state):
    rows, heads, size = state.shape[:3]
    return pl.pallas_call(
        read_kernel,
        out_shape=jax.ShapeDtypeStruct((rows, heads * size), bf16),
        in_specs=in_vmem(7),
        out_specs=in_vmem(1)[0],
        scratch_shapes=[
            pltpu.VMEM((heads // 2, 2 * size, rows), f32),
            pltpu.VMEM((heads, rows, size), f32),
        ],
        cost_estimate=pl.CostEstimate(flops=1 << 22, bytes_accessed=1 << 23, transcendentals=0),
        compiler_params=pltpu.CompilerParams(vmem_limit_bytes=8 << 20),
        name="heads_read",
    )(query, forget, value, gate, bound[None], head_gain[None], state)


def updated_state(forget, value, bound, state):
    rows, heads, size = state.shape[:3]
    return pl.pallas_call(
        state_kernel,
        out_shape=jax.ShapeDtypeStruct(state.shape, f32),
        in_specs=in_vmem(4),
        out_specs=pl.BlockSpec(memory_space=pltpu.HBM),
        scratch_shapes=[
            pltpu.VMEM((heads // 2, 2 * size, rows), f32),
            pltpu.VMEM((heads // 2, 2 * size, rows), f32),
            pltpu.VMEM((heads, rows, size), f32),
            pltpu.VMEM((2, rows, 2, size, size), f32),
            pltpu.SemaphoreType.DMA((2,)),
        ],
        cost_estimate=pl.CostEstimate(flops=1 << 27, bytes_accessed=1 << 25, transcendentals=0),
        compiler_params=pltpu.CompilerParams(vmem_limit_bytes=10 << 20),
        name="state_update",
    )(forget, value, bound[None], state)


def mixer(t, ours, other, w_up, w_down):
    blocks, rows, size = ours.shape
    shape = (4, rows, blocks // 4 * size)
    return pl.pallas_call(
        mlp_kernel,
        out_shape=(jax.ShapeDtypeStruct(shape, bf16), jax.ShapeDtypeStruct(shape, f32)),
        in_specs=[pl.BlockSpec(memory_space=pltpu.SMEM), *in_vmem(4)],
        out_specs=tuple(in_vmem(2)),
        scratch_shapes=[pltpu.VMEM((rows, 2 * blocks * size), bf16)],
        cost_estimate=pl.CostEstimate(flops=1 << 31, bytes_accessed=1 << 23, transcendentals=0),
        compiler_params=pltpu.CompilerParams(vmem_limit_bytes=18 << 20),
        name="channel_mixer",
    )(t.reshape(1), ours, other, w_up, w_down)


def per_device(
    tokens,
    state,
    w_query,
    w_forget,
    w_input,
    w_gate,
    lower_bound,
    head_gain,
    w_out,
    gain_one,
    bias_one,
    w_up,
    w_down,
    gain_two,
    bias_two,
):
    z, y, t = lax.axis_index("z"), lax.axis_index("y"), lax.axis_index("tp")
    rows = tokens.shape[0]
    rows_own = rows // 16
    width = w_query.shape[1]

    streams = []
    for weight, z_first, flip in (
        (w_query, True, 1),
        (w_forget, True, 3),
        (w_input, False, 1),
        (w_gate, False, 3),
    ):
        if z_first:
            order = row_order(rows, z, flip, y, flip, 4, 1)
            axes = ("z", flip, "y", flip)
        else:
            order = row_order(rows, y, flip, z, flip, 1, 4)
            axes = ("y", flip, "z", flip)
        streams.append(scattered_sum(dot(order, tokens).astype(bf16), weight, *axes))
    query_raw, forget_raw, value_raw, gate_raw = streams
    state = pltpu.with_memory_space_constraint(state, pltpu.VMEM)
    mixout = mixed_heads(query_raw, forget_raw, value_raw, gate_raw, lower_bound, head_gain, state)
    new_state = updated_state(forget_raw, value_raw, lower_bound, state)

    mixout = of_all(of_all(mixout[None], "y").reshape(1, 4 * rows_own, width), "z").reshape(rows, width)
    columns = w_out.shape[1] // 2
    w_out = w_out.reshape(width, 2, columns)
    theirs = dot(mixout, lax.dynamic_index_in_dim(w_out, 1 - t, 1, False))
    arrived = flipped(theirs, "tp", 1)
    mixed = dot(mixout, lax.dynamic_index_in_dim(w_out, t, 1, False)) + arrived
    own_tokens = lax.dynamic_slice_in_dim(tokens, t * columns, columns, 1)
    first = residual_scale * own_tokens.astype(f32) + mixed
    total, squares = packed_total(
        (jnp.sum(first, axis=1), jnp.sum(first * first, axis=1)), ("z", "y", "tp")
    )
    normed_own = finish_norm(first, total, squares, D, gain_one, bias_one).astype(bf16)

    gathered = of_all(of_all(normed_own[None], "y").reshape(1, 4, rows, columns), "z")
    ours = gathered.reshape(16, rows, columns)
    other = flipped(ours, "tp", 1)
    w_up = pltpu.with_memory_space_constraint(w_up, pltpu.VMEM)
    w_down = pltpu.with_memory_space_constraint(w_down, pltpu.VMEM)
    theirs, mine = mixer(t, ours, other, w_up, w_down)
    mlp = halved(mine, flipped(theirs, "tp", 1)).astype(bf16)
    mlp = exchanged(mlp, "z").astype(f32).sum(axis=0).astype(bf16)
    tiles = jnp.moveaxis(mlp.reshape(rows, 4, columns), 1, 0)
    mlp = exchanged(tiles, "y").astype(f32).sum(axis=0)
    second = residual_scale * normed_own.astype(f32) + mlp
    total, squares = packed_total(
        (jnp.sum(second, axis=1), jnp.sum(second * second, axis=1)), ("z", "y", "tp")
    )
    result = finish_norm(second, total, squares, D, gain_two, bias_two).astype(bf16)
    return (result, new_state)


def solution(mesh):
    fine = Mesh(mesh.devices.reshape(4, 4, 4, 2), ("dp", "z", "y", "tp"))
    kv = ("z", "y")
    every = ("z", "y", "tp")
    placed = (
        P("dp", kv),
        P(("dp", "z", "y"), "tp", None, None),
        P(kv, "tp"),
        P(kv, "tp"),
        P(kv, "tp"),
        P(kv, "tp"),
        P("tp"),
        P(),
        P("tp", kv),
        P(every),
        P(every),
        P(None, every),
        P(every, None),
        P(every),
        P(every),
    )
    return jax.shard_map(
        per_device,
        mesh=fine,
        in_specs=placed,
        out_specs=(P("dp", every), P(("dp", "z", "y"), "tp", None, None)),
        check_vma=False,
    )
```

```python
import jax
import jax.numpy as jnp
from jax import lax
from jax.experimental import pallas as pl
from jax.experimental.pallas import tpu as pltpu
from jax.sharding import Mesh
from jax.sharding import PartitionSpec as P

D = 4096
epsilon = 0.1
residual_scale = 1.68
f32 = jnp.float32
bf16 = jnp.bfloat16


def dot(a, b):
    return jnp.dot(a, b, preferred_element_type=f32)


def flipped(value, axis, bits):
    return lax.ppermute(value, axis, [(i, i ^ bits) for i in range(lax.axis_size(axis))])


def exchanged(tiles, axis):
    return lax.all_to_all(tiles, axis, split_axis=0, concat_axis=0, tiled=True)


def of_all(value, axis):
    return exchanged(jnp.broadcast_to(value, (lax.axis_size(axis), *value.shape)), axis)


def relative(flip):
    return (0, 4 - flip, flip, 2)


def row_order(rows, outer, outer_flip, inner, inner_flip, outer_stride, inner_stride):
    own = rows // 16
    p = lax.broadcasted_iota(jnp.int32, (rows, rows), 0)
    c = lax.broadcasted_iota(jnp.int32, (rows, rows), 1)
    block = p // own

    def flip_of(i, flip):
        r = relative(flip)
        return jnp.where(i == 0, r[0], jnp.where(i == 1, r[1], jnp.where(i == 2, r[2], r[3])))

    o = jnp.bitwise_xor(outer, flip_of(block // 4, outer_flip))
    i = jnp.bitwise_xor(inner, flip_of(block % 4, inner_flip))
    source = (o * outer_stride + i * inner_stride) * own + p % own
    return (c == source).astype(bf16)


def halved(kept, received):
    return kept + received.astype(f32)


def scattered_sum(tokens, weight, first, flip_first, second, flip_second):
    rows = tokens.shape[0]
    sent = dot(tokens[rows // 2 :], weight).astype(bf16)
    arrived = flipped(sent, first, flip_first)
    total = halved(dot(tokens[: rows // 2], weight), arrived)
    for axis, flip in ((first, 4 - flip_first), (second, flip_second), (second, 4 - flip_second)):
        rows = total.shape[0]
        arrived = flipped(total[rows // 2 :].astype(bf16), axis, flip)
        total = halved(total[: rows // 2], arrived)
    return total


def packed_total(arrays, axis):
    line = jnp.stack(arrays)
    got = of_all(line[None], axis).sum(axis=0)[0]
    return got[0], got[1]


def finish_norm(values, total, squares, width, gain, bias):
    center = total[:, None] / width
    spread = squares[:, None] / width - center * center
    return (values - center) * lax.rsqrt(spread + epsilon) * gain + bias


def rounded(ref):
    return ref[...].astype(bf16).astype(f32)


def gates(forget_raw, bound):
    rest = 1.0 - bound
    return bound + rest * jax.nn.sigmoid(forget_raw), rest * jax.nn.sigmoid(-forget_raw)


def pieces(value):
    high = value.astype(bf16)
    rest = value - high.astype(f32)
    middle = rest.astype(bf16)
    return high, middle, (rest - middle.astype(f32)).astype(bf16)


def spread(stacked, chooser):
    return lax.dot_general(stacked, chooser, (((0,), (0,)), ((), ())), preferred_element_type=f32)


def choosers(rows, lanes):
    k = lax.broadcasted_iota(jnp.int32, (rows, rows * lanes), 0)
    n = lax.broadcasted_iota(jnp.int32, (rows, rows * lanes), 1)
    one = jnp.where(k == n // lanes, 1.0, 0.0).astype(bf16)
    return jnp.concatenate([one] * 3, axis=0)


def read_kernel(
    q_ref, f_ref, v_ref, g_ref, bound_ref, gain_ref, choose_ref, state_ref, mix_ref, stacked, reads
):
    rows, heads, size = state_ref.shape[:3]
    wide = 2 * size
    query = rounded(q_ref)
    query = query * jax.nn.sigmoid(query)
    forget, keyvec = gates(rounded(f_ref), bound_ref[...])
    value = rounded(v_ref)
    gate = rounded(g_ref)
    scaled = jnp.concatenate(pieces(forget * query), axis=0)
    for pair in range(heads // 2):
        stacked[pair] = scaled[:, pair * wide : (pair + 1) * wide]

    def body(pair, carry):
        for two in range(rows // 2):
            at = slice(2 * two * wide, 2 * (two + 1) * wide)
            columns = spread(stacked[pair], choose_ref[:, at])
            for half in range(2):
                for b in range(2):
                    column = columns[half * size : (half + 1) * size, b * wide : b * wide + size]
                    product = state_ref[2 * two + b, 2 * pair + half] * column
                    folded = jnp.sum(product.reshape(size // 8, 8, size), axis=0)
                    reads[2 * pair + half, 2 * two + b : 2 * two + b + 1, :] = jnp.sum(
                        folded, axis=0, keepdims=True
                    )
        return carry

    lax.fori_loop(0, heads // 2, body, 0)
    agreement = keyvec * query
    gate = gate * jax.nn.sigmoid(gate)
    for pair in range(heads // 2):
        done = []
        for head in (2 * pair, 2 * pair + 1):
            own = slice(head * size, (head + 1) * size)
            read = reads[head] + jnp.sum(agreement[:, own], axis=1, keepdims=True) * value[:, own]
            power = jnp.mean(read * read, axis=1, keepdims=True)
            done.append(read * lax.rsqrt(power + epsilon) * gain_ref[...] * gate[:, own])
        mix_ref[:, pair * wide : (pair + 1) * wide] = jnp.concatenate(done, axis=1).astype(bf16)


def state_kernel(
    f_ref, v_ref, bound_ref, choose_ref, state_ref, out_ref, forgets, keys, values, old, ready, old_sems, sems
):
    rows, heads, size = state_ref.shape[:3]
    wide = 2 * size
    pairs = heads // 2

    def fetched(pair):
        slot = pair % 2
        return pltpu.make_async_copy(state_ref.at[:, pl.ds(2 * pair, 2)], old.at[slot], old_sems.at[slot])

    fetched(0).start()
    fetched(1).start()
    forget, keyvec = gates(rounded(f_ref), bound_ref[...])
    forget = jnp.concatenate(pieces(forget), axis=0)
    keyvec = jnp.concatenate(pieces(keyvec), axis=0)
    value = rounded(v_ref)
    for pair in range(heads // 2):
        own = slice(pair * wide, (pair + 1) * wide)
        forgets[pair] = forget[:, own]
        keys[pair] = keyvec[:, own]
    for head in range(heads):
        values[head] = value[:, head * size : (head + 1) * size]

    def copied(pair):
        slot = pair % 2
        return pltpu.make_async_copy(ready.at[slot], out_ref.at[:, pl.ds(2 * pair, 2)], sems.at[slot])

    def body(pair, carry):
        @pl.when(pair >= 2)
        def _():
            copied(pair - 2).wait()

        fetched(pair).wait()
        slot = pair % 2
        for two in range(rows // 2):
            at = slice(2 * two * wide, 2 * (two + 1) * wide)
            kept = spread(forgets[pair], choose_ref[:, at])
            added = spread(keys[pair], choose_ref[:, at])
            for half in range(2):
                for b in range(2):
                    part = (slice(half * size, (half + 1) * size), slice(b * wide, b * wide + size))
                    row = 2 * two + b
                    ready[slot, row, half] = (
                        kept[part] * old[slot, row, half]
                        + added[part] * values[2 * pair + half, row : row + 1, :]
                    )
        copied(pair).start()

        @pl.when(pair + 2 < pairs)
        def _():
            fetched(pair + 2).start()

        return carry

    lax.fori_loop(0, pairs, body, 0)
    copied(pairs - 2).wait()
    copied(pairs - 1).wait()


def message_kernel(mine_ref, arrived_ref, tokens_ref, gain_ref, bias_ref, out_ref):
    rows, size = mine_ref.shape
    first = residual_scale * tokens_ref[...].astype(f32) + (mine_ref[...] + arrived_ref[...])
    center = jnp.mean(first, axis=1, keepdims=True)
    first = first - center
    power = jnp.sum(first * first, axis=1, keepdims=True)
    lane = lax.broadcasted_iota(jnp.int32, (rows, size), 1)
    turned = jnp.where(lane == 0, center, jnp.where(lane == 1, power, 0.0))
    turned = [jnp.transpose(turned[r : r + size])[0:8] for r in range(0, rows, size)]
    centers = pieces(jnp.concatenate([v[0:1] for v in turned], axis=0))
    powers = pieces(jnp.concatenate([v[1:2] for v in turned], axis=0))
    tail = [p.astype(f32) for p in (*centers, *powers[:2], *pieces(gain_ref[...]), *pieces(bias_ref[...]))]
    tail = jnp.concatenate(tail, axis=0).astype(bf16)
    first = first.astype(bf16)
    for i in range(out_ref.shape[0]):
        out_ref[i, :rows] = first
        out_ref[i, rows:] = tail


def mlp_kernel(
    at_ref,
    ours_ref,
    other_ref,
    choose_ref,
    up_hbm,
    down_hbm,
    theirs_ref,
    mine_ref,
    own_ref,
    joined,
    shifts,
    up_ref,
    down_ref,
    sems,
):
    up_copy = pltpu.make_async_copy(up_hbm, up_ref, sems.at[0])
    down_copy = pltpu.make_async_copy(down_hbm, down_ref, sems.at[1])
    up_copy.start()
    down_copy.start()
    t, kv = at_ref[0], at_ref[1]
    blocks, rows, size = ours_ref.shape
    rows -= 16
    tails = []
    for ref in (ours_ref, other_ref):
        for k in range(blocks):
            tails.append(ref[k, rows:].astype(f32))
    centers = [v[0:2] + v[2:4] + v[4:6] for v in tails]
    center = sum(centers) * (1.0 / len(centers))
    centers = [c - center for c in centers]
    power = sum(v[6:8] + v[8:10] for v in tails) + size * sum(c * c for c in centers)
    scale = lax.rsqrt(power * (1.0 / (size * len(tails))) + epsilon)
    wanted = [*(c * scale for c in centers)]
    lines = [jnp.concatenate([v[r : r + 1] for v in wanted], axis=0) for r in range(rows // size)]
    lines = jnp.concatenate(lines, axis=1)
    shifts[...] = jnp.concatenate(pieces(lines), axis=0)
    factor = jnp.concatenate(
        [jnp.transpose(jnp.broadcast_to(scale[r : r + 1], (size, size))) for r in range(rows // size)], axis=0
    )
    for side, ref in enumerate((ours_ref, other_ref)):
        for k in range(blocks):
            block = side * blocks + k
            shift = spread(shifts[...], choose_ref[:, block * size : (block + 1) * size])
            v = tails[block]
            gain = v[10:11] + v[11:12] + v[12:13]
            bias = v[13:14] + v[14:15] + v[15:16]
            value = (ref[k, :rows].astype(f32) * factor + shift) * gain + bias
            to = 2 * k + (t if side == 0 else 1 - t)
            joined[:, pl.ds(pl.multiple_of(to * size, size), size)] = value.astype(bf16)
    own_ref[...] = joined[:, pl.ds(pl.multiple_of((2 * kv + t) * size, size), size)]
    up_copy.wait()
    upper = dot(joined[...], up_ref[...])
    hidden = jnp.square(jnp.maximum(upper, 0.0)).astype(bf16)
    down_copy.wait()
    for k in range(blocks):
        both = dot(hidden, down_ref[:, 2 * k * size : 2 * (k + 1) * size])
        left, right = both[:, :size], both[:, size:]
        at = slice((k % 4) * size, (k % 4 + 1) * size)
        theirs_ref[k // 4, :, at] = jnp.where(t == 0, right, left).astype(bf16)
        mine_ref[k // 4, :, at] = jnp.where(t == 0, left, right)


def in_vmem(n):
    return [pl.BlockSpec(memory_space=pltpu.VMEM)] * n


def in_hbm(value):
    return pltpu.with_memory_space_constraint(value, pltpu.HBM)


def mixed_heads(query, forget, value, gate, bound, head_gain, chooser, state):
    rows, heads, size = state.shape[:3]
    return pl.pallas_call(
        read_kernel,
        out_shape=jax.ShapeDtypeStruct((rows, heads * size), bf16),
        in_specs=in_vmem(8),
        out_specs=in_vmem(1)[0],
        scratch_shapes=[
            pltpu.VMEM((heads // 2, 3 * rows, 2 * size), bf16),
            pltpu.VMEM((heads, rows, size), f32),
        ],
        cost_estimate=pl.CostEstimate(flops=1 << 22, bytes_accessed=1 << 23, transcendentals=0),
        compiler_params=pltpu.CompilerParams(vmem_limit_bytes=8 << 20),
        name="heads_read",
    )(query, forget, value, gate, bound[None], head_gain[None], chooser, state)


def updated_state(forget, value, bound, chooser, state):
    rows, heads, size = state.shape[:3]
    return pl.pallas_call(
        state_kernel,
        out_shape=jax.ShapeDtypeStruct(state.shape, f32),
        in_specs=[*in_vmem(4), pl.BlockSpec(memory_space=pltpu.HBM)],
        out_specs=pl.BlockSpec(memory_space=pltpu.HBM),
        scratch_shapes=[
            pltpu.VMEM((heads // 2, 3 * rows, 2 * size), bf16),
            pltpu.VMEM((heads // 2, 3 * rows, 2 * size), bf16),
            pltpu.VMEM((heads, rows, size), f32),
            pltpu.VMEM((2, rows, 2, size, size), f32),
            pltpu.VMEM((2, rows, 2, size, size), f32),
            pltpu.SemaphoreType.DMA((2,)),
            pltpu.SemaphoreType.DMA((2,)),
        ],
        cost_estimate=pl.CostEstimate(flops=1 << 27, bytes_accessed=1 << 25, transcendentals=0),
        compiler_params=pltpu.CompilerParams(vmem_limit_bytes=12 << 20),
        name="state_update",
    )(forget, value, bound[None], chooser, in_hbm(state))


def message(mine, arrived, own_tokens, gain, bias):
    rows, size = mine.shape
    return pl.pallas_call(
        message_kernel,
        out_shape=jax.ShapeDtypeStruct((4, rows + 16, size), bf16),
        in_specs=in_vmem(5),
        out_specs=in_vmem(1)[0],
        compiler_params=pltpu.CompilerParams(vmem_limit_bytes=4 << 20),
        name="first_message",
    )(mine, arrived, own_tokens, gain[None], bias[None])


def mixer(at, ours, other, chooser, w_up, w_down):
    blocks, rows, size = ours.shape
    rows -= 16
    shape = (4, rows, blocks // 4 * size)
    return pl.pallas_call(
        mlp_kernel,
        out_shape=(
            jax.ShapeDtypeStruct(shape, bf16),
            jax.ShapeDtypeStruct(shape, f32),
            jax.ShapeDtypeStruct((rows, size), bf16),
        ),
        in_specs=[
            pl.BlockSpec(memory_space=pltpu.SMEM),
            *in_vmem(3),
            *[pl.BlockSpec(memory_space=pltpu.HBM)] * 2,
        ],
        out_specs=tuple(in_vmem(3)),
        scratch_shapes=[
            pltpu.VMEM((rows, 2 * blocks * size), bf16),
            pltpu.VMEM((6 * blocks, rows), bf16),
            pltpu.VMEM(w_up.shape, bf16),
            pltpu.VMEM(w_down.shape, bf16),
            pltpu.SemaphoreType.DMA((2,)),
        ],
        cost_estimate=pl.CostEstimate(flops=1 << 31, bytes_accessed=1 << 23, transcendentals=0),
        compiler_params=pltpu.CompilerParams(vmem_limit_bytes=28 << 20),
        name="channel_mixer",
    )(at, ours, other, chooser, in_hbm(w_up), in_hbm(w_down))


def per_device(
    tokens,
    state,
    w_query,
    w_forget,
    w_input,
    w_gate,
    lower_bound,
    head_gain,
    w_out,
    gain_one,
    bias_one,
    w_up,
    w_down,
    gain_two,
    bias_two,
):
    z, y, t = lax.axis_index("z"), lax.axis_index("y"), lax.axis_index("tp")
    rows = tokens.shape[0]
    rows_own = rows // 16
    width = w_query.shape[1]

    streams = []
    for weight, z_first, flip in (
        (w_query, True, 1),
        (w_forget, True, 3),
        (w_input, False, 1),
        (w_gate, False, 3),
    ):
        if z_first:
            order = row_order(rows, z, flip, y, flip, 4, 1)
            axes = ("z", flip, "y", flip)
        else:
            order = row_order(rows, y, flip, z, flip, 1, 4)
            axes = ("y", flip, "z", flip)
        streams.append(scattered_sum(dot(order, tokens).astype(bf16), weight, *axes))
    query_raw, forget_raw, value_raw, gate_raw = streams
    chooser = choosers(rows_own, 2 * head_gain.shape[0])
    held = pltpu.with_memory_space_constraint(state, pltpu.VMEM)
    mixout = mixed_heads(
        query_raw, forget_raw, value_raw, gate_raw, lower_bound, head_gain, chooser, held
    )
    new_state = updated_state(forget_raw, value_raw, lower_bound, chooser, state)

    mixout = of_all(of_all(mixout[None], "y").reshape(1, 4 * rows_own, width), "z").reshape(rows, width)
    mixout, new_state = lax.optimization_barrier((mixout, new_state))
    columns = w_out.shape[1] // 2
    w_out = w_out.reshape(width, 2, columns)
    theirs = dot(mixout, lax.dynamic_index_in_dim(w_out, 1 - t, 1, False))
    arrived = flipped(theirs, "tp", 1)
    mine = dot(mixout, lax.dynamic_index_in_dim(w_out, t, 1, False))
    own_tokens = lax.dynamic_slice_in_dim(tokens, t * columns, columns, 1)
    sent = message(mine, arrived, own_tokens, gain_one, bias_one)
    gathered = of_all(exchanged(sent, "y")[None], "z")
    ours = gathered.reshape(16, rows + 16, columns)
    other = flipped(ours, "tp", 1)
    at = jnp.stack([t, 4 * z + y])
    theirs, mine, normed_own = mixer(at, ours, other, choosers(32, columns), w_up, w_down)
    mlp = halved(mine, flipped(theirs, "tp", 1)).astype(bf16)
    mlp = exchanged(mlp, "z").astype(f32).sum(axis=0).astype(bf16)
    tiles = jnp.moveaxis(mlp.reshape(rows, 4, columns), 1, 0)
    mlp = exchanged(tiles, "y").astype(f32).sum(axis=0)
    second = residual_scale * normed_own.astype(f32) + mlp
    total, squares = packed_total(
        (jnp.sum(second, axis=1), jnp.sum(second * second, axis=1)), ("z", "y", "tp")
    )
    result = finish_norm(second, total, squares, D, gain_two, bias_two).astype(bf16)
    return (result, new_state)


def solution(mesh):
    fine = Mesh(mesh.devices.reshape(4, 4, 4, 2), ("dp", "z", "y", "tp"))
    kv = ("z", "y")
    every = ("z", "y", "tp")
    placed = (
        P("dp", kv),
        P(("dp", "z", "y"), "tp", None, None),
        P(kv, "tp"),
        P(kv, "tp"),
        P(kv, "tp"),
        P(kv, "tp"),
        P("tp"),
        P(),
        P("tp", kv),
        P(every),
        P(every),
        P(None, every),
        P(every, None),
        P(every),
        P(every),
    )
    return jax.shard_map(
        per_device,
        mesh=fine,
        in_specs=placed,
        out_specs=(P("dp", every), P(("dp", "z", "y"), "tp", None, None)),
        check_vma=False,
    )
```

```python
import jax
import jax.numpy as jnp
from jax import lax
from jax.experimental import pallas as pl
from jax.experimental.pallas import tpu as pltpu
from jax.sharding import Mesh
from jax.sharding import PartitionSpec as P

D = 4096
epsilon = 0.1
residual_scale = 1.68
f32 = jnp.float32
bf16 = jnp.bfloat16


def dot(a, b):
    return jnp.dot(a, b, preferred_element_type=f32)


def flipped(value, axis, bits):
    return lax.ppermute(value, axis, [(i, i ^ bits) for i in range(lax.axis_size(axis))])


def exchanged(tiles, axis):
    return lax.all_to_all(tiles, axis, split_axis=0, concat_axis=0, tiled=True)


def of_all(value, axis):
    return exchanged(jnp.broadcast_to(value, (lax.axis_size(axis), *value.shape)), axis)


def relative(flip):
    return (0, 4 - flip, flip, 2)


def row_order(rows, outer, outer_flip, inner, inner_flip, outer_stride, inner_stride):
    own = rows // 16
    p = lax.broadcasted_iota(jnp.int32, (rows, rows), 0)
    c = lax.broadcasted_iota(jnp.int32, (rows, rows), 1)
    block = p // own

    def flip_of(i, flip):
        r = relative(flip)
        return jnp.where(i == 0, r[0], jnp.where(i == 1, r[1], jnp.where(i == 2, r[2], r[3])))

    o = jnp.bitwise_xor(outer, flip_of(block // 4, outer_flip))
    i = jnp.bitwise_xor(inner, flip_of(block % 4, inner_flip))
    source = (o * outer_stride + i * inner_stride) * own + p % own
    return (c == source).astype(bf16)


def halved(kept, received):
    return kept + received.astype(f32)


def scattered_sum(tokens, weight, first, flip_first, second, flip_second):
    rows = tokens.shape[0]
    sent = dot(tokens[rows // 2 :], weight).astype(bf16)
    arrived = flipped(sent, first, flip_first)
    total = halved(dot(tokens[: rows // 2], weight), arrived)
    for axis, flip in ((first, 4 - flip_first), (second, flip_second), (second, 4 - flip_second)):
        rows = total.shape[0]
        arrived = flipped(total[rows // 2 :].astype(bf16), axis, flip)
        total = halved(total[: rows // 2], arrived)
    return total


def packed_total(arrays, axis):
    line = jnp.stack(arrays)
    got = of_all(line[None], axis).sum(axis=0)[0]
    return got[0], got[1]


def finish_norm(values, total, squares, width, gain, bias):
    center = total[:, None] / width
    spread = squares[:, None] / width - center * center
    return (values - center) * lax.rsqrt(spread + epsilon) * gain + bias


def rounded(ref):
    return ref[...].astype(bf16).astype(f32)


def gates(forget_raw, bound):
    rest = 1.0 - bound
    return bound + rest * jax.nn.sigmoid(forget_raw), rest * jax.nn.sigmoid(-forget_raw)


def pieces(value):
    high = value.astype(bf16)
    rest = value - high.astype(f32)
    middle = rest.astype(bf16)
    return high, middle, (rest - middle.astype(f32)).astype(bf16)


def spread(stacked, chooser):
    return dot(stacked, chooser)


def choosers(rows, lanes):
    k = lax.broadcasted_iota(jnp.int32, (rows, rows * lanes), 0)
    n = lax.broadcasted_iota(jnp.int32, (rows, rows * lanes), 1)
    one = jnp.where(k == n // lanes, 1.0, 0.0).astype(bf16)
    return jnp.concatenate([one] * 3, axis=0)


def read_kernel(
    q_ref, f_ref, v_ref, g_ref, bound_ref, gain_ref, choose_ref, state_ref, mix_ref, stacked, reads
):
    rows, heads, size = state_ref.shape[:3]
    wide = 2 * size
    query = rounded(q_ref)
    query = query * jax.nn.sigmoid(query)
    forget, keyvec = gates(rounded(f_ref), bound_ref[...])
    value = rounded(v_ref)
    gate = rounded(g_ref)
    scaled = jnp.concatenate(pieces(forget * query), axis=0)
    for pair in range(heads // 2):
        stacked[pair] = jnp.transpose(scaled[:, pair * wide : (pair + 1) * wide])

    def body(pair, carry):
        for two in range(rows // 2):
            at = slice(2 * two * wide, 2 * (two + 1) * wide)
            columns = spread(stacked[pair], choose_ref[:, at])
            for half in range(2):
                for b in range(2):
                    column = columns[half * size : (half + 1) * size, b * wide : b * wide + size]
                    product = state_ref[2 * two + b, 2 * pair + half] * column
                    folded = jnp.sum(product.reshape(size // 8, 8, size), axis=0)
                    reads[2 * pair + half, 2 * two + b : 2 * two + b + 1, :] = jnp.sum(
                        folded, axis=0, keepdims=True
                    )
        return carry

    lax.fori_loop(0, heads // 2, body, 0)
    agreement = keyvec * query
    gate = gate * jax.nn.sigmoid(gate)
    for pair in range(heads // 2):
        done = []
        for head in (2 * pair, 2 * pair + 1):
            own = slice(head * size, (head + 1) * size)
            read = reads[head] + jnp.sum(agreement[:, own], axis=1, keepdims=True) * value[:, own]
            power = jnp.mean(read * read, axis=1, keepdims=True)
            done.append(read * lax.rsqrt(power + epsilon) * gain_ref[...] * gate[:, own])
        mix = jnp.concatenate(done, axis=1).astype(bf16)
        for i in range(mix_ref.shape[0]):
            mix_ref[i, :, pair * wide : (pair + 1) * wide] = mix


def state_kernel(
    f_ref, v_ref, bound_ref, choose_ref, state_ref, out_ref, forgets, keys, values, old, ready, old_sems, sems
):
    rows, heads, size = state_ref.shape[:3]
    wide = 2 * size
    pairs = heads // 2

    def fetched(pair):
        slot = pair % 2
        return pltpu.make_async_copy(state_ref.at[:, pl.ds(2 * pair, 2)], old.at[slot], old_sems.at[slot])

    fetched(0).start()
    fetched(1).start()
    forget, keyvec = gates(rounded(f_ref), bound_ref[...])
    forget = jnp.concatenate(pieces(forget), axis=0)
    keyvec = jnp.concatenate(pieces(keyvec), axis=0)
    value = rounded(v_ref)
    for pair in range(heads // 2):
        own = slice(pair * wide, (pair + 1) * wide)
        forgets[pair] = jnp.transpose(forget[:, own])
        keys[pair] = jnp.transpose(keyvec[:, own])
    for head in range(heads):
        values[head] = value[:, head * size : (head + 1) * size]

    def copied(pair):
        slot = pair % 2
        return pltpu.make_async_copy(ready.at[slot], out_ref.at[:, pl.ds(2 * pair, 2)], sems.at[slot])

    def body(pair, carry):
        @pl.when(pair >= 2)
        def _():
            copied(pair - 2).wait()

        fetched(pair).wait()
        slot = pair % 2
        for two in range(rows // 2):
            at = slice(2 * two * wide, 2 * (two + 1) * wide)
            kept = spread(forgets[pair], choose_ref[:, at])
            added = spread(keys[pair], choose_ref[:, at])
            for half in range(2):
                for b in range(2):
                    part = (slice(half * size, (half + 1) * size), slice(b * wide, b * wide + size))
                    row = 2 * two + b
                    ready[slot, row, half] = (
                        kept[part] * old[slot, row, half]
                        + added[part] * values[2 * pair + half, row : row + 1, :]
                    )
        copied(pair).start()

        @pl.when(pair + 2 < pairs)
        def _():
            fetched(pair + 2).start()

        return carry

    lax.fori_loop(0, pairs, body, 0)
    copied(pairs - 2).wait()
    copied(pairs - 1).wait()


def message_kernel(mine_ref, arrived_ref, tokens_ref, gain_ref, bias_ref, out_ref):
    rows, size = mine_ref.shape
    first = residual_scale * tokens_ref[...].astype(f32) + (mine_ref[...] + arrived_ref[...])
    center = jnp.mean(first, axis=1, keepdims=True)
    first = first - center
    power = jnp.sum(first * first, axis=1, keepdims=True)
    lane = lax.broadcasted_iota(jnp.int32, (rows, size), 1)
    turned = jnp.where(lane == 0, center, jnp.where(lane == 1, power, 0.0))
    turned = [jnp.transpose(turned[r : r + size])[0:8] for r in range(0, rows, size)]
    centers = pieces(jnp.concatenate([v[0:1] for v in turned], axis=0))
    powers = pieces(jnp.concatenate([v[1:2] for v in turned], axis=0))
    tail = [p.astype(f32) for p in (*centers, *powers[:2], *pieces(gain_ref[...]), *pieces(bias_ref[...]))]
    tail = jnp.concatenate(tail, axis=0).astype(bf16)
    first = first.astype(bf16)
    for i in range(out_ref.shape[0]):
        out_ref[i, :rows] = first
        out_ref[i, rows:] = tail


def mlp_kernel(
    at_ref,
    ours_ref,
    other_ref,
    choose_ref,
    up_hbm,
    down_hbm,
    theirs_ref,
    mine_ref,
    own_ref,
    joined,
    shifts,
    up_ref,
    down_ref,
    sems,
):
    up_copy = pltpu.make_async_copy(up_hbm, up_ref, sems.at[0])
    down_copy = pltpu.make_async_copy(down_hbm, down_ref, sems.at[1])
    up_copy.start()
    down_copy.start()
    t, kv = at_ref[0], at_ref[1]
    blocks, rows, size = ours_ref.shape
    rows -= 16
    tails = []
    for ref in (ours_ref, other_ref):
        for k in range(blocks):
            tails.append(ref[k, rows:].astype(f32))
    centers = [v[0:2] + v[2:4] + v[4:6] for v in tails]
    center = sum(centers) * (1.0 / len(centers))
    centers = [c - center for c in centers]
    power = sum(v[6:8] + v[8:10] for v in tails) + size * sum(c * c for c in centers)
    scale = lax.rsqrt(power * (1.0 / (size * len(tails))) + epsilon)
    wanted = [*(c * scale for c in centers)]
    lines = [jnp.concatenate([v[r : r + 1] for v in wanted], axis=0) for r in range(rows // size)]
    lines = jnp.concatenate(lines, axis=1)
    shifts[...] = jnp.transpose(jnp.concatenate(pieces(lines), axis=0))
    factor = jnp.concatenate(
        [jnp.transpose(jnp.broadcast_to(scale[r : r + 1], (size, size))) for r in range(rows // size)], axis=0
    )
    for side, ref in enumerate((ours_ref, other_ref)):
        for k in range(blocks):
            block = side * blocks + k
            shift = spread(shifts[...], choose_ref[:, block * size : (block + 1) * size])
            v = tails[block]
            gain = v[10:11] + v[11:12] + v[12:13]
            bias = v[13:14] + v[14:15] + v[15:16]
            value = (ref[k, :rows].astype(f32) * factor + shift) * gain + bias
            to = 2 * k + (t if side == 0 else 1 - t)
            joined[:, pl.ds(pl.multiple_of(to * size, size), size)] = value.astype(bf16)
    own_ref[...] = joined[:, pl.ds(pl.multiple_of((2 * kv + t) * size, size), size)]
    up_copy.wait()
    upper = dot(joined[...], up_ref[...])
    hidden = jnp.square(jnp.maximum(upper, 0.0)).astype(bf16)
    down_copy.wait()
    for k in range(blocks):
        both = dot(hidden, down_ref[:, 2 * k * size : 2 * (k + 1) * size])
        left, right = both[:, :size], both[:, size:]
        theirs_ref[k] = jnp.where(t == 0, right, left).astype(bf16)
        mine_ref[k] = jnp.where(t == 0, left, right)


def in_vmem(n):
    return [pl.BlockSpec(memory_space=pltpu.VMEM)] * n


def in_hbm(value):
    return pltpu.with_memory_space_constraint(value, pltpu.HBM)


def mixed_heads(query, forget, value, gate, bound, head_gain, chooser, state):
    rows, heads, size = state.shape[:3]
    return pl.pallas_call(
        read_kernel,
        out_shape=jax.ShapeDtypeStruct((16, rows, heads * size), bf16),
        in_specs=in_vmem(8),
        out_specs=in_vmem(1)[0],
        scratch_shapes=[
            pltpu.VMEM((heads // 2, 2 * size, 3 * rows), bf16),
            pltpu.VMEM((heads, rows, size), f32),
        ],
        cost_estimate=pl.CostEstimate(flops=1 << 22, bytes_accessed=1 << 23, transcendentals=0),
        compiler_params=pltpu.CompilerParams(vmem_limit_bytes=8 << 20),
        name="heads_read",
    )(query, forget, value, gate, bound[None], head_gain[None], chooser, state)


def updated_state(forget, value, bound, chooser, state):
    rows, heads, size = state.shape[:3]
    return pl.pallas_call(
        state_kernel,
        out_shape=jax.ShapeDtypeStruct(state.shape, f32),
        in_specs=[*in_vmem(4), pl.BlockSpec(memory_space=pltpu.HBM)],
        out_specs=pl.BlockSpec(memory_space=pltpu.HBM),
        scratch_shapes=[
            pltpu.VMEM((heads // 2, 2 * size, 3 * rows), bf16),
            pltpu.VMEM((heads // 2, 2 * size, 3 * rows), bf16),
            pltpu.VMEM((heads, rows, size), f32),
            pltpu.VMEM((2, rows, 2, size, size), f32),
            pltpu.VMEM((2, rows, 2, size, size), f32),
            pltpu.SemaphoreType.DMA((2,)),
            pltpu.SemaphoreType.DMA((2,)),
        ],
        cost_estimate=pl.CostEstimate(flops=1 << 27, bytes_accessed=1 << 25, transcendentals=0),
        compiler_params=pltpu.CompilerParams(vmem_limit_bytes=12 << 20),
        name="state_update",
    )(forget, value, bound[None], chooser, in_hbm(state))


def message(mine, arrived, own_tokens, gain, bias):
    rows, size = mine.shape
    return pl.pallas_call(
        message_kernel,
        out_shape=jax.ShapeDtypeStruct((16, rows + 16, size), bf16),
        in_specs=in_vmem(5),
        out_specs=in_vmem(1)[0],
        compiler_params=pltpu.CompilerParams(vmem_limit_bytes=4 << 20),
        name="first_message",
    )(mine, arrived, own_tokens, gain[None], bias[None])


def mixer(at, ours, other, chooser, w_up, w_down):
    blocks, rows, size = ours.shape
    rows -= 16
    shape = (blocks, rows, size)
    return pl.pallas_call(
        mlp_kernel,
        out_shape=(
            jax.ShapeDtypeStruct(shape, bf16),
            jax.ShapeDtypeStruct(shape, f32),
            jax.ShapeDtypeStruct((rows, size), bf16),
        ),
        in_specs=[
            pl.BlockSpec(memory_space=pltpu.SMEM),
            *in_vmem(3),
            *[pl.BlockSpec(memory_space=pltpu.HBM)] * 2,
        ],
        out_specs=tuple(in_vmem(3)),
        scratch_shapes=[
            pltpu.VMEM((rows, 2 * blocks * size), bf16),
            pltpu.VMEM((rows, 6 * blocks), bf16),
            pltpu.VMEM(w_up.shape, bf16),
            pltpu.VMEM(w_down.shape, bf16),
            pltpu.SemaphoreType.DMA((2,)),
        ],
        cost_estimate=pl.CostEstimate(flops=1 << 31, bytes_accessed=1 << 23, transcendentals=0),
        compiler_params=pltpu.CompilerParams(vmem_limit_bytes=28 << 20),
        name="channel_mixer",
    )(at, ours, other, chooser, in_hbm(w_up), in_hbm(w_down))


def per_device(
    tokens,
    state,
    w_query,
    w_forget,
    w_input,
    w_gate,
    lower_bound,
    head_gain,
    w_out,
    gain_one,
    bias_one,
    w_up,
    w_down,
    gain_two,
    bias_two,
):
    z, y, t = lax.axis_index("z"), lax.axis_index("y"), lax.axis_index("tp")
    rows = tokens.shape[0]
    rows_own = rows // 16
    width = w_query.shape[1]

    streams = []
    for weight, z_first, flip in (
        (w_query, True, 1),
        (w_forget, True, 3),
        (w_input, False, 1),
        (w_gate, False, 3),
    ):
        if z_first:
            order = row_order(rows, z, flip, y, flip, 4, 1)
            axes = ("z", flip, "y", flip)
        else:
            order = row_order(rows, y, flip, z, flip, 1, 4)
            axes = ("y", flip, "z", flip)
        streams.append(scattered_sum(dot(order, tokens).astype(bf16), weight, *axes))
    query_raw, forget_raw, value_raw, gate_raw = streams
    chooser = choosers(rows_own, 2 * head_gain.shape[0])
    held = pltpu.with_memory_space_constraint(state, pltpu.VMEM)
    mixout = mixed_heads(
        query_raw, forget_raw, value_raw, gate_raw, lower_bound, head_gain, chooser, held
    )
    new_state = updated_state(forget_raw, value_raw, lower_bound, chooser, state)

    mixout = exchanged(mixout, ("z", "y")).reshape(rows, width)
    mixout, new_state = lax.optimization_barrier((mixout, new_state))
    columns = w_out.shape[1] // 2
    w_out = w_out.reshape(width, 2, columns)
    theirs = dot(mixout, lax.dynamic_index_in_dim(w_out, 1 - t, 1, False))
    arrived = flipped(theirs, "tp", 1)
    mine = dot(mixout, lax.dynamic_index_in_dim(w_out, t, 1, False))
    own_tokens = lax.dynamic_slice_in_dim(tokens, t * columns, columns, 1)
    sent = message(mine, arrived, own_tokens, gain_one, bias_one)
    ours = exchanged(sent, ("z", "y"))
    other = flipped(ours, "tp", 1)
    at = jnp.stack([t, 4 * z + y])
    theirs, mine, normed_own = mixer(at, ours, other, choosers(32, columns), w_up, w_down)
    mlp = halved(mine, flipped(theirs, "tp", 1)).astype(bf16)
    mlp = exchanged(mlp, ("z", "y")).astype(f32).sum(axis=0)
    second = residual_scale * normed_own.astype(f32) + mlp
    total, squares = packed_total(
        (jnp.sum(second, axis=1), jnp.sum(second * second, axis=1)), ("z", "y", "tp")
    )
    result = finish_norm(second, total, squares, D, gain_two, bias_two).astype(bf16)
    return (result, new_state)


def solution(mesh):
    fine = Mesh(mesh.devices.reshape(4, 4, 4, 2), ("dp", "z", "y", "tp"))
    kv = ("z", "y")
    every = ("z", "y", "tp")
    placed = (
        P("dp", kv),
        P(("dp", "z", "y"), "tp", None, None),
        P(kv, "tp"),
        P(kv, "tp"),
        P(kv, "tp"),
        P(kv, "tp"),
        P("tp"),
        P(),
        P("tp", kv),
        P(every),
        P(every),
        P(None, every),
        P(every, None),
        P(every),
        P(every),
    )
    return jax.shard_map(
        per_device,
        mesh=fine,
        in_specs=placed,
        out_specs=(P("dp", every), P(("dp", "z", "y"), "tp", None, None)),
        check_vma=False,
    )
```

```python
import jax
import jax.numpy as jnp
from jax import lax
from jax.experimental import pallas as pl
from jax.experimental.pallas import tpu as pltpu
from jax.sharding import Mesh
from jax.sharding import PartitionSpec as P

D = 4096
epsilon = 0.1
residual_scale = 1.68
f32 = jnp.float32
bf16 = jnp.bfloat16


def dot(a, b):
    return jnp.dot(a, b, preferred_element_type=f32)


def flipped(value, axis, bits):
    return lax.ppermute(value, axis, [(i, i ^ bits) for i in range(lax.axis_size(axis))])


def exchanged(tiles, axis):
    return lax.all_to_all(tiles, axis, split_axis=0, concat_axis=0, tiled=True)


def of_all(value, axis):
    return exchanged(jnp.broadcast_to(value, (lax.axis_size(axis), *value.shape)), axis)


def relative(flip):
    return (0, 4 - flip, flip, 2)


def row_order(rows, outer, outer_flip, inner, inner_flip, outer_stride, inner_stride):
    own = rows // 16
    p = lax.broadcasted_iota(jnp.int32, (rows, rows), 0)
    c = lax.broadcasted_iota(jnp.int32, (rows, rows), 1)
    block = p // own

    def flip_of(i, flip):
        r = relative(flip)
        return jnp.where(i == 0, r[0], jnp.where(i == 1, r[1], jnp.where(i == 2, r[2], r[3])))

    o = jnp.bitwise_xor(outer, flip_of(block // 4, outer_flip))
    i = jnp.bitwise_xor(inner, flip_of(block % 4, inner_flip))
    source = (o * outer_stride + i * inner_stride) * own + p % own
    return (c == source).astype(bf16)


def halved(kept, received):
    return kept + received.astype(f32)


def scattered_sum(tokens, weight, first, flip_first, second, flip_second):
    rows = tokens.shape[0]
    sent = dot(tokens[rows // 2 :], weight).astype(bf16)
    arrived = flipped(sent, first, flip_first)
    total = halved(dot(tokens[: rows // 2], weight), arrived)
    for axis, flip in ((first, 4 - flip_first), (second, flip_second), (second, 4 - flip_second)):
        rows = total.shape[0]
        arrived = flipped(total[rows // 2 :].astype(bf16), axis, flip)
        total = halved(total[: rows // 2], arrived)
    return total


def packed_total(arrays, axis):
    line = jnp.stack(arrays)
    got = of_all(line[None], axis).sum(axis=0)[0]
    return got[0], got[1]


def finish_norm(values, total, squares, width, gain, bias):
    center = total[:, None] / width
    spread = squares[:, None] / width - center * center
    return (values - center) * lax.rsqrt(spread + epsilon) * gain + bias


def rounded(ref):
    return ref[...].astype(bf16).astype(f32)


def gates(forget_raw, bound):
    rest = 1.0 - bound
    return bound + rest * jax.nn.sigmoid(forget_raw), rest * jax.nn.sigmoid(-forget_raw)


def pieces(value):
    high = value.astype(bf16)
    rest = value - high.astype(f32)
    middle = rest.astype(bf16)
    return high, middle, (rest - middle.astype(f32)).astype(bf16)


def spread(stacked, chooser):
    return dot(stacked, chooser)


def choosers(rows, lanes):
    k = lax.broadcasted_iota(jnp.int32, (rows, rows * lanes), 0)
    n = lax.broadcasted_iota(jnp.int32, (rows, rows * lanes), 1)
    one = jnp.where(k == n // lanes, 1.0, 0.0).astype(bf16)
    return jnp.concatenate([one] * 3, axis=0)


def by_pairs(value, wide):
    return jnp.concatenate([value[:, at : at + wide] for at in range(0, value.shape[1], wide)], axis=0)


def read_kernel(q_ref, f_ref, bound_ref, choose_ref, state_hbm, reads_ref, stacked, state_ref, sems):
    rows, heads, size = state_ref.shape[:3]
    wide = 2 * size

    def fetched(pair):
        part = (slice(None), pl.ds(2 * pair, 2))
        return pltpu.make_async_copy(state_hbm.at[part], state_ref.at[part], sems.at[pair])

    for pair in range(heads // 2):
        fetched(pair).start()
    query = rounded(q_ref)
    forget, _ = gates(rounded(f_ref), bound_ref[...])
    scaled = jnp.concatenate(pieces(forget * query * jax.nn.sigmoid(query)), axis=0)
    for pair in range(heads // 2):
        stacked[pair] = jnp.transpose(scaled[:, pair * wide : (pair + 1) * wide])

    def body(pair, carry):
        fetched(pair).wait()
        for two in range(rows // 2):
            at = slice(2 * two * wide, 2 * (two + 1) * wide)
            columns = spread(stacked[pair], choose_ref[:, at])
            for b in range(2):
                folded = []
                for half in range(2):
                    column = columns[half * size : (half + 1) * size, b * wide : b * wide + size]
                    product = state_ref[2 * two + b, 2 * pair + half] * column
                    folded.append(jnp.sum(product.reshape(size // 8, 8, size), axis=0))
                total = jnp.sum(jnp.concatenate(folded, axis=1), axis=0, keepdims=True)
                reads_ref[pair, 2 * two + b : 2 * two + b + 1, :] = total
        return carry

    lax.fori_loop(0, heads // 2, body, 0)


def head_sums(value, size):
    wide = value.shape[1]
    a = lax.broadcasted_iota(jnp.int32, (wide, wide), 0) // size
    b = lax.broadcasted_iota(jnp.int32, (wide, wide), 1) // size
    ones = jnp.where(a == b, 1.0, 0.0).astype(bf16)
    return sum(dot(piece, ones) for piece in pieces(value))


def mix_kernel(q_ref, f_ref, v_ref, g_ref, bound_ref, gain_ref, reads_ref, mix_ref):
    pairs, rows, wide = reads_ref.shape
    query = rounded(q_ref)
    query = query * jax.nn.sigmoid(query)
    _, keyvec = gates(rounded(f_ref), bound_ref[...])
    gate = rounded(g_ref)
    gate = by_pairs(gate * jax.nn.sigmoid(gate), wide)
    agreement = head_sums(by_pairs(keyvec * query, wide), wide // 2)
    read = reads_ref[...].reshape(pairs * rows, wide) + agreement * by_pairs(rounded(v_ref), wide)
    power = head_sums(read * read, wide // 2) * (2.0 / wide)
    mix = (read * lax.rsqrt(power + epsilon) * gain_ref[...] * gate).astype(bf16)
    for pair in range(pairs):
        for i in range(mix_ref.shape[0]):
            mix_ref[i, :, pair * wide : (pair + 1) * wide] = mix[pair * rows : (pair + 1) * rows]


def state_kernel(
    f_ref, v_ref, bound_ref, choose_ref, state_ref, out_ref, forgets, keys, values, old, ready, old_sems, sems
):
    rows, heads, size = state_ref.shape[:3]
    wide = 2 * size
    pairs = heads // 2
    slots = ready.shape[0]

    def fetched(pair):
        slot = pair % slots
        return pltpu.make_async_copy(state_ref.at[:, pl.ds(2 * pair, 2)], old.at[slot], old_sems.at[slot])

    for slot in range(slots):
        fetched(slot).start()
    forget, keyvec = gates(rounded(f_ref), bound_ref[...])
    forget = jnp.concatenate(pieces(forget), axis=0)
    keyvec = jnp.concatenate(pieces(keyvec), axis=0)
    value = rounded(v_ref)
    for pair in range(heads // 2):
        own = slice(pair * wide, (pair + 1) * wide)
        forgets[pair] = jnp.transpose(forget[:, own])
        keys[pair] = jnp.transpose(keyvec[:, own])
    for head in range(heads):
        values[head] = value[:, head * size : (head + 1) * size]

    def copied(pair):
        slot = pair % slots
        return pltpu.make_async_copy(ready.at[slot], out_ref.at[:, pl.ds(2 * pair, 2)], sems.at[slot])

    def body(pair, carry):
        @pl.when(pair >= slots)
        def _():
            copied(pair - slots).wait()

        fetched(pair).wait()
        slot = pair % slots
        for two in range(rows // 2):
            at = slice(2 * two * wide, 2 * (two + 1) * wide)
            kept = spread(forgets[pair], choose_ref[:, at])
            added = spread(keys[pair], choose_ref[:, at])
            for half in range(2):
                for b in range(2):
                    part = (slice(half * size, (half + 1) * size), slice(b * wide, b * wide + size))
                    row = 2 * two + b
                    ready[slot, row, half] = (
                        kept[part] * old[slot, row, half]
                        + added[part] * values[2 * pair + half, row : row + 1, :]
                    )
        copied(pair).start()

        @pl.when(pair + slots < pairs)
        def _():
            fetched(pair + slots).start()

        return carry

    lax.fori_loop(0, pairs, body, 0)
    for slot in range(slots):
        copied(pairs - slots + slot).wait()


def message_kernel(mine_ref, arrived_ref, tokens_ref, gain_ref, bias_ref, out_ref):
    rows, size = mine_ref.shape
    first = residual_scale * tokens_ref[...].astype(f32) + (mine_ref[...] + arrived_ref[...])
    center = jnp.mean(first, axis=1, keepdims=True)
    first = first - center
    power = jnp.sum(first * first, axis=1, keepdims=True)
    lane = lax.broadcasted_iota(jnp.int32, (rows, size), 1)
    turned = jnp.where(lane == 0, center, jnp.where(lane == 1, power, 0.0))
    turned = [jnp.transpose(turned[r : r + size])[0:8] for r in range(0, rows, size)]
    centers = pieces(jnp.concatenate([v[0:1] for v in turned], axis=0))
    powers = pieces(jnp.concatenate([v[1:2] for v in turned], axis=0))
    tail = [p.astype(f32) for p in (*centers, *powers[:2], *pieces(gain_ref[...]), *pieces(bias_ref[...]))]
    tail = jnp.concatenate(tail, axis=0).astype(bf16)
    first = first.astype(bf16)
    for i in range(out_ref.shape[0]):
        out_ref[i, :rows] = first
        out_ref[i, rows:] = tail


def mlp_kernel(
    at_ref,
    ours_ref,
    other_ref,
    choose_ref,
    up_hbm,
    down_hbm,
    theirs_ref,
    mine_ref,
    own_ref,
    joined,
    shifts,
    up_ref,
    down_ref,
    sems,
):
    up_copy = pltpu.make_async_copy(up_hbm, up_ref, sems.at[0])
    down_copy = pltpu.make_async_copy(down_hbm, down_ref, sems.at[1])
    up_copy.start()
    t, kv = at_ref[0], at_ref[1]
    blocks, rows, size = ours_ref.shape
    rows -= 16
    tails = []
    for ref in (ours_ref, other_ref):
        for k in range(blocks):
            tails.append(ref[k, rows:].astype(f32))
    centers = [v[0:2] + v[2:4] + v[4:6] for v in tails]
    center = sum(centers) * (1.0 / len(centers))
    centers = [c - center for c in centers]
    power = sum(v[6:8] + v[8:10] for v in tails) + size * sum(c * c for c in centers)
    scale = lax.rsqrt(power * (1.0 / (size * len(tails))) + epsilon)
    wanted = [*(c * scale for c in centers)]
    lines = [jnp.concatenate([v[r : r + 1] for v in wanted], axis=0) for r in range(rows // size)]
    lines = jnp.concatenate(lines, axis=1)
    shifts[...] = jnp.transpose(jnp.concatenate(pieces(lines), axis=0))
    factor = jnp.concatenate(
        [jnp.transpose(jnp.broadcast_to(scale[r : r + 1], (size, size))) for r in range(rows // size)], axis=0
    )
    for side, ref in enumerate((ours_ref, other_ref)):
        if side == 1:
            down_copy.start()
        for k in range(blocks):
            block = side * blocks + k
            shift = spread(shifts[...], choose_ref[:, block * size : (block + 1) * size])
            v = tails[block]
            gain = v[10:11] + v[11:12] + v[12:13]
            bias = v[13:14] + v[14:15] + v[15:16]
            value = (ref[k, :rows].astype(f32) * factor + shift) * gain + bias
            to = 2 * k + (t if side == 0 else 1 - t)
            joined[:, pl.ds(pl.multiple_of(to * size, size), size)] = value.astype(bf16)
    own_ref[...] = joined[:, pl.ds(pl.multiple_of((2 * kv + t) * size, size), size)]
    up_copy.wait()
    upper = dot(joined[...], up_ref[...])
    hidden = jnp.square(jnp.maximum(upper, 0.0)).astype(bf16)
    down_copy.wait()
    for k in range(blocks):
        both = dot(hidden, down_ref[:, 2 * k * size : 2 * (k + 1) * size])
        left, right = both[:, :size], both[:, size:]
        theirs_ref[k] = jnp.where(t == 0, right, left).astype(bf16)
        mine_ref[k] = jnp.where(t == 0, left, right)


def in_hbm(value):
    return pltpu.with_memory_space_constraint(value, pltpu.HBM)


def in_vmem(n):
    return [pl.BlockSpec(memory_space=pltpu.VMEM)] * n


def in_hbm(value):
    return pltpu.with_memory_space_constraint(value, pltpu.HBM)


def head_reads(query, forget, bound, chooser, state):
    rows, heads, size = state.shape[:3]
    return pl.pallas_call(
        read_kernel,
        out_shape=jax.ShapeDtypeStruct((heads // 2, rows, 2 * size), f32),
        in_specs=[*in_vmem(4), pl.BlockSpec(memory_space=pltpu.HBM)],
        out_specs=in_vmem(1)[0],
        scratch_shapes=[
            pltpu.VMEM((heads // 2, 2 * size, 3 * rows), bf16),
            pltpu.VMEM(state.shape, f32),
            pltpu.SemaphoreType.DMA((heads // 2,)),
        ],
        cost_estimate=pl.CostEstimate(flops=1 << 26, bytes_accessed=1 << 23, transcendentals=0),
        compiler_params=pltpu.CompilerParams(vmem_limit_bytes=22 << 20),
        name="heads_read",
    )(query, forget, bound[None], chooser, in_hbm(state))


def mixed_heads(query, forget, value, gate, bound, head_gain, reads):
    pairs, rows, wide = reads.shape
    return pl.pallas_call(
        mix_kernel,
        out_shape=jax.ShapeDtypeStruct((16, rows, pairs * wide), bf16),
        in_specs=in_vmem(7),
        out_specs=in_vmem(1)[0],
        compiler_params=pltpu.CompilerParams(vmem_limit_bytes=6 << 20),
        name="heads_mix",
    )(query, forget, value, gate, bound[None], jnp.tile(head_gain, 2)[None], reads)


def updated_state(forget, value, bound, chooser, state):
    rows, heads, size = state.shape[:3]
    slots = 4
    block = pltpu.VMEM((slots, rows, 2, size, size), f32)
    return pl.pallas_call(
        state_kernel,
        out_shape=jax.ShapeDtypeStruct(state.shape, f32),
        in_specs=[*in_vmem(4), pl.BlockSpec(memory_space=pltpu.HBM)],
        out_specs=pl.BlockSpec(memory_space=pltpu.HBM),
        scratch_shapes=[
            pltpu.VMEM((heads // 2, 2 * size, 3 * rows), bf16),
            pltpu.VMEM((heads // 2, 2 * size, 3 * rows), bf16),
            pltpu.VMEM((heads, rows, size), f32),
            block,
            block,
            pltpu.SemaphoreType.DMA((slots,)),
            pltpu.SemaphoreType.DMA((slots,)),
        ],
        cost_estimate=pl.CostEstimate(flops=1 << 27, bytes_accessed=1 << 25, transcendentals=0),
        compiler_params=pltpu.CompilerParams(vmem_limit_bytes=16 << 20),
        name="state_update",
    )(forget, value, bound[None], chooser, in_hbm(state))


def message(mine, arrived, own_tokens, gain, bias):
    rows, size = mine.shape
    return pl.pallas_call(
        message_kernel,
        out_shape=jax.ShapeDtypeStruct((16, rows + 16, size), bf16),
        in_specs=in_vmem(5),
        out_specs=in_vmem(1)[0],
        compiler_params=pltpu.CompilerParams(vmem_limit_bytes=4 << 20),
        name="first_message",
    )(mine, arrived, own_tokens, gain[None], bias[None])


def mixer(at, ours, other, chooser, w_up, w_down):
    blocks, rows, size = ours.shape
    rows -= 16
    shape = (blocks, rows, size)
    return pl.pallas_call(
        mlp_kernel,
        out_shape=(
            jax.ShapeDtypeStruct(shape, bf16),
            jax.ShapeDtypeStruct(shape, f32),
            jax.ShapeDtypeStruct((rows, size), bf16),
        ),
        in_specs=[
            pl.BlockSpec(memory_space=pltpu.SMEM),
            *in_vmem(3),
            *[pl.BlockSpec(memory_space=pltpu.HBM)] * 2,
        ],
        out_specs=tuple(in_vmem(3)),
        scratch_shapes=[
            pltpu.VMEM((rows, 2 * blocks * size), bf16),
            pltpu.VMEM((rows, 6 * blocks), bf16),
            pltpu.VMEM(w_up.shape, bf16),
            pltpu.VMEM(w_down.shape, bf16),
            pltpu.SemaphoreType.DMA((2,)),
        ],
        cost_estimate=pl.CostEstimate(flops=1 << 31, bytes_accessed=1 << 23, transcendentals=0),
        compiler_params=pltpu.CompilerParams(vmem_limit_bytes=28 << 20),
        name="channel_mixer",
    )(at, ours, other, chooser, in_hbm(w_up), in_hbm(w_down))


def per_device(
    tokens,
    state,
    w_query,
    w_forget,
    w_input,
    w_gate,
    lower_bound,
    head_gain,
    w_out,
    gain_one,
    bias_one,
    w_up,
    w_down,
    gain_two,
    bias_two,
):
    z, y, t = lax.axis_index("z"), lax.axis_index("y"), lax.axis_index("tp")
    rows = tokens.shape[0]
    rows_own = rows // 16
    width = w_query.shape[1]

    streams = []
    for weight, z_first, flip in (
        (w_query, True, 1),
        (w_forget, True, 3),
        (w_input, False, 1),
        (w_gate, False, 3),
    ):
        if z_first:
            order = row_order(rows, z, flip, y, flip, 4, 1)
            axes = ("z", flip, "y", flip)
        else:
            order = row_order(rows, y, flip, z, flip, 1, 4)
            axes = ("y", flip, "z", flip)
        streams.append(scattered_sum(dot(order, tokens).astype(bf16), weight, *axes))
    query_raw, forget_raw, value_raw, gate_raw = streams
    chooser = choosers(rows_own, 2 * head_gain.shape[0])
    reads = head_reads(query_raw, forget_raw, lower_bound, chooser, state)
    mixout = mixed_heads(query_raw, forget_raw, value_raw, gate_raw, lower_bound, head_gain, reads)
    new_state = updated_state(forget_raw, value_raw, lower_bound, chooser, state)

    mixout = exchanged(mixout, ("z", "y")).reshape(rows, width)
    mixout, new_state = lax.optimization_barrier((mixout, new_state))
    columns = w_out.shape[1] // 2
    w_out = w_out.reshape(width, 2, columns)
    theirs = dot(mixout, lax.dynamic_index_in_dim(w_out, 1 - t, 1, False))
    arrived = flipped(theirs, "tp", 1)
    mine = dot(mixout, lax.dynamic_index_in_dim(w_out, t, 1, False))
    own_tokens = lax.dynamic_slice_in_dim(tokens, t * columns, columns, 1)
    sent = message(mine, arrived, own_tokens, gain_one, bias_one)
    ours = exchanged(sent, ("z", "y"))
    other = flipped(ours, "tp", 1)
    at = jnp.stack([t, 4 * z + y])
    theirs, mine, normed_own = mixer(at, ours, other, choosers(32, columns), w_up, w_down)
    mlp = halved(mine, flipped(theirs, "tp", 1)).astype(bf16)
    mlp = exchanged(mlp, ("z", "y")).astype(f32).sum(axis=0)
    second = residual_scale * normed_own.astype(f32) + mlp
    total, squares = packed_total(
        (jnp.sum(second, axis=1), jnp.sum(second * second, axis=1)), ("z", "y", "tp")
    )
    result = finish_norm(second, total, squares, D, gain_two, bias_two).astype(bf16)
    return (result, new_state)


def solution(mesh):
    fine = Mesh(mesh.devices.reshape(4, 4, 4, 2), ("dp", "z", "y", "tp"))
    kv = ("z", "y")
    every = ("z", "y", "tp")
    placed = (
        P("dp", kv),
        P(("dp", "z", "y"), "tp", None, None),
        P(kv, "tp"),
        P(kv, "tp"),
        P(kv, "tp"),
        P(kv, "tp"),
        P("tp"),
        P(),
        P("tp", kv),
        P(every),
        P(every),
        P(None, every),
        P(every, None),
        P(every),
        P(every),
    )
    return jax.shard_map(
        per_device,
        mesh=fine,
        in_specs=placed,
        out_specs=(P("dp", every), P(("dp", "z", "y"), "tp", None, None)),
        check_vma=False,
    )
```

```python
import jax
import jax.numpy as jnp
from jax import lax
from jax.experimental import pallas as pl
from jax.experimental.pallas import tpu as pltpu
from jax.sharding import Mesh
from jax.sharding import PartitionSpec as P

D = 4096
epsilon = 0.1
residual_scale = 1.68
f32 = jnp.float32
bf16 = jnp.bfloat16


def dot(a, b):
    return jnp.dot(a, b, preferred_element_type=f32)


def flipped(value, axis, bits):
    return lax.ppermute(value, axis, [(i, i ^ bits) for i in range(lax.axis_size(axis))])


def exchanged(tiles, axis):
    return lax.all_to_all(tiles, axis, split_axis=0, concat_axis=0, tiled=True)


def of_all(value, axis):
    return exchanged(jnp.broadcast_to(value, (lax.axis_size(axis), *value.shape)), axis)


def relative(flip):
    return (0, 4 - flip, flip, 2)


def row_order(rows, outer, outer_flip, inner, inner_flip, outer_stride, inner_stride):
    own = rows // 16
    p = lax.broadcasted_iota(jnp.int32, (rows, rows), 0)
    c = lax.broadcasted_iota(jnp.int32, (rows, rows), 1)
    block = p // own

    def flip_of(i, flip):
        r = relative(flip)
        return jnp.where(i == 0, r[0], jnp.where(i == 1, r[1], jnp.where(i == 2, r[2], r[3])))

    o = jnp.bitwise_xor(outer, flip_of(block // 4, outer_flip))
    i = jnp.bitwise_xor(inner, flip_of(block % 4, inner_flip))
    source = (o * outer_stride + i * inner_stride) * own + p % own
    return (c == source).astype(bf16)


def halved(kept, received):
    return kept + received.astype(f32)


def project_kernel(tokens_ref, order_ref, weight_ref, sent_ref, kept_ref):
    rows = tokens_ref.shape[0]
    tokens = dot(order_ref[...], tokens_ref[...]).astype(bf16)
    sent_ref[...] = dot(tokens[rows // 2 :], weight_ref[...]).astype(bf16)
    kept_ref[...] = dot(tokens[: rows // 2], weight_ref[...])


def halve_kernel(kept_ref, arrived_ref, sent_ref, next_ref):
    rows = next_ref.shape[0]
    sent_ref[...] = halved(kept_ref[rows:], arrived_ref[rows:]).astype(bf16)
    next_ref[...] = halved(kept_ref[:rows], arrived_ref[:rows])


def to_halves(kernel, rows, width, name, *args):
    return pl.pallas_call(
        kernel,
        out_shape=(jax.ShapeDtypeStruct((rows, width), bf16), jax.ShapeDtypeStruct((rows, width), f32)),
        in_specs=in_vmem(len(args)),
        out_specs=tuple(in_vmem(2)),
        compiler_params=pltpu.CompilerParams(vmem_limit_bytes=4 << 20),
        cost_estimate=pl.CostEstimate(flops=rows << 16, bytes_accessed=rows << 14, transcendentals=0),
        name=name,
    )(*args)


def scattered_sum(tokens, order, weight, first, flip_first, second, flip_second):
    rows, width = tokens.shape[0], weight.shape[1]
    sent, kept = to_halves(project_kernel, rows // 2, width, "project", tokens, order, weight)
    steps = ((first, flip_first), (first, 4 - flip_first), (second, flip_second), (second, 4 - flip_second))
    for axis, flip in steps:
        arrived = flipped(sent, axis, flip)
        rows //= 2
        if rows > tokens.shape[0] // 16:
            sent, kept = to_halves(halve_kernel, rows // 2, width, "halve", kept, arrived)
    return halved(kept, arrived)


def packed_total(arrays, axis):
    line = jnp.stack(arrays)
    got = of_all(line[None], axis).sum(axis=0)[0]
    return got[0], got[1]


def finish_norm(values, total, squares, width, gain, bias):
    center = total[:, None] / width
    spread = squares[:, None] / width - center * center
    return (values - center) * lax.rsqrt(spread + epsilon) * gain + bias


def rounded(ref):
    return ref[...].astype(bf16).astype(f32)


def gates(forget_raw, bound):
    rest = 1.0 - bound
    return bound + rest * jax.nn.sigmoid(forget_raw), rest * jax.nn.sigmoid(-forget_raw)


def pieces(value):
    high = value.astype(bf16)
    rest = value - high.astype(f32)
    middle = rest.astype(bf16)
    return high, middle, (rest - middle.astype(f32)).astype(bf16)


def spread(stacked, chooser):
    return dot(stacked, chooser)


def choosers(rows, lanes):
    k = lax.broadcasted_iota(jnp.int32, (rows, rows * lanes), 0)
    n = lax.broadcasted_iota(jnp.int32, (rows, rows * lanes), 1)
    one = jnp.where(k == n // lanes, 1.0, 0.0).astype(bf16)
    return jnp.concatenate([one] * 3, axis=0)


def by_pairs(value, wide):
    return jnp.concatenate([value[:, at : at + wide] for at in range(0, value.shape[1], wide)], axis=0)


def read_kernel(q_ref, f_ref, bound_ref, choose_ref, state_hbm, reads_ref, stacked, state_ref, sems):
    slots, rows, _, size = state_ref.shape[:4]
    wide = 2 * size
    pairs = stacked.shape[0]

    def fetched(pair):
        slot = pair % slots
        return pltpu.make_async_copy(state_hbm.at[:, pl.ds(2 * pair, 2)], state_ref.at[slot], sems.at[slot])

    for pair in range(slots):
        fetched(pair).start()
    query = rounded(q_ref)
    forget, _ = gates(rounded(f_ref), bound_ref[...])
    scaled = jnp.concatenate(pieces(forget * query * jax.nn.sigmoid(query)), axis=0)
    for pair in range(pairs):
        stacked[pair] = jnp.transpose(scaled[:, pair * wide : (pair + 1) * wide])

    def body(pair, carry):
        fetched(pair).wait()
        slot = pair % slots
        for two in range(rows // 2):
            at = slice(2 * two * wide, 2 * (two + 1) * wide)
            columns = spread(stacked[pair], choose_ref[:, at])
            for b in range(2):
                folded = []
                for half in range(2):
                    column = columns[half * size : (half + 1) * size, b * wide : b * wide + size]
                    product = state_ref[slot, 2 * two + b, half] * column
                    folded.append(jnp.sum(product.reshape(size // 8, 8, size), axis=0))
                total = jnp.sum(jnp.concatenate(folded, axis=1), axis=0, keepdims=True)
                reads_ref[pair, 2 * two + b : 2 * two + b + 1, :] = total

        @pl.when(pair + slots < pairs)
        def _():
            fetched(pair + slots).start()

        return carry

    lax.fori_loop(0, pairs, body, 0)


def head_sums(value, size):
    wide = value.shape[1]
    a = lax.broadcasted_iota(jnp.int32, (wide, wide), 0) // size
    b = lax.broadcasted_iota(jnp.int32, (wide, wide), 1) // size
    ones = jnp.where(a == b, 1.0, 0.0).astype(bf16)
    return sum(dot(piece, ones) for piece in pieces(value))


def mix_kernel(q_ref, f_ref, v_ref, g_ref, bound_ref, gain_ref, reads_ref, mix_ref):
    pairs, rows, wide = reads_ref.shape
    query = rounded(q_ref)
    query = query * jax.nn.sigmoid(query)
    _, keyvec = gates(rounded(f_ref), bound_ref[...])
    gate = rounded(g_ref)
    gate = by_pairs(gate * jax.nn.sigmoid(gate), wide)
    agreement = head_sums(by_pairs(keyvec * query, wide), wide // 2)
    read = reads_ref[...].reshape(pairs * rows, wide) + agreement * by_pairs(rounded(v_ref), wide)
    power = head_sums(read * read, wide // 2) * (2.0 / wide)
    mix = (read * lax.rsqrt(power + epsilon) * gain_ref[...] * gate).astype(bf16)
    for pair in range(pairs):
        for i in range(mix_ref.shape[0]):
            mix_ref[i, :, pair * wide : (pair + 1) * wide] = mix[pair * rows : (pair + 1) * rows]


def state_kernel(
    f_ref, v_ref, bound_ref, choose_ref, state_ref, out_ref, forgets, keys, values, old, ready, old_sems, sems
):
    rows, heads, size = state_ref.shape[:3]
    wide = 2 * size
    pairs = heads // 2
    slots = ready.shape[0]

    def fetched(pair):
        slot = pair % slots
        return pltpu.make_async_copy(state_ref.at[:, pl.ds(2 * pair, 2)], old.at[slot], old_sems.at[slot])

    for slot in range(slots):
        fetched(slot).start()
    forget, keyvec = gates(rounded(f_ref), bound_ref[...])
    forget = jnp.concatenate(pieces(forget), axis=0)
    keyvec = jnp.concatenate(pieces(keyvec), axis=0)
    value = rounded(v_ref)
    for pair in range(heads // 2):
        own = slice(pair * wide, (pair + 1) * wide)
        forgets[pair] = jnp.transpose(forget[:, own])
        keys[pair] = jnp.transpose(keyvec[:, own])
    for head in range(heads):
        values[head] = value[:, head * size : (head + 1) * size]

    def copied(pair):
        slot = pair % slots
        return pltpu.make_async_copy(ready.at[slot], out_ref.at[:, pl.ds(2 * pair, 2)], sems.at[slot])

    def body(pair, carry):
        @pl.when(pair >= slots)
        def _():
            copied(pair - slots).wait()

        fetched(pair).wait()
        slot = pair % slots
        for two in range(rows // 2):
            at = slice(2 * two * wide, 2 * (two + 1) * wide)
            kept = spread(forgets[pair], choose_ref[:, at])
            added = spread(keys[pair], choose_ref[:, at])
            for half in range(2):
                for b in range(2):
                    part = (slice(half * size, (half + 1) * size), slice(b * wide, b * wide + size))
                    row = 2 * two + b
                    ready[slot, row, half] = (
                        kept[part] * old[slot, row, half]
                        + added[part] * values[2 * pair + half, row : row + 1, :]
                    )
        copied(pair).start()

        @pl.when(pair + slots < pairs)
        def _():
            fetched(pair + slots).start()

        return carry

    lax.fori_loop(0, pairs, body, 0)
    for slot in range(slots):
        copied(pairs - slots + slot).wait()


def message_kernel(mine_ref, arrived_ref, tokens_ref, gain_ref, bias_ref, out_ref):
    rows, size = mine_ref.shape
    first = residual_scale * tokens_ref[...].astype(f32) + (mine_ref[...] + arrived_ref[...])
    center = jnp.mean(first, axis=1, keepdims=True)
    first = first - center
    power = jnp.sum(first * first, axis=1, keepdims=True)
    lane = lax.broadcasted_iota(jnp.int32, (rows, size), 1)
    turned = jnp.where(lane == 0, center, jnp.where(lane == 1, power, 0.0))
    turned = [jnp.transpose(turned[r : r + size])[0:8] for r in range(0, rows, size)]
    centers = pieces(jnp.concatenate([v[0:1] for v in turned], axis=0))
    powers = pieces(jnp.concatenate([v[1:2] for v in turned], axis=0))
    tail = [p.astype(f32) for p in (*centers, *powers[:2], *pieces(gain_ref[...]), *pieces(bias_ref[...]))]
    tail = jnp.concatenate(tail, axis=0).astype(bf16)
    first = first.astype(bf16)
    for i in range(out_ref.shape[0]):
        out_ref[i, :rows] = first
        out_ref[i, rows:] = tail


def mlp_kernel(
    at_ref,
    ours_ref,
    other_ref,
    choose_ref,
    up_hbm,
    down_hbm,
    theirs_ref,
    mine_ref,
    own_ref,
    joined,
    shifts,
    up_ref,
    down_ref,
    sems,
):
    up_copy = pltpu.make_async_copy(up_hbm, up_ref, sems.at[0])
    down_copy = pltpu.make_async_copy(down_hbm, down_ref, sems.at[1])
    up_copy.start()
    t, kv = at_ref[0], at_ref[1]
    blocks, rows, size = ours_ref.shape
    rows -= 16
    tails = []
    for ref in (ours_ref, other_ref):
        for k in range(blocks):
            tails.append(ref[k, rows:].astype(f32))
    centers = [v[0:2] + v[2:4] + v[4:6] for v in tails]
    center = sum(centers) * (1.0 / len(centers))
    centers = [c - center for c in centers]
    power = sum(v[6:8] + v[8:10] for v in tails) + size * sum(c * c for c in centers)
    scale = lax.rsqrt(power * (1.0 / (size * len(tails))) + epsilon)
    wanted = [*(c * scale for c in centers)]
    lines = [jnp.concatenate([v[r : r + 1] for v in wanted], axis=0) for r in range(rows // size)]
    lines = jnp.concatenate(lines, axis=1)
    shifts[...] = jnp.transpose(jnp.concatenate(pieces(lines), axis=0))
    factor = jnp.concatenate(
        [jnp.transpose(jnp.broadcast_to(scale[r : r + 1], (size, size))) for r in range(rows // size)], axis=0
    )
    for side, ref in enumerate((ours_ref, other_ref)):
        if side == 1:
            down_copy.start()
        for k in range(blocks):
            block = side * blocks + k
            shift = spread(shifts[...], choose_ref[:, block * size : (block + 1) * size])
            v = tails[block]
            gain = v[10:11] + v[11:12] + v[12:13]
            bias = v[13:14] + v[14:15] + v[15:16]
            value = (ref[k, :rows].astype(f32) * factor + shift) * gain + bias
            to = 2 * k + (t if side == 0 else 1 - t)
            joined[:, pl.ds(pl.multiple_of(to * size, size), size)] = value.astype(bf16)
    own_ref[...] = joined[:, pl.ds(pl.multiple_of((2 * kv + t) * size, size), size)]
    up_copy.wait()
    upper = dot(joined[...], up_ref[...])
    hidden = jnp.square(jnp.maximum(upper, 0.0)).astype(bf16)
    down_copy.wait()
    for k in range(blocks):
        both = dot(hidden, down_ref[:, 2 * k * size : 2 * (k + 1) * size])
        left, right = both[:, :size], both[:, size:]
        theirs_ref[k] = jnp.where(t == 0, right, left).astype(bf16)
        mine_ref[k] = jnp.where(t == 0, left, right)


def in_hbm(value):
    return pltpu.with_memory_space_constraint(value, pltpu.HBM)


def in_vmem(n):
    return [pl.BlockSpec(memory_space=pltpu.VMEM)] * n


def in_hbm(value):
    return pltpu.with_memory_space_constraint(value, pltpu.HBM)


def head_reads(query, forget, bound, chooser, state):
    rows, heads, size = state.shape[:3]
    return pl.pallas_call(
        read_kernel,
        out_shape=jax.ShapeDtypeStruct((heads // 2, rows, 2 * size), f32),
        in_specs=[*in_vmem(4), pl.BlockSpec(memory_space=pltpu.HBM)],
        out_specs=in_vmem(1)[0],
        scratch_shapes=[
            pltpu.VMEM((heads // 2, 2 * size, 3 * rows), bf16),
            pltpu.VMEM((5, rows, 2, size, size), f32),
            pltpu.SemaphoreType.DMA((5,)),
        ],
        cost_estimate=pl.CostEstimate(flops=1 << 26, bytes_accessed=1 << 23, transcendentals=0),
        compiler_params=pltpu.CompilerParams(vmem_limit_bytes=9 << 20),
        name="heads_read",
    )(query, forget, bound[None], chooser, in_hbm(state))


def mixed_heads(query, forget, value, gate, bound, head_gain, reads):
    pairs, rows, wide = reads.shape
    return pl.pallas_call(
        mix_kernel,
        out_shape=jax.ShapeDtypeStruct((16, rows, pairs * wide), bf16),
        in_specs=in_vmem(7),
        out_specs=in_vmem(1)[0],
        compiler_params=pltpu.CompilerParams(vmem_limit_bytes=6 << 20),
        name="heads_mix",
    )(query, forget, value, gate, bound[None], jnp.tile(head_gain, 2)[None], reads)


def updated_state(forget, value, bound, chooser, state):
    rows, heads, size = state.shape[:3]
    slots = 4
    block = pltpu.VMEM((slots, rows, 2, size, size), f32)
    return pl.pallas_call(
        state_kernel,
        out_shape=jax.ShapeDtypeStruct(state.shape, f32),
        in_specs=[*in_vmem(4), pl.BlockSpec(memory_space=pltpu.HBM)],
        out_specs=pl.BlockSpec(memory_space=pltpu.HBM),
        scratch_shapes=[
            pltpu.VMEM((heads // 2, 2 * size, 3 * rows), bf16),
            pltpu.VMEM((heads // 2, 2 * size, 3 * rows), bf16),
            pltpu.VMEM((heads, rows, size), f32),
            block,
            block,
            pltpu.SemaphoreType.DMA((slots,)),
            pltpu.SemaphoreType.DMA((slots,)),
        ],
        cost_estimate=pl.CostEstimate(flops=1 << 27, bytes_accessed=1 << 25, transcendentals=0),
        compiler_params=pltpu.CompilerParams(vmem_limit_bytes=16 << 20),
        name="state_update",
    )(forget, value, bound[None], chooser, in_hbm(state))


def message(mine, arrived, own_tokens, gain, bias):
    rows, size = mine.shape
    return pl.pallas_call(
        message_kernel,
        out_shape=jax.ShapeDtypeStruct((16, rows + 16, size), bf16),
        in_specs=in_vmem(5),
        out_specs=in_vmem(1)[0],
        compiler_params=pltpu.CompilerParams(vmem_limit_bytes=4 << 20),
        name="first_message",
    )(mine, arrived, own_tokens, gain[None], bias[None])


def mixer(at, ours, other, chooser, w_up, w_down):
    blocks, rows, size = ours.shape
    rows -= 16
    shape = (blocks, rows, size)
    return pl.pallas_call(
        mlp_kernel,
        out_shape=(
            jax.ShapeDtypeStruct(shape, bf16),
            jax.ShapeDtypeStruct(shape, f32),
            jax.ShapeDtypeStruct((rows, size), bf16),
        ),
        in_specs=[
            pl.BlockSpec(memory_space=pltpu.SMEM),
            *in_vmem(3),
            *[pl.BlockSpec(memory_space=pltpu.HBM)] * 2,
        ],
        out_specs=tuple(in_vmem(3)),
        scratch_shapes=[
            pltpu.VMEM((rows, 2 * blocks * size), bf16),
            pltpu.VMEM((rows, 6 * blocks), bf16),
            pltpu.VMEM(w_up.shape, bf16),
            pltpu.VMEM(w_down.shape, bf16),
            pltpu.SemaphoreType.DMA((2,)),
        ],
        cost_estimate=pl.CostEstimate(flops=1 << 31, bytes_accessed=1 << 23, transcendentals=0),
        compiler_params=pltpu.CompilerParams(vmem_limit_bytes=28 << 20),
        name="channel_mixer",
    )(at, ours, other, chooser, in_hbm(w_up), in_hbm(w_down))


def per_device(
    tokens,
    state,
    w_query,
    w_forget,
    w_input,
    w_gate,
    lower_bound,
    head_gain,
    w_out,
    gain_one,
    bias_one,
    w_up,
    w_down,
    gain_two,
    bias_two,
):
    z, y, t = lax.axis_index("z"), lax.axis_index("y"), lax.axis_index("tp")
    rows = tokens.shape[0]
    rows_own = rows // 16
    width = w_query.shape[1]

    streams = []
    for weight, z_first, flip in (
        (w_query, True, 1),
        (w_forget, True, 3),
        (w_input, False, 1),
        (w_gate, False, 3),
    ):
        if z_first:
            order = row_order(rows, z, flip, y, flip, 4, 1)
            axes = ("z", flip, "y", flip)
        else:
            order = row_order(rows, y, flip, z, flip, 1, 4)
            axes = ("y", flip, "z", flip)
        streams.append(scattered_sum(tokens, order, weight, *axes))
    query_raw, forget_raw, value_raw, gate_raw = streams
    chooser = choosers(rows_own, 2 * head_gain.shape[0])
    reads = head_reads(query_raw, forget_raw, lower_bound, chooser, state)
    mixout = mixed_heads(query_raw, forget_raw, value_raw, gate_raw, lower_bound, head_gain, reads)
    new_state = updated_state(forget_raw, value_raw, lower_bound, chooser, state)

    mixout = exchanged(mixout, ("z", "y")).reshape(rows, width)
    mixout, new_state = lax.optimization_barrier((mixout, new_state))
    columns = w_out.shape[1] // 2
    w_out = w_out.reshape(width, 2, columns)
    theirs = dot(mixout, lax.dynamic_index_in_dim(w_out, 1 - t, 1, False))
    arrived = flipped(theirs, "tp", 1)
    mine = dot(mixout, lax.dynamic_index_in_dim(w_out, t, 1, False))
    own_tokens = lax.dynamic_slice_in_dim(tokens, t * columns, columns, 1)
    sent = message(mine, arrived, own_tokens, gain_one, bias_one)
    ours = exchanged(sent, ("z", "y"))
    other = flipped(ours, "tp", 1)
    at = jnp.stack([t, 4 * z + y])
    theirs, mine, normed_own = mixer(at, ours, other, choosers(32, columns), w_up, w_down)
    mlp = halved(mine, flipped(theirs, "tp", 1)).astype(bf16)
    mlp = exchanged(mlp, ("z", "y")).astype(f32).sum(axis=0)
    second = residual_scale * normed_own.astype(f32) + mlp
    total, squares = packed_total(
        (jnp.sum(second, axis=1), jnp.sum(second * second, axis=1)), ("z", "y", "tp")
    )
    result = finish_norm(second, total, squares, D, gain_two, bias_two).astype(bf16)
    return (result, new_state)


def solution(mesh):
    fine = Mesh(mesh.devices.reshape(4, 4, 4, 2), ("dp", "z", "y", "tp"))
    kv = ("z", "y")
    every = ("z", "y", "tp")
    placed = (
        P("dp", kv),
        P(("dp", "z", "y"), "tp", None, None),
        P(kv, "tp"),
        P(kv, "tp"),
        P(kv, "tp"),
        P(kv, "tp"),
        P("tp"),
        P(),
        P("tp", kv),
        P(every),
        P(every),
        P(None, every),
        P(every, None),
        P(every),
        P(every),
    )
    return jax.shard_map(
        per_device,
        mesh=fine,
        in_specs=placed,
        out_specs=(P("dp", every), P(("dp", "z", "y"), "tp", None, None)),
        check_vma=False,
    )
```

```python
import jax
import jax.numpy as jnp
from jax import lax
from jax.experimental import pallas as pl
from jax.experimental.pallas import tpu as pltpu
from jax.sharding import Mesh
from jax.sharding import PartitionSpec as P

D = 4096
epsilon = 0.1
residual_scale = 1.68
f32 = jnp.float32
bf16 = jnp.bfloat16


def dot(a, b):
    return jnp.dot(a, b, preferred_element_type=f32)


def flipped(value, axis, bits):
    return lax.ppermute(value, axis, [(i, i ^ bits) for i in range(lax.axis_size(axis))])


def exchanged(tiles, axis):
    return lax.all_to_all(tiles, axis, split_axis=0, concat_axis=0, tiled=True)


def of_all(value, axis):
    return exchanged(jnp.broadcast_to(value, (lax.axis_size(axis), *value.shape)), axis)


def relative(flip):
    return (0, 4 - flip, flip, 2)


def row_order(rows, outer, outer_flip, inner, inner_flip, outer_stride, inner_stride):
    own = rows // 16
    p = lax.broadcasted_iota(jnp.int32, (rows, rows), 0)
    c = lax.broadcasted_iota(jnp.int32, (rows, rows), 1)
    block = p // own

    def flip_of(i, flip):
        r = relative(flip)
        return jnp.where(i == 0, r[0], jnp.where(i == 1, r[1], jnp.where(i == 2, r[2], r[3])))

    o = jnp.bitwise_xor(outer, flip_of(block // 4, outer_flip))
    i = jnp.bitwise_xor(inner, flip_of(block % 4, inner_flip))
    source = (o * outer_stride + i * inner_stride) * own + p % own
    return (c == source).astype(bf16)


def halved(kept, received):
    return kept + received.astype(f32)


def project_kernel(tokens_ref, order_ref, weight_ref, sent_ref, kept_ref):
    rows = tokens_ref.shape[0]
    tokens = dot(order_ref[...], tokens_ref[...]).astype(bf16)
    sent_ref[...] = dot(tokens[rows // 2 :], weight_ref[...]).astype(bf16)
    kept_ref[...] = dot(tokens[: rows // 2], weight_ref[...])


def halve_kernel(kept_ref, arrived_ref, sent_ref, next_ref):
    rows = next_ref.shape[0]
    sent_ref[...] = halved(kept_ref[rows:], arrived_ref[rows:]).astype(bf16)
    next_ref[...] = halved(kept_ref[:rows], arrived_ref[:rows])


def to_halves(kernel, rows, width, name, *args):
    return pl.pallas_call(
        kernel,
        out_shape=(jax.ShapeDtypeStruct((rows, width), bf16), jax.ShapeDtypeStruct((rows, width), f32)),
        in_specs=in_vmem(len(args)),
        out_specs=tuple(in_vmem(2)),
        compiler_params=pltpu.CompilerParams(vmem_limit_bytes=4 << 20),
        cost_estimate=pl.CostEstimate(flops=rows << 16, bytes_accessed=rows << 14, transcendentals=0),
        name=name,
    )(*args)


def scattered_sum(tokens, order, weight, first, flip_first, second, flip_second):
    rows, width = tokens.shape[0], weight.shape[1]
    sent, kept = to_halves(project_kernel, rows // 2, width, "project", tokens, order, weight)
    opened = sent
    steps = ((first, flip_first), (first, 4 - flip_first), (second, flip_second), (second, 4 - flip_second))
    for axis, flip in steps:
        arrived = flipped(sent, axis, flip)
        rows //= 2
        if rows > tokens.shape[0] // 16:
            sent, kept = to_halves(halve_kernel, rows // 2, width, "halve", kept, arrived)
    return (kept, arrived), opened


def packed_total(arrays, axis):
    line = jnp.stack(arrays)
    got = of_all(line[None], axis).sum(axis=0)[0]
    return got[0], got[1]


def finish_norm(values, total, squares, width, gain, bias):
    center = total[:, None] / width
    spread = squares[:, None] / width - center * center
    return (values - center) * lax.rsqrt(spread + epsilon) * gain + bias


def rounded(kept_ref, arrived_ref):
    return halved(kept_ref[...], arrived_ref[...]).astype(bf16).astype(f32)


def gates(forget_raw, bound):
    rest = 1.0 - bound
    return bound + rest * jax.nn.sigmoid(forget_raw), rest * jax.nn.sigmoid(-forget_raw)


def pieces(value):
    high = value.astype(bf16)
    rest = value - high.astype(f32)
    middle = rest.astype(bf16)
    return high, middle, (rest - middle.astype(f32)).astype(bf16)


def spread(stacked, chooser):
    return dot(stacked, chooser)


def choosers(rows, lanes):
    k = lax.broadcasted_iota(jnp.int32, (rows, rows * lanes), 0)
    n = lax.broadcasted_iota(jnp.int32, (rows, rows * lanes), 1)
    one = jnp.where(k == n // lanes, 1.0, 0.0).astype(bf16)
    return jnp.concatenate([one] * 3, axis=0)


def by_pairs(value, wide):
    return jnp.concatenate([value[:, at : at + wide] for at in range(0, value.shape[1], wide)], axis=0)


def read_kernel(q_kept, q_ref, f_kept, f_ref, bound_ref, choose_ref, state_hbm, reads_ref, stacked, state_ref, sems):
    slots, rows, _, size = state_ref.shape[:4]
    wide = 2 * size
    pairs = stacked.shape[0]

    def fetched(pair):
        slot = pair % slots
        return pltpu.make_async_copy(state_hbm.at[:, pl.ds(2 * pair, 2)], state_ref.at[slot], sems.at[slot])

    for pair in range(slots):
        fetched(pair).start()
    query = rounded(q_kept, q_ref)
    forget, _ = gates(rounded(f_kept, f_ref), bound_ref[...])
    scaled = jnp.concatenate(pieces(forget * query * jax.nn.sigmoid(query)), axis=0)
    for pair in range(pairs):
        stacked[pair] = jnp.transpose(scaled[:, pair * wide : (pair + 1) * wide])

    def body(pair, carry):
        fetched(pair).wait()
        slot = pair % slots
        for two in range(rows // 2):
            at = slice(2 * two * wide, 2 * (two + 1) * wide)
            columns = spread(stacked[pair], choose_ref[:, at])
            for b in range(2):
                folded = []
                for half in range(2):
                    column = columns[half * size : (half + 1) * size, b * wide : b * wide + size]
                    product = state_ref[slot, 2 * two + b, half] * column
                    folded.append(jnp.sum(product.reshape(size // 8, 8, size), axis=0))
                total = jnp.sum(jnp.concatenate(folded, axis=1), axis=0, keepdims=True)
                reads_ref[pair, 2 * two + b : 2 * two + b + 1, :] = total

        @pl.when(pair + slots < pairs)
        def _():
            fetched(pair + slots).start()

        return carry

    lax.fori_loop(0, pairs, body, 0)


def head_sums(value, size):
    wide = value.shape[1]
    a = lax.broadcasted_iota(jnp.int32, (wide, wide), 0) // size
    b = lax.broadcasted_iota(jnp.int32, (wide, wide), 1) // size
    ones = jnp.where(a == b, 1.0, 0.0).astype(bf16)
    return sum(dot(piece, ones) for piece in pieces(value))


def mix_kernel(
    q_kept, q_ref, f_kept, f_ref, v_kept, v_ref, g_kept, g_ref, bound_ref, gain_ref, reads_ref, mix_ref
):
    pairs, rows, wide = reads_ref.shape
    query = rounded(q_kept, q_ref)
    query = query * jax.nn.sigmoid(query)
    _, keyvec = gates(rounded(f_kept, f_ref), bound_ref[...])
    gate = rounded(g_kept, g_ref)
    gate = by_pairs(gate * jax.nn.sigmoid(gate), wide)
    agreement = head_sums(by_pairs(keyvec * query, wide), wide // 2)
    read = reads_ref[...].reshape(pairs * rows, wide) + agreement * by_pairs(rounded(v_kept, v_ref), wide)
    power = head_sums(read * read, wide // 2) * (2.0 / wide)
    mix = (read * lax.rsqrt(power + epsilon) * gain_ref[...] * gate).astype(bf16)
    for pair in range(pairs):
        for i in range(mix_ref.shape[0]):
            mix_ref[i, :, pair * wide : (pair + 1) * wide] = mix[pair * rows : (pair + 1) * rows]


def state_kernel(
    f_kept,
    f_ref,
    v_kept,
    v_ref,
    bound_ref,
    choose_ref,
    state_ref,
    out_ref,
    forgets,
    keys,
    values,
    old,
    ready,
    old_sems,
    sems,
):
    rows, heads, size = state_ref.shape[:3]
    wide = 2 * size
    pairs = heads // 2
    slots = ready.shape[0]

    def fetched(pair):
        slot = pair % slots
        return pltpu.make_async_copy(state_ref.at[:, pl.ds(2 * pair, 2)], old.at[slot], old_sems.at[slot])

    for slot in range(slots):
        fetched(slot).start()
    forget, keyvec = gates(rounded(f_kept, f_ref), bound_ref[...])
    forget = jnp.concatenate(pieces(forget), axis=0)
    keyvec = jnp.concatenate(pieces(keyvec), axis=0)
    value = rounded(v_kept, v_ref)
    for pair in range(heads // 2):
        own = slice(pair * wide, (pair + 1) * wide)
        forgets[pair] = jnp.transpose(forget[:, own])
        keys[pair] = jnp.transpose(keyvec[:, own])
    for head in range(heads):
        values[head] = value[:, head * size : (head + 1) * size]

    def copied(pair):
        slot = pair % slots
        return pltpu.make_async_copy(ready.at[slot], out_ref.at[:, pl.ds(2 * pair, 2)], sems.at[slot])

    def body(pair, carry):
        @pl.when(pair >= slots)
        def _():
            copied(pair - slots).wait()

        fetched(pair).wait()
        slot = pair % slots
        for two in range(rows // 2):
            at = slice(2 * two * wide, 2 * (two + 1) * wide)
            kept = spread(forgets[pair], choose_ref[:, at])
            added = spread(keys[pair], choose_ref[:, at])
            for half in range(2):
                for b in range(2):
                    part = (slice(half * size, (half + 1) * size), slice(b * wide, b * wide + size))
                    row = 2 * two + b
                    ready[slot, row, half] = (
                        kept[part] * old[slot, row, half]
                        + added[part] * values[2 * pair + half, row : row + 1, :]
                    )
        copied(pair).start()

        @pl.when(pair + slots < pairs)
        def _():
            fetched(pair + slots).start()

        return carry

    lax.fori_loop(0, pairs, body, 0)
    for slot in range(slots):
        copied(pairs - slots + slot).wait()


def message_kernel(mine_ref, arrived_ref, tokens_ref, gain_ref, bias_ref, out_ref):
    rows, size = mine_ref.shape
    first = residual_scale * tokens_ref[...].astype(f32) + (mine_ref[...] + arrived_ref[...])
    center = jnp.mean(first, axis=1, keepdims=True)
    first = first - center
    power = jnp.sum(first * first, axis=1, keepdims=True)
    lane = lax.broadcasted_iota(jnp.int32, (rows, size), 1)
    turned = jnp.where(lane == 0, center, jnp.where(lane == 1, power, 0.0))
    turned = [jnp.transpose(turned[r : r + size])[0:8] for r in range(0, rows, size)]
    centers = pieces(jnp.concatenate([v[0:1] for v in turned], axis=0))
    powers = pieces(jnp.concatenate([v[1:2] for v in turned], axis=0))
    tail = [p.astype(f32) for p in (*centers, *powers[:2], *pieces(gain_ref[...]), *pieces(bias_ref[...]))]
    tail = jnp.concatenate(tail, axis=0).astype(bf16)
    first = first.astype(bf16)
    for i in range(out_ref.shape[0]):
        out_ref[i, :rows] = first
        out_ref[i, rows:] = tail


def mlp_kernel(
    at_ref,
    ours_ref,
    other_ref,
    choose_ref,
    up_hbm,
    down_hbm,
    theirs_ref,
    mine_ref,
    own_ref,
    joined,
    shifts,
    up_ref,
    down_ref,
    sems,
):
    up_copy = pltpu.make_async_copy(up_hbm, up_ref, sems.at[0])
    down_copy = pltpu.make_async_copy(down_hbm, down_ref, sems.at[1])
    up_copy.start()
    t, kv = at_ref[0], at_ref[1]
    blocks, rows, size = ours_ref.shape
    rows -= 16
    tails = []
    for ref in (ours_ref, other_ref):
        for k in range(blocks):
            tails.append(ref[k, rows:].astype(f32))
    centers = [v[0:2] + v[2:4] + v[4:6] for v in tails]
    center = sum(centers) * (1.0 / len(centers))
    centers = [c - center for c in centers]
    power = sum(v[6:8] + v[8:10] for v in tails) + size * sum(c * c for c in centers)
    scale = lax.rsqrt(power * (1.0 / (size * len(tails))) + epsilon)
    wanted = [*(c * scale for c in centers)]
    lines = [jnp.concatenate([v[r : r + 1] for v in wanted], axis=0) for r in range(rows // size)]
    lines = jnp.concatenate(lines, axis=1)
    shifts[...] = jnp.transpose(jnp.concatenate(pieces(lines), axis=0))
    factor = jnp.concatenate(
        [jnp.transpose(jnp.broadcast_to(scale[r : r + 1], (size, size))) for r in range(rows // size)], axis=0
    )
    for side, ref in enumerate((ours_ref, other_ref)):
        if side == 1:
            down_copy.start()
        for k in range(blocks):
            block = side * blocks + k
            shift = spread(shifts[...], choose_ref[:, block * size : (block + 1) * size])
            v = tails[block]
            gain = v[10:11] + v[11:12] + v[12:13]
            bias = v[13:14] + v[14:15] + v[15:16]
            value = (ref[k, :rows].astype(f32) * factor + shift) * gain + bias
            to = 2 * k + (t if side == 0 else 1 - t)
            joined[:, pl.ds(pl.multiple_of(to * size, size), size)] = value.astype(bf16)
    own_ref[...] = joined[:, pl.ds(pl.multiple_of((2 * kv + t) * size, size), size)]
    up_copy.wait()
    upper = dot(joined[...], up_ref[...])
    hidden = jnp.square(jnp.maximum(upper, 0.0)).astype(bf16)
    down_copy.wait()
    for k in range(blocks):
        both = dot(hidden, down_ref[:, 2 * k * size : 2 * (k + 1) * size])
        left, right = both[:, :size], both[:, size:]
        theirs_ref[k] = jnp.where(t == 0, right, left).astype(bf16)
        mine_ref[k] = jnp.where(t == 0, left, right)


def in_hbm(value):
    return pltpu.with_memory_space_constraint(value, pltpu.HBM)


def in_vmem(n):
    return [pl.BlockSpec(memory_space=pltpu.VMEM)] * n


def in_hbm(value):
    return pltpu.with_memory_space_constraint(value, pltpu.HBM)


def head_reads(query, forget, bound, chooser, state):
    rows, heads, size = state.shape[:3]
    return pl.pallas_call(
        read_kernel,
        out_shape=jax.ShapeDtypeStruct((heads // 2, rows, 2 * size), f32),
        in_specs=[*in_vmem(6), pl.BlockSpec(memory_space=pltpu.HBM)],
        out_specs=in_vmem(1)[0],
        scratch_shapes=[
            pltpu.VMEM((heads // 2, 2 * size, 3 * rows), bf16),
            pltpu.VMEM((5, rows, 2, size, size), f32),
            pltpu.SemaphoreType.DMA((5,)),
        ],
        cost_estimate=pl.CostEstimate(flops=1 << 26, bytes_accessed=1 << 23, transcendentals=0),
        compiler_params=pltpu.CompilerParams(vmem_limit_bytes=9 << 20),
        name="heads_read",
    )(*query, *forget, bound[None], chooser, in_hbm(state))


def mixed_heads(query, forget, value, gate, bound, head_gain, reads):
    pairs, rows, wide = reads.shape
    return pl.pallas_call(
        mix_kernel,
        out_shape=jax.ShapeDtypeStruct((16, rows, pairs * wide), bf16),
        in_specs=in_vmem(11),
        out_specs=in_vmem(1)[0],
        compiler_params=pltpu.CompilerParams(vmem_limit_bytes=6 << 20),
        name="heads_mix",
    )(*query, *forget, *value, *gate, bound[None], jnp.tile(head_gain, 2)[None], reads)


def updated_state(forget, value, bound, chooser, state):
    rows, heads, size = state.shape[:3]
    slots = 4
    block = pltpu.VMEM((slots, rows, 2, size, size), f32)
    return pl.pallas_call(
        state_kernel,
        out_shape=jax.ShapeDtypeStruct(state.shape, f32),
        in_specs=[*in_vmem(6), pl.BlockSpec(memory_space=pltpu.HBM)],
        out_specs=pl.BlockSpec(memory_space=pltpu.HBM),
        scratch_shapes=[
            pltpu.VMEM((heads // 2, 2 * size, 3 * rows), bf16),
            pltpu.VMEM((heads // 2, 2 * size, 3 * rows), bf16),
            pltpu.VMEM((heads, rows, size), f32),
            block,
            block,
            pltpu.SemaphoreType.DMA((slots,)),
            pltpu.SemaphoreType.DMA((slots,)),
        ],
        cost_estimate=pl.CostEstimate(flops=1 << 27, bytes_accessed=1 << 25, transcendentals=0),
        compiler_params=pltpu.CompilerParams(vmem_limit_bytes=16 << 20),
        name="state_update",
    )(*forget, *value, bound[None], chooser, in_hbm(state))


def message(mine, arrived, own_tokens, gain, bias):
    rows, size = mine.shape
    return pl.pallas_call(
        message_kernel,
        out_shape=jax.ShapeDtypeStruct((16, rows + 16, size), bf16),
        in_specs=in_vmem(5),
        out_specs=in_vmem(1)[0],
        compiler_params=pltpu.CompilerParams(vmem_limit_bytes=4 << 20),
        name="first_message",
    )(mine, arrived, own_tokens, gain[None], bias[None])


def mixer(at, ours, other, chooser, w_up, w_down):
    blocks, rows, size = ours.shape
    rows -= 16
    shape = (blocks, rows, size)
    return pl.pallas_call(
        mlp_kernel,
        out_shape=(
            jax.ShapeDtypeStruct(shape, bf16),
            jax.ShapeDtypeStruct(shape, f32),
            jax.ShapeDtypeStruct((rows, size), bf16),
        ),
        in_specs=[
            pl.BlockSpec(memory_space=pltpu.SMEM),
            *in_vmem(3),
            *[pl.BlockSpec(memory_space=pltpu.HBM)] * 2,
        ],
        out_specs=tuple(in_vmem(3)),
        scratch_shapes=[
            pltpu.VMEM((rows, 2 * blocks * size), bf16),
            pltpu.VMEM((rows, 6 * blocks), bf16),
            pltpu.VMEM(w_up.shape, bf16),
            pltpu.VMEM(w_down.shape, bf16),
            pltpu.SemaphoreType.DMA((2,)),
        ],
        cost_estimate=pl.CostEstimate(flops=1 << 31, bytes_accessed=1 << 23, transcendentals=0),
        compiler_params=pltpu.CompilerParams(vmem_limit_bytes=28 << 20),
        name="channel_mixer",
    )(at, ours, other, chooser, in_hbm(w_up), in_hbm(w_down))


def per_device(
    tokens,
    state,
    w_query,
    w_forget,
    w_input,
    w_gate,
    lower_bound,
    head_gain,
    w_out,
    gain_one,
    bias_one,
    w_up,
    w_down,
    gain_two,
    bias_two,
):
    z, y, t = lax.axis_index("z"), lax.axis_index("y"), lax.axis_index("tp")
    rows = tokens.shape[0]
    rows_own = rows // 16
    width = w_query.shape[1]

    streams = []
    tokens_next = tokens
    for weight, z_first, flip in (
        (w_query, True, 1),
        (w_forget, True, 3),
        (w_input, False, 1),
        (w_gate, False, 3),
    ):
        if z_first:
            order = row_order(rows, z, flip, y, flip, 4, 1)
            axes = ("z", flip, "y", flip)
        else:
            order = row_order(rows, y, flip, z, flip, 1, 4)
            axes = ("y", flip, "z", flip)
        total, opened = scattered_sum(tokens_next, order, weight, *axes)
        streams.append(total)
        tokens_next, _ = lax.optimization_barrier((tokens_next, opened))
    query_raw, forget_raw, value_raw, gate_raw = streams
    chooser = choosers(rows_own, 2 * head_gain.shape[0])
    reads = head_reads(query_raw, forget_raw, lower_bound, chooser, state)
    mixout = mixed_heads(query_raw, forget_raw, value_raw, gate_raw, lower_bound, head_gain, reads)
    new_state = updated_state(forget_raw, value_raw, lower_bound, chooser, state)

    mixout = exchanged(mixout, ("z", "y")).reshape(rows, width)
    mixout, new_state = lax.optimization_barrier((mixout, new_state))
    columns = w_out.shape[1] // 2
    w_out = w_out.reshape(width, 2, columns)
    theirs = dot(mixout, lax.dynamic_index_in_dim(w_out, 1 - t, 1, False))
    arrived = flipped(theirs, "tp", 1)
    mine = dot(mixout, lax.dynamic_index_in_dim(w_out, t, 1, False))
    own_tokens = lax.dynamic_slice_in_dim(tokens, t * columns, columns, 1)
    sent = message(mine, arrived, own_tokens, gain_one, bias_one)
    at = jnp.stack([t, 4 * z + y])
    sent, at, wide_chooser = lax.optimization_barrier((sent, at, choosers(32, columns)))
    ours = exchanged(sent, ("z", "y"))
    other = flipped(ours, "tp", 1)
    theirs, mine, normed_own = mixer(at, ours, other, wide_chooser, w_up, w_down)
    mlp = halved(mine, flipped(theirs, "tp", 1)).astype(bf16)
    mlp = exchanged(mlp, ("z", "y")).astype(f32).sum(axis=0)
    second = residual_scale * normed_own.astype(f32) + mlp
    total, squares = packed_total(
        (jnp.sum(second, axis=1), jnp.sum(second * second, axis=1)), ("z", "y", "tp")
    )
    result = finish_norm(second, total, squares, D, gain_two, bias_two).astype(bf16)
    return (result, new_state)


def solution(mesh):
    fine = Mesh(mesh.devices.reshape(4, 4, 4, 2), ("dp", "z", "y", "tp"))
    kv = ("z", "y")
    every = ("z", "y", "tp")
    placed = (
        P("dp", kv),
        P(("dp", "z", "y"), "tp", None, None),
        P(kv, "tp"),
        P(kv, "tp"),
        P(kv, "tp"),
        P(kv, "tp"),
        P("tp"),
        P(),
        P("tp", kv),
        P(every),
        P(every),
        P(None, every),
        P(every, None),
        P(every),
        P(every),
    )
    return jax.shard_map(
        per_device,
        mesh=fine,
        in_specs=placed,
        out_specs=(P("dp", every), P(("dp", "z", "y"), "tp", None, None)),
        check_vma=False,
    )
```

```python
import jax
import jax.numpy as jnp
from jax import lax
from jax.experimental import pallas as pl
from jax.experimental.pallas import tpu as pltpu
from jax.sharding import Mesh
from jax.sharding import PartitionSpec as P

D = 4096
epsilon = 0.1
residual_scale = 1.68
f32 = jnp.float32
bf16 = jnp.bfloat16


def dot(a, b):
    return jnp.dot(a, b, preferred_element_type=f32)


def flipped(value, axis, bits):
    return lax.ppermute(value, axis, [(i, i ^ bits) for i in range(lax.axis_size(axis))])


def exchanged(tiles, axis):
    return lax.all_to_all(tiles, axis, split_axis=0, concat_axis=0, tiled=True)


def of_all(value, axis):
    return exchanged(jnp.broadcast_to(value, (lax.axis_size(axis), *value.shape)), axis)


def relative(flip):
    return (0, 4 - flip, flip, 2)


def row_order(rows, outer, outer_flip, inner, inner_flip, outer_stride, inner_stride):
    own = rows // 16
    p = lax.broadcasted_iota(jnp.int32, (rows, rows), 0)
    c = lax.broadcasted_iota(jnp.int32, (rows, rows), 1)
    block = p // own

    def flip_of(i, flip):
        r = relative(flip)
        return jnp.where(i == 0, r[0], jnp.where(i == 1, r[1], jnp.where(i == 2, r[2], r[3])))

    o = jnp.bitwise_xor(outer, flip_of(block // 4, outer_flip))
    i = jnp.bitwise_xor(inner, flip_of(block % 4, inner_flip))
    source = (o * outer_stride + i * inner_stride) * own + p % own
    return (c == source).astype(bf16)


def halved(kept, received):
    return kept + received.astype(f32)


def project_kernel(tokens_ref, order_ref, weight_ref, sent_ref, kept_ref):
    rows = tokens_ref.shape[0]
    tokens = dot(order_ref[...], tokens_ref[...]).astype(bf16)
    sent_ref[...] = dot(tokens[rows // 2 :], weight_ref[...]).astype(bf16)
    kept_ref[...] = dot(tokens[: rows // 2], weight_ref[...])


def halve_kernel(kept_ref, arrived_ref, sent_ref, next_ref):
    rows = next_ref.shape[0]
    sent_ref[...] = halved(kept_ref[rows:], arrived_ref[rows:]).astype(bf16)
    next_ref[...] = halved(kept_ref[:rows], arrived_ref[:rows])


def to_halves(kernel, rows, width, name, *args):
    return pl.pallas_call(
        kernel,
        out_shape=(jax.ShapeDtypeStruct((rows, width), bf16), jax.ShapeDtypeStruct((rows, width), f32)),
        in_specs=in_vmem(len(args)),
        out_specs=tuple(in_vmem(2)),
        compiler_params=pltpu.CompilerParams(vmem_limit_bytes=4 << 20),
        cost_estimate=pl.CostEstimate(flops=rows << 16, bytes_accessed=rows << 14, transcendentals=0),
        name=name,
    )(*args)


def scattered_sum(tokens, order, weight, first, flip_first, second, flip_second):
    rows, width = tokens.shape[0], weight.shape[1]
    sent, kept = to_halves(project_kernel, rows // 2, width, "project", tokens, order, weight)
    opened = sent
    steps = ((first, flip_first), (first, 4 - flip_first), (second, flip_second), (second, 4 - flip_second))
    for axis, flip in steps:
        arrived = flipped(sent, axis, flip)
        rows //= 2
        if rows > tokens.shape[0] // 16:
            sent, kept = to_halves(halve_kernel, rows // 2, width, "halve", kept, arrived)
    return (kept, arrived), opened


def packed_total(arrays, axis):
    line = jnp.stack(arrays)
    got = of_all(line[None], axis).sum(axis=0)[0]
    return got[0], got[1]


def finish_norm(values, total, squares, width, gain, bias):
    center = total[:, None] / width
    spread = squares[:, None] / width - center * center
    return (values - center) * lax.rsqrt(spread + epsilon) * gain + bias


def rounded(kept_ref, arrived_ref):
    return halved(kept_ref[...], arrived_ref[...]).astype(bf16).astype(f32)


def gates(forget_raw, bound):
    rest = 1.0 - bound
    return bound + rest * jax.nn.sigmoid(forget_raw), rest * jax.nn.sigmoid(-forget_raw)


def pieces(value):
    high = value.astype(bf16)
    rest = value - high.astype(f32)
    middle = rest.astype(bf16)
    return high, middle, (rest - middle.astype(f32)).astype(bf16)


def spread(stacked, chooser):
    return dot(stacked, chooser)


def choosers(rows, lanes):
    k = lax.broadcasted_iota(jnp.int32, (rows, rows * lanes), 0)
    n = lax.broadcasted_iota(jnp.int32, (rows, rows * lanes), 1)
    one = jnp.where(k == n // lanes, 1.0, 0.0).astype(bf16)
    return jnp.concatenate([one] * 3, axis=0)


def by_pairs(value, wide):
    return jnp.concatenate([value[:, at : at + wide] for at in range(0, value.shape[1], wide)], axis=0)


def read_kernel(q_kept, q_ref, f_kept, f_ref, bound_ref, choose_ref, state_hbm, reads_ref, stacked, state_ref, sems):
    slots, rows, _, size = state_ref.shape[:4]
    wide = 2 * size
    pairs = stacked.shape[0]

    def fetched(pair):
        slot = pair % slots
        return pltpu.make_async_copy(state_hbm.at[:, pl.ds(2 * pair, 2)], state_ref.at[slot], sems.at[slot])

    for pair in range(slots):
        fetched(pair).start()
    query = rounded(q_kept, q_ref)
    forget, _ = gates(rounded(f_kept, f_ref), bound_ref[...])
    scaled = jnp.concatenate(pieces(forget * query * jax.nn.sigmoid(query)), axis=0)
    for pair in range(pairs):
        stacked[pair] = jnp.transpose(scaled[:, pair * wide : (pair + 1) * wide])

    def body(pair, carry):
        fetched(pair).wait()
        slot = pair % slots
        for two in range(rows // 2):
            at = slice(2 * two * wide, 2 * (two + 1) * wide)
            columns = spread(stacked[pair], choose_ref[:, at])
            for b in range(2):
                folded = []
                for half in range(2):
                    column = columns[half * size : (half + 1) * size, b * wide : b * wide + size]
                    product = state_ref[slot, 2 * two + b, half] * column
                    folded.append(jnp.sum(product.reshape(size // 8, 8, size), axis=0))
                total = jnp.sum(jnp.concatenate(folded, axis=1), axis=0, keepdims=True)
                reads_ref[pair, 2 * two + b : 2 * two + b + 1, :] = total

        @pl.when(pair + slots < pairs)
        def _():
            fetched(pair + slots).start()

        return carry

    lax.fori_loop(0, pairs, body, 0)


def head_sums(value, size):
    wide = value.shape[1]
    a = lax.broadcasted_iota(jnp.int32, (wide, wide), 0) // size
    b = lax.broadcasted_iota(jnp.int32, (wide, wide), 1) // size
    ones = jnp.where(a == b, 1.0, 0.0).astype(bf16)
    return sum(dot(piece, ones) for piece in pieces(value))


def mix_kernel(
    q_kept, q_ref, f_kept, f_ref, v_kept, v_ref, g_kept, g_ref, bound_ref, gain_ref, reads_ref, mix_ref
):
    pairs, rows, wide = reads_ref.shape
    query = rounded(q_kept, q_ref)
    query = query * jax.nn.sigmoid(query)
    _, keyvec = gates(rounded(f_kept, f_ref), bound_ref[...])
    gate = rounded(g_kept, g_ref)
    gate = by_pairs(gate * jax.nn.sigmoid(gate), wide)
    agreement = head_sums(by_pairs(keyvec * query, wide), wide // 2)
    read = reads_ref[...].reshape(pairs * rows, wide) + agreement * by_pairs(rounded(v_kept, v_ref), wide)
    power = head_sums(read * read, wide // 2) * (2.0 / wide)
    mix = (read * lax.rsqrt(power + epsilon) * gain_ref[...] * gate).astype(bf16)
    for pair in range(pairs):
        for i in range(mix_ref.shape[0]):
            mix_ref[i, :, pair * wide : (pair + 1) * wide] = mix[pair * rows : (pair + 1) * rows]


def state_kernel(
    f_kept,
    f_ref,
    v_kept,
    v_ref,
    bound_ref,
    choose_ref,
    state_ref,
    out_ref,
    forgets,
    keys,
    values,
    old,
    ready,
    old_sems,
    sems,
):
    rows, heads, size = state_ref.shape[:3]
    wide = 2 * size
    pairs = heads // 2
    slots = ready.shape[0]

    def fetched(pair):
        slot = pair % slots
        return pltpu.make_async_copy(state_ref.at[:, pl.ds(2 * pair, 2)], old.at[slot], old_sems.at[slot])

    for slot in range(slots):
        fetched(slot).start()
    forget, keyvec = gates(rounded(f_kept, f_ref), bound_ref[...])
    forget = jnp.concatenate(pieces(forget), axis=0)
    keyvec = jnp.concatenate(pieces(keyvec), axis=0)
    value = rounded(v_kept, v_ref)
    for pair in range(heads // 2):
        own = slice(pair * wide, (pair + 1) * wide)
        forgets[pair] = jnp.transpose(forget[:, own])
        keys[pair] = jnp.transpose(keyvec[:, own])
    for head in range(heads):
        values[head] = value[:, head * size : (head + 1) * size]

    def copied(pair):
        slot = pair % slots
        return pltpu.make_async_copy(ready.at[slot], out_ref.at[:, pl.ds(2 * pair, 2)], sems.at[slot])

    def body(pair, carry):
        @pl.when(pair >= slots)
        def _():
            copied(pair - slots).wait()

        fetched(pair).wait()
        slot = pair % slots
        for two in range(rows // 2):
            at = slice(2 * two * wide, 2 * (two + 1) * wide)
            kept = spread(forgets[pair], choose_ref[:, at])
            added = spread(keys[pair], choose_ref[:, at])
            for half in range(2):
                for b in range(2):
                    part = (slice(half * size, (half + 1) * size), slice(b * wide, b * wide + size))
                    row = 2 * two + b
                    ready[slot, row, half] = (
                        kept[part] * old[slot, row, half]
                        + added[part] * values[2 * pair + half, row : row + 1, :]
                    )
        copied(pair).start()

        @pl.when(pair + slots < pairs)
        def _():
            fetched(pair + slots).start()

        return carry

    lax.fori_loop(0, pairs, body, 0)
    for slot in range(slots):
        copied(pairs - slots + slot).wait()


def out_kernel(at_ref, mix_ref, weight_ref, theirs_ref, mine_ref):
    size = mine_ref.shape[1]
    both = dot(mix_ref[...], weight_ref[...])
    left, right = both[:, :size], both[:, size:]
    theirs_ref[...] = jnp.where(at_ref[0] == 0, right, left)
    mine_ref[...] = jnp.where(at_ref[0] == 0, left, right)


def message_kernel(mine_ref, arrived_ref, tokens_ref, gain_ref, bias_ref, out_ref):
    rows, size = mine_ref.shape
    first = residual_scale * tokens_ref[...].astype(f32) + (mine_ref[...] + arrived_ref[...])
    center = jnp.mean(first, axis=1, keepdims=True)
    first = first - center
    power = jnp.sum(first * first, axis=1, keepdims=True)
    lane = lax.broadcasted_iota(jnp.int32, (rows, size), 1)
    turned = jnp.where(lane == 0, center, jnp.where(lane == 1, power, 0.0))
    turned = [jnp.transpose(turned[r : r + size])[0:8] for r in range(0, rows, size)]
    centers = pieces(jnp.concatenate([v[0:1] for v in turned], axis=0))
    powers = pieces(jnp.concatenate([v[1:2] for v in turned], axis=0))
    tail = [p.astype(f32) for p in (*centers, *powers[:2], *pieces(gain_ref[...]), *pieces(bias_ref[...]))]
    tail = jnp.concatenate(tail, axis=0).astype(bf16)
    first = first.astype(bf16)
    for i in range(out_ref.shape[0]):
        out_ref[i, :rows] = first
        out_ref[i, rows:] = tail


def mlp_kernel(
    at_ref,
    ours_ref,
    other_ref,
    choose_ref,
    up_hbm,
    down_hbm,
    theirs_ref,
    mine_ref,
    own_ref,
    joined,
    shifts,
    up_ref,
    down_ref,
    sems,
):
    up_copy = pltpu.make_async_copy(up_hbm, up_ref, sems.at[0])
    down_copy = pltpu.make_async_copy(down_hbm, down_ref, sems.at[1])
    up_copy.start()
    t, kv = at_ref[0], at_ref[1]
    blocks, rows, size = ours_ref.shape
    rows -= 16
    tails = []
    for ref in (ours_ref, other_ref):
        for k in range(blocks):
            tails.append(ref[k, rows:].astype(f32))
    centers = [v[0:2] + v[2:4] + v[4:6] for v in tails]
    center = sum(centers) * (1.0 / len(centers))
    centers = [c - center for c in centers]
    power = sum(v[6:8] + v[8:10] for v in tails) + size * sum(c * c for c in centers)
    scale = lax.rsqrt(power * (1.0 / (size * len(tails))) + epsilon)
    wanted = [*(c * scale for c in centers)]
    lines = [jnp.concatenate([v[r : r + 1] for v in wanted], axis=0) for r in range(rows // size)]
    lines = jnp.concatenate(lines, axis=1)
    shifts[...] = jnp.transpose(jnp.concatenate(pieces(lines), axis=0))
    factor = jnp.concatenate(
        [jnp.transpose(jnp.broadcast_to(scale[r : r + 1], (size, size))) for r in range(rows // size)], axis=0
    )
    for side, ref in enumerate((ours_ref, other_ref)):
        if side == 1:
            down_copy.start()
        for k in range(blocks):
            block = side * blocks + k
            shift = spread(shifts[...], choose_ref[:, block * size : (block + 1) * size])
            v = tails[block]
            gain = v[10:11] + v[11:12] + v[12:13]
            bias = v[13:14] + v[14:15] + v[15:16]
            value = (ref[k, :rows].astype(f32) * factor + shift) * gain + bias
            to = 2 * k + (t if side == 0 else 1 - t)
            joined[:, pl.ds(pl.multiple_of(to * size, size), size)] = value.astype(bf16)
    own_ref[...] = joined[:, pl.ds(pl.multiple_of((2 * kv + t) * size, size), size)]
    up_copy.wait()
    upper = dot(joined[...], up_ref[...])
    hidden = jnp.square(jnp.maximum(upper, 0.0)).astype(bf16)
    down_copy.wait()
    for k in range(blocks):
        both = dot(hidden, down_ref[:, 2 * k * size : 2 * (k + 1) * size])
        left, right = both[:, :size], both[:, size:]
        theirs_ref[k] = jnp.where(t == 0, right, left).astype(bf16)
        mine_ref[k] = jnp.where(t == 0, left, right)


def in_hbm(value):
    return pltpu.with_memory_space_constraint(value, pltpu.HBM)


def in_vmem(n):
    return [pl.BlockSpec(memory_space=pltpu.VMEM)] * n


def in_hbm(value):
    return pltpu.with_memory_space_constraint(value, pltpu.HBM)


def head_reads(query, forget, bound, chooser, state):
    rows, heads, size = state.shape[:3]
    return pl.pallas_call(
        read_kernel,
        out_shape=jax.ShapeDtypeStruct((heads // 2, rows, 2 * size), f32),
        in_specs=[*in_vmem(6), pl.BlockSpec(memory_space=pltpu.HBM)],
        out_specs=in_vmem(1)[0],
        scratch_shapes=[
            pltpu.VMEM((heads // 2, 2 * size, 3 * rows), bf16),
            pltpu.VMEM((5, rows, 2, size, size), f32),
            pltpu.SemaphoreType.DMA((5,)),
        ],
        cost_estimate=pl.CostEstimate(flops=1 << 26, bytes_accessed=1 << 23, transcendentals=0),
        compiler_params=pltpu.CompilerParams(vmem_limit_bytes=9 << 20),
        name="heads_read",
    )(*query, *forget, bound[None], chooser, in_hbm(state))


def mixed_heads(query, forget, value, gate, bound, head_gain, reads):
    pairs, rows, wide = reads.shape
    return pl.pallas_call(
        mix_kernel,
        out_shape=jax.ShapeDtypeStruct((16, rows, pairs * wide), bf16),
        in_specs=in_vmem(11),
        out_specs=in_vmem(1)[0],
        compiler_params=pltpu.CompilerParams(vmem_limit_bytes=6 << 20),
        name="heads_mix",
    )(*query, *forget, *value, *gate, bound[None], jnp.tile(head_gain, 2)[None], reads)


def updated_state(forget, value, bound, chooser, state):
    rows, heads, size = state.shape[:3]
    slots = 4
    block = pltpu.VMEM((slots, rows, 2, size, size), f32)
    return pl.pallas_call(
        state_kernel,
        out_shape=jax.ShapeDtypeStruct(state.shape, f32),
        in_specs=[*in_vmem(6), pl.BlockSpec(memory_space=pltpu.HBM)],
        out_specs=pl.BlockSpec(memory_space=pltpu.HBM),
        scratch_shapes=[
            pltpu.VMEM((heads // 2, 2 * size, 3 * rows), bf16),
            pltpu.VMEM((heads // 2, 2 * size, 3 * rows), bf16),
            pltpu.VMEM((heads, rows, size), f32),
            block,
            block,
            pltpu.SemaphoreType.DMA((slots,)),
            pltpu.SemaphoreType.DMA((slots,)),
        ],
        cost_estimate=pl.CostEstimate(flops=1 << 27, bytes_accessed=1 << 25, transcendentals=0),
        compiler_params=pltpu.CompilerParams(vmem_limit_bytes=16 << 20),
        name="state_update",
    )(*forget, *value, bound[None], chooser, in_hbm(state))


def out_halves(at, mixout, w_out):
    half = jax.ShapeDtypeStruct((mixout.shape[0], w_out.shape[1] // 2), f32)
    return pl.pallas_call(
        out_kernel,
        out_shape=(half, half),
        in_specs=[pl.BlockSpec(memory_space=pltpu.SMEM), *in_vmem(2)],
        out_specs=tuple(in_vmem(2)),
        cost_estimate=pl.CostEstimate(flops=1 << 28, bytes_accessed=1 << 21, transcendentals=0),
        compiler_params=pltpu.CompilerParams(vmem_limit_bytes=4 << 20),
        name="out_halves",
    )(at, mixout, w_out)


def message(mine, arrived, own_tokens, gain, bias):
    rows, size = mine.shape
    return pl.pallas_call(
        message_kernel,
        out_shape=jax.ShapeDtypeStruct((16, rows + 16, size), bf16),
        in_specs=in_vmem(5),
        out_specs=in_vmem(1)[0],
        compiler_params=pltpu.CompilerParams(vmem_limit_bytes=4 << 20),
        name="first_message",
    )(mine, arrived, own_tokens, gain[None], bias[None])


def mixer(at, ours, other, chooser, w_up, w_down):
    blocks, rows, size = ours.shape
    rows -= 16
    shape = (blocks, rows, size)
    return pl.pallas_call(
        mlp_kernel,
        out_shape=(
            jax.ShapeDtypeStruct(shape, bf16),
            jax.ShapeDtypeStruct(shape, f32),
            jax.ShapeDtypeStruct((rows, size), bf16),
        ),
        in_specs=[
            pl.BlockSpec(memory_space=pltpu.SMEM),
            *in_vmem(3),
            *[pl.BlockSpec(memory_space=pltpu.HBM)] * 2,
        ],
        out_specs=tuple(in_vmem(3)),
        scratch_shapes=[
            pltpu.VMEM((rows, 2 * blocks * size), bf16),
            pltpu.VMEM((rows, 6 * blocks), bf16),
            pltpu.VMEM(w_up.shape, bf16),
            pltpu.VMEM(w_down.shape, bf16),
            pltpu.SemaphoreType.DMA((2,)),
        ],
        cost_estimate=pl.CostEstimate(flops=1 << 31, bytes_accessed=1 << 23, transcendentals=0),
        compiler_params=pltpu.CompilerParams(vmem_limit_bytes=28 << 20),
        name="channel_mixer",
    )(at, ours, other, chooser, in_hbm(w_up), in_hbm(w_down))


def per_device(
    tokens,
    state,
    w_query,
    w_forget,
    w_input,
    w_gate,
    lower_bound,
    head_gain,
    w_out,
    gain_one,
    bias_one,
    w_up,
    w_down,
    gain_two,
    bias_two,
):
    z, y, t = lax.axis_index("z"), lax.axis_index("y"), lax.axis_index("tp")
    rows = tokens.shape[0]
    rows_own = rows // 16
    width = w_query.shape[1]

    streams = []
    tokens_next = tokens
    for weight, z_first, flip in (
        (w_query, True, 1),
        (w_forget, True, 3),
        (w_input, False, 1),
        (w_gate, False, 3),
    ):
        if z_first:
            order = row_order(rows, z, flip, y, flip, 4, 1)
            axes = ("z", flip, "y", flip)
        else:
            order = row_order(rows, y, flip, z, flip, 1, 4)
            axes = ("y", flip, "z", flip)
        total, opened = scattered_sum(tokens_next, order, weight, *axes)
        streams.append(total)
        tokens_next, _ = lax.optimization_barrier((tokens_next, opened))
    query_raw, forget_raw, value_raw, gate_raw = streams
    chooser = choosers(rows_own, 2 * head_gain.shape[0])
    reads = head_reads(query_raw, forget_raw, lower_bound, chooser, state)
    mixout = mixed_heads(query_raw, forget_raw, value_raw, gate_raw, lower_bound, head_gain, reads)
    columns = w_out.shape[1] // 2
    at = jnp.stack([t, 4 * z + y])
    mixout, at, chooser, wide_chooser = lax.optimization_barrier(
        (mixout, at, chooser, choosers(32, columns))
    )
    mixout = exchanged(mixout, ("z", "y")).reshape(rows, width)
    theirs, mine = out_halves(at, mixout, w_out)
    arrived = flipped(theirs, "tp", 1)
    own_tokens = lax.dynamic_slice_in_dim(tokens, t * columns, columns, 1)
    sent = message(mine, arrived, own_tokens, gain_one, bias_one)
    sent, forget_raw, value_raw = lax.optimization_barrier((sent, forget_raw, value_raw))
    new_state = updated_state(forget_raw, value_raw, lower_bound, chooser, state)
    ours = exchanged(sent, ("z", "y"))
    ours, new_state = lax.optimization_barrier((ours, new_state))
    other = flipped(ours, "tp", 1)
    theirs, mine, normed_own = mixer(at, ours, other, wide_chooser, w_up, w_down)
    mlp = halved(mine, flipped(theirs, "tp", 1)).astype(bf16)
    mlp = exchanged(mlp, ("z", "y")).astype(f32).sum(axis=0)
    second = residual_scale * normed_own.astype(f32) + mlp
    total, squares = packed_total(
        (jnp.sum(second, axis=1), jnp.sum(second * second, axis=1)), ("z", "y", "tp")
    )
    result = finish_norm(second, total, squares, D, gain_two, bias_two).astype(bf16)
    return (result, new_state)


def solution(mesh):
    fine = Mesh(mesh.devices.reshape(4, 4, 4, 2), ("dp", "z", "y", "tp"))
    kv = ("z", "y")
    every = ("z", "y", "tp")
    placed = (
        P("dp", kv),
        P(("dp", "z", "y"), "tp", None, None),
        P(kv, "tp"),
        P(kv, "tp"),
        P(kv, "tp"),
        P(kv, "tp"),
        P("tp"),
        P(),
        P("tp", kv),
        P(every),
        P(every),
        P(None, every),
        P(every, None),
        P(every),
        P(every),
    )
    return jax.shard_map(
        per_device,
        mesh=fine,
        in_specs=placed,
        out_specs=(P("dp", every), P(("dp", "z", "y"), "tp", None, None)),
        check_vma=False,
    )
```

```python
import jax
import jax.numpy as jnp
from jax import lax
from jax.experimental import pallas as pl
from jax.experimental.pallas import tpu as pltpu
from jax.sharding import Mesh
from jax.sharding import PartitionSpec as P

D = 4096
epsilon = 0.1
residual_scale = 1.68
f32 = jnp.float32
bf16 = jnp.bfloat16


def dot(a, b):
    return jnp.dot(a, b, preferred_element_type=f32)


def flipped(value, axis, bits):
    return lax.ppermute(value, axis, [(i, i ^ bits) for i in range(lax.axis_size(axis))])


def exchanged(tiles, axis):
    return lax.all_to_all(tiles, axis, split_axis=0, concat_axis=0, tiled=True)


def of_all(value, axis):
    return exchanged(jnp.broadcast_to(value, (lax.axis_size(axis), *value.shape)), axis)


def relative(flip):
    return (0, 4 - flip, flip, 2)


def row_order(rows, outer, outer_flip, inner, inner_flip, outer_stride, inner_stride):
    own = rows // 16
    p = lax.broadcasted_iota(jnp.int32, (rows, rows), 0)
    c = lax.broadcasted_iota(jnp.int32, (rows, rows), 1)
    block = p // own

    def flip_of(i, flip):
        r = relative(flip)
        return jnp.where(i == 0, r[0], jnp.where(i == 1, r[1], jnp.where(i == 2, r[2], r[3])))

    o = jnp.bitwise_xor(outer, flip_of(block // 4, outer_flip))
    i = jnp.bitwise_xor(inner, flip_of(block % 4, inner_flip))
    source = (o * outer_stride + i * inner_stride) * own + p % own
    return (c == source).astype(bf16)


def halved(kept, received):
    return kept + received.astype(f32)


def project_kernel(tokens_ref, order_ref, weight_ref, sent_ref, kept_ref):
    rows = tokens_ref.shape[0]
    tokens = dot(order_ref[...], tokens_ref[...]).astype(bf16)
    sent_ref[...] = dot(tokens[rows // 2 :], weight_ref[...]).astype(bf16)
    kept_ref[...] = dot(tokens[: rows // 2], weight_ref[...])


def halve_kernel(kept_ref, arrived_ref, sent_ref, next_ref):
    rows = next_ref.shape[0]
    sent_ref[...] = halved(kept_ref[rows:], arrived_ref[rows:]).astype(bf16)
    next_ref[...] = halved(kept_ref[:rows], arrived_ref[:rows])


def to_halves(kernel, rows, width, name, *args):
    return pl.pallas_call(
        kernel,
        out_shape=(jax.ShapeDtypeStruct((rows, width), bf16), jax.ShapeDtypeStruct((rows, width), f32)),
        in_specs=in_vmem(len(args)),
        out_specs=tuple(in_vmem(2)),
        compiler_params=pltpu.CompilerParams(vmem_limit_bytes=4 << 20),
        cost_estimate=pl.CostEstimate(flops=rows << 16, bytes_accessed=rows << 14, transcendentals=0),
        name=name,
    )(*args)


def scattered_sum(tokens, order, weight, first, flip_first, second, flip_second):
    rows, width = tokens.shape[0], weight.shape[1]
    sent, kept = to_halves(project_kernel, rows // 2, width, "project", tokens, order, weight)
    opened = sent
    steps = ((first, flip_first), (first, 4 - flip_first), (second, flip_second), (second, 4 - flip_second))
    for axis, flip in steps:
        arrived = flipped(sent, axis, flip)
        rows //= 2
        if rows > tokens.shape[0] // 16:
            sent, kept = to_halves(halve_kernel, rows // 2, width, "halve", kept, arrived)
    return (kept, arrived), opened


def packed_total(arrays, axis):
    line = jnp.stack(arrays)
    got = of_all(line[None], axis).sum(axis=0)[0]
    return got[0], got[1]


def finish_norm(values, total, squares, width, gain, bias):
    center = total[:, None] / width
    spread = squares[:, None] / width - center * center
    return (values - center) * lax.rsqrt(spread + epsilon) * gain + bias


def rounded(kept_ref, arrived_ref):
    return halved(kept_ref[...], arrived_ref[...]).astype(bf16).astype(f32)


def gates(forget_raw, bound):
    rest = 1.0 - bound
    return bound + rest * jax.nn.sigmoid(forget_raw), rest * jax.nn.sigmoid(-forget_raw)


def pieces(value):
    high = value.astype(bf16)
    rest = value - high.astype(f32)
    middle = rest.astype(bf16)
    return high, middle, (rest - middle.astype(f32)).astype(bf16)


def spread(stacked, chooser):
    return dot(stacked, chooser)


def choosers(rows, lanes):
    k = lax.broadcasted_iota(jnp.int32, (rows, rows * lanes), 0)
    n = lax.broadcasted_iota(jnp.int32, (rows, rows * lanes), 1)
    one = jnp.where(k == n // lanes, 1.0, 0.0).astype(bf16)
    return jnp.concatenate([one] * 3, axis=0)


def by_pairs(value, wide):
    return jnp.concatenate([value[:, at : at + wide] for at in range(0, value.shape[1], wide)], axis=0)


def read_kernel(
    q_kept, q_ref, f_kept, f_ref, bound_ref, state_hbm, reads_ref, stacked, state_ref, choose_ref, sems
):
    slots, rows, _, size = state_ref.shape[:4]
    wide = 2 * size
    pairs = stacked.shape[0]

    def fetched(pair):
        slot = pair % slots
        return pltpu.make_async_copy(state_hbm.at[:, pl.ds(2 * pair, 2)], state_ref.at[slot], sems.at[slot])

    for pair in range(slots):
        fetched(pair).start()
    choose_ref[...] = choosers(rows, wide)
    query = rounded(q_kept, q_ref)
    forget, _ = gates(rounded(f_kept, f_ref), bound_ref[...])
    scaled = jnp.concatenate(pieces(forget * query * jax.nn.sigmoid(query)), axis=0)
    for pair in range(pairs):
        stacked[pair] = jnp.transpose(scaled[:, pair * wide : (pair + 1) * wide])

    def body(pair, carry):
        fetched(pair).wait()
        slot = pair % slots
        for two in range(rows // 2):
            at = slice(2 * two * wide, 2 * (two + 1) * wide)
            columns = spread(stacked[pair], choose_ref[:, at])
            for b in range(2):
                folded = []
                for half in range(2):
                    column = columns[half * size : (half + 1) * size, b * wide : b * wide + size]
                    product = state_ref[slot, 2 * two + b, half] * column
                    folded.append(jnp.sum(product.reshape(size // 8, 8, size), axis=0))
                total = jnp.sum(jnp.concatenate(folded, axis=1), axis=0, keepdims=True)
                reads_ref[pair, 2 * two + b : 2 * two + b + 1, :] = total

        @pl.when(pair + slots < pairs)
        def _():
            fetched(pair + slots).start()

        return carry

    lax.fori_loop(0, pairs, body, 0)


def head_sums(value, size):
    wide = value.shape[1]
    a = lax.broadcasted_iota(jnp.int32, (wide, wide), 0) // size
    b = lax.broadcasted_iota(jnp.int32, (wide, wide), 1) // size
    ones = jnp.where(a == b, 1.0, 0.0).astype(bf16)
    return sum(dot(piece, ones) for piece in pieces(value))


def mix_kernel(
    q_kept, q_ref, f_kept, f_ref, v_kept, v_ref, g_kept, g_ref, bound_ref, gain_ref, reads_ref, mix_ref
):
    pairs, rows, wide = reads_ref.shape
    query = rounded(q_kept, q_ref)
    query = query * jax.nn.sigmoid(query)
    _, keyvec = gates(rounded(f_kept, f_ref), bound_ref[...])
    gate = rounded(g_kept, g_ref)
    gate = by_pairs(gate * jax.nn.sigmoid(gate), wide)
    gain = jnp.concatenate([gain_ref[...]] * 2, axis=1)
    agreement = head_sums(by_pairs(keyvec * query, wide), wide // 2)
    read = reads_ref[...].reshape(pairs * rows, wide) + agreement * by_pairs(rounded(v_kept, v_ref), wide)
    power = head_sums(read * read, wide // 2) * (2.0 / wide)
    mix = (read * lax.rsqrt(power + epsilon) * gain * gate).astype(bf16)
    for pair in range(pairs):
        for i in range(mix_ref.shape[0]):
            mix_ref[i, :, pair * wide : (pair + 1) * wide] = mix[pair * rows : (pair + 1) * rows]


def state_kernel(
    f_kept,
    f_ref,
    v_kept,
    v_ref,
    bound_ref,
    state_ref,
    out_ref,
    forgets,
    keys,
    values,
    old,
    ready,
    choose_ref,
    old_sems,
    sems,
):
    rows, heads, size = state_ref.shape[:3]
    wide = 2 * size
    pairs = heads // 2
    slots = ready.shape[0]

    def fetched(pair):
        slot = pair % slots
        return pltpu.make_async_copy(state_ref.at[:, pl.ds(2 * pair, 2)], old.at[slot], old_sems.at[slot])

    for slot in range(slots):
        fetched(slot).start()
    choose_ref[...] = choosers(rows, wide)
    forget, keyvec = gates(rounded(f_kept, f_ref), bound_ref[...])
    forget = jnp.concatenate(pieces(forget), axis=0)
    keyvec = jnp.concatenate(pieces(keyvec), axis=0)
    value = rounded(v_kept, v_ref)
    for pair in range(heads // 2):
        own = slice(pair * wide, (pair + 1) * wide)
        forgets[pair] = jnp.transpose(forget[:, own])
        keys[pair] = jnp.transpose(keyvec[:, own])
    for head in range(heads):
        values[head] = value[:, head * size : (head + 1) * size]

    def copied(pair):
        slot = pair % slots
        return pltpu.make_async_copy(ready.at[slot], out_ref.at[:, pl.ds(2 * pair, 2)], sems.at[slot])

    def body(pair, carry):
        @pl.when(pair >= slots)
        def _():
            copied(pair - slots).wait()

        fetched(pair).wait()
        slot = pair % slots
        for two in range(rows // 2):
            at = slice(2 * two * wide, 2 * (two + 1) * wide)
            kept = spread(forgets[pair], choose_ref[:, at])
            added = spread(keys[pair], choose_ref[:, at])
            for half in range(2):
                for b in range(2):
                    part = (slice(half * size, (half + 1) * size), slice(b * wide, b * wide + size))
                    row = 2 * two + b
                    ready[slot, row, half] = (
                        kept[part] * old[slot, row, half]
                        + added[part] * values[2 * pair + half, row : row + 1, :]
                    )
        copied(pair).start()

        @pl.when(pair + slots < pairs)
        def _():
            fetched(pair + slots).start()

        return carry

    lax.fori_loop(0, pairs, body, 0)
    for slot in range(slots):
        copied(pairs - slots + slot).wait()


def out_kernel(at_ref, mix_ref, weight_ref, theirs_ref, mine_ref):
    size = mine_ref.shape[1]
    both = dot(mix_ref[...], weight_ref[...])
    left, right = both[:, :size], both[:, size:]
    theirs_ref[...] = jnp.where(at_ref[0] == 0, right, left)
    mine_ref[...] = jnp.where(at_ref[0] == 0, left, right)


def message_kernel(at_ref, mine_ref, arrived_ref, tokens_ref, gain_ref, bias_ref, out_ref):
    rows, size = mine_ref.shape
    tokens = tokens_ref[...].astype(f32)
    tokens = jnp.where(at_ref[0] == 0, tokens[:, :size], tokens[:, size:])
    first = residual_scale * tokens + (mine_ref[...] + arrived_ref[...])
    center = jnp.mean(first, axis=1, keepdims=True)
    first = first - center
    power = jnp.sum(first * first, axis=1, keepdims=True)
    lane = lax.broadcasted_iota(jnp.int32, (rows, size), 1)
    turned = jnp.where(lane == 0, center, jnp.where(lane == 1, power, 0.0))
    turned = [jnp.transpose(turned[r : r + size])[0:8] for r in range(0, rows, size)]
    centers = pieces(jnp.concatenate([v[0:1] for v in turned], axis=0))
    powers = pieces(jnp.concatenate([v[1:2] for v in turned], axis=0))
    tail = [p.astype(f32) for p in (*centers, *powers[:2], *pieces(gain_ref[...]), *pieces(bias_ref[...]))]
    tail = jnp.concatenate(tail, axis=0).astype(bf16)
    first = first.astype(bf16)
    for i in range(out_ref.shape[0]):
        out_ref[i, :rows] = first
        out_ref[i, rows:] = tail


def mlp_kernel(
    at_ref,
    ours_ref,
    other_ref,
    up_hbm,
    down_hbm,
    theirs_ref,
    mine_ref,
    own_ref,
    joined,
    shifts,
    up_ref,
    down_ref,
    sems,
):
    up_copy = pltpu.make_async_copy(up_hbm, up_ref, sems.at[0])
    down_copy = pltpu.make_async_copy(down_hbm, down_ref, sems.at[1])
    up_copy.start()
    t, kv = at_ref[0], at_ref[1]
    blocks, rows, size = ours_ref.shape
    rows -= 16
    tails = []
    for ref in (ours_ref, other_ref):
        for k in range(blocks):
            tails.append(ref[k, rows:].astype(f32))
    centers = [v[0:2] + v[2:4] + v[4:6] for v in tails]
    center = sum(centers) * (1.0 / len(centers))
    centers = [c - center for c in centers]
    power = sum(v[6:8] + v[8:10] for v in tails) + size * sum(c * c for c in centers)
    scale = lax.rsqrt(power * (1.0 / (size * len(tails))) + epsilon)
    wanted = [*(c * scale for c in centers)]
    lines = [jnp.concatenate([v[r : r + 1] for v in wanted], axis=0) for r in range(rows // size)]
    lines = jnp.concatenate(lines, axis=1)
    shifts[...] = jnp.transpose(jnp.concatenate(pieces(lines), axis=0))
    factor = jnp.concatenate(
        [jnp.transpose(jnp.broadcast_to(scale[r : r + 1], (size, size))) for r in range(rows // size)], axis=0
    )
    piece_of = lax.broadcasted_iota(jnp.int32, (6 * blocks, size), 0) % (2 * blocks)
    for side, ref in enumerate((ours_ref, other_ref)):
        if side == 1:
            down_copy.start()
        for k in range(blocks):
            block = side * blocks + k
            shift = spread(shifts[...], jnp.where(piece_of == block, 1.0, 0.0).astype(bf16))
            v = tails[block]
            gain = v[10:11] + v[11:12] + v[12:13]
            bias = v[13:14] + v[14:15] + v[15:16]
            value = (ref[k, :rows].astype(f32) * factor + shift) * gain + bias
            to = 2 * k + (t if side == 0 else 1 - t)
            joined[:, pl.ds(pl.multiple_of(to * size, size), size)] = value.astype(bf16)
    own_ref[...] = joined[:, pl.ds(pl.multiple_of((2 * kv + t) * size, size), size)]
    up_copy.wait()
    upper = dot(joined[...], up_ref[...])
    hidden = jnp.square(jnp.maximum(upper, 0.0)).astype(bf16)
    down_copy.wait()
    for k in range(blocks):
        both = dot(hidden, down_ref[:, 2 * k * size : 2 * (k + 1) * size])
        left, right = both[:, :size], both[:, size:]
        theirs_ref[k] = jnp.where(t == 0, right, left).astype(bf16)
        mine_ref[k] = jnp.where(t == 0, left, right)


def in_hbm(value):
    return pltpu.with_memory_space_constraint(value, pltpu.HBM)


def in_vmem(n):
    return [pl.BlockSpec(memory_space=pltpu.VMEM)] * n


def in_hbm(value):
    return pltpu.with_memory_space_constraint(value, pltpu.HBM)


def head_reads(query, forget, bound, state):
    rows, heads, size = state.shape[:3]
    return pl.pallas_call(
        read_kernel,
        out_shape=jax.ShapeDtypeStruct((heads // 2, rows, 2 * size), f32),
        in_specs=[*in_vmem(5), pl.BlockSpec(memory_space=pltpu.HBM)],
        out_specs=in_vmem(1)[0],
        scratch_shapes=[
            pltpu.VMEM((heads // 2, 2 * size, 3 * rows), bf16),
            pltpu.VMEM((5, rows, 2, size, size), f32),
            pltpu.VMEM((3 * rows, 2 * rows * size), bf16),
            pltpu.SemaphoreType.DMA((5,)),
        ],
        cost_estimate=pl.CostEstimate(flops=1 << 26, bytes_accessed=1 << 23, transcendentals=0),
        compiler_params=pltpu.CompilerParams(vmem_limit_bytes=9 << 20),
        name="heads_read",
    )(*query, *forget, bound[None], in_hbm(state))


def mixed_heads(query, forget, value, gate, bound, head_gain, reads):
    pairs, rows, wide = reads.shape
    return pl.pallas_call(
        mix_kernel,
        out_shape=jax.ShapeDtypeStruct((16, rows, pairs * wide), bf16),
        in_specs=in_vmem(11),
        out_specs=in_vmem(1)[0],
        compiler_params=pltpu.CompilerParams(vmem_limit_bytes=6 << 20),
        name="heads_mix",
    )(*query, *forget, *value, *gate, bound[None], head_gain[None], reads)


def updated_state(forget, value, bound, state):
    rows, heads, size = state.shape[:3]
    slots = 4
    block = pltpu.VMEM((slots, rows, 2, size, size), f32)
    return pl.pallas_call(
        state_kernel,
        out_shape=jax.ShapeDtypeStruct(state.shape, f32),
        in_specs=[*in_vmem(5), pl.BlockSpec(memory_space=pltpu.HBM)],
        out_specs=pl.BlockSpec(memory_space=pltpu.HBM),
        scratch_shapes=[
            pltpu.VMEM((heads // 2, 2 * size, 3 * rows), bf16),
            pltpu.VMEM((heads // 2, 2 * size, 3 * rows), bf16),
            pltpu.VMEM((heads, rows, size), f32),
            block,
            block,
            pltpu.VMEM((3 * rows, 2 * rows * size), bf16),
            pltpu.SemaphoreType.DMA((slots,)),
            pltpu.SemaphoreType.DMA((slots,)),
        ],
        cost_estimate=pl.CostEstimate(flops=1 << 27, bytes_accessed=1 << 25, transcendentals=0),
        compiler_params=pltpu.CompilerParams(vmem_limit_bytes=16 << 20),
        name="state_update",
    )(*forget, *value, bound[None], in_hbm(state))


def out_halves(at, mixout, w_out):
    half = jax.ShapeDtypeStruct((mixout.shape[0], w_out.shape[1] // 2), f32)
    return pl.pallas_call(
        out_kernel,
        out_shape=(half, half),
        in_specs=[pl.BlockSpec(memory_space=pltpu.SMEM), *in_vmem(2)],
        out_specs=tuple(in_vmem(2)),
        cost_estimate=pl.CostEstimate(flops=1 << 28, bytes_accessed=1 << 21, transcendentals=0),
        compiler_params=pltpu.CompilerParams(vmem_limit_bytes=4 << 20),
        name="out_halves",
    )(at, mixout, w_out)


def message(at, mine, arrived, tokens, gain, bias):
    rows, size = mine.shape
    return pl.pallas_call(
        message_kernel,
        out_shape=jax.ShapeDtypeStruct((16, rows + 16, size), bf16),
        in_specs=[pl.BlockSpec(memory_space=pltpu.SMEM), *in_vmem(5)],
        out_specs=in_vmem(1)[0],
        compiler_params=pltpu.CompilerParams(vmem_limit_bytes=4 << 20),
        name="first_message",
    )(at, mine, arrived, tokens, gain[None], bias[None])


def mixer(at, ours, other, w_up, w_down):
    blocks, rows, size = ours.shape
    rows -= 16
    shape = (blocks, rows, size)
    return pl.pallas_call(
        mlp_kernel,
        out_shape=(
            jax.ShapeDtypeStruct(shape, bf16),
            jax.ShapeDtypeStruct(shape, f32),
            jax.ShapeDtypeStruct((rows, size), bf16),
        ),
        in_specs=[
            pl.BlockSpec(memory_space=pltpu.SMEM),
            *in_vmem(2),
            *[pl.BlockSpec(memory_space=pltpu.HBM)] * 2,
        ],
        out_specs=tuple(in_vmem(3)),
        scratch_shapes=[
            pltpu.VMEM((rows, 2 * blocks * size), bf16),
            pltpu.VMEM((rows, 6 * blocks), bf16),
            pltpu.VMEM(w_up.shape, bf16),
            pltpu.VMEM(w_down.shape, bf16),
            pltpu.SemaphoreType.DMA((2,)),
        ],
        cost_estimate=pl.CostEstimate(flops=1 << 31, bytes_accessed=1 << 23, transcendentals=0),
        compiler_params=pltpu.CompilerParams(vmem_limit_bytes=28 << 20),
        name="channel_mixer",
    )(at, ours, other, in_hbm(w_up), in_hbm(w_down))


def per_device(
    tokens,
    state,
    w_query,
    w_forget,
    w_input,
    w_gate,
    lower_bound,
    head_gain,
    w_out,
    gain_one,
    bias_one,
    w_up,
    w_down,
    gain_two,
    bias_two,
):
    z, y, t = lax.axis_index("z"), lax.axis_index("y"), lax.axis_index("tp")
    rows = tokens.shape[0]
    rows_own = rows // 16
    width = w_query.shape[1]

    streams = []
    at = jnp.stack([t, 4 * z + y])
    tokens_next, at = lax.optimization_barrier((tokens, at))
    for weight, z_first, flip in (
        (w_query, True, 1),
        (w_forget, True, 3),
        (w_input, False, 1),
        (w_gate, False, 3),
    ):
        if z_first:
            order = row_order(rows, z, flip, y, flip, 4, 1)
            axes = ("z", flip, "y", flip)
        else:
            order = row_order(rows, y, flip, z, flip, 1, 4)
            axes = ("y", flip, "z", flip)
        total, opened = scattered_sum(tokens_next, order, weight, *axes)
        streams.append(total)
        tokens_next, _ = lax.optimization_barrier((tokens_next, opened))
    query_raw, forget_raw, value_raw, gate_raw = streams
    reads = head_reads(query_raw, forget_raw, lower_bound, state)
    mixout = mixed_heads(query_raw, forget_raw, value_raw, gate_raw, lower_bound, head_gain, reads)
    columns = w_out.shape[1] // 2
    mixout = exchanged(mixout, ("z", "y")).reshape(rows, width)
    theirs, mine = out_halves(at, mixout, w_out)
    arrived = flipped(theirs, "tp", 1)
    sent = message(at, mine, arrived, tokens, gain_one, bias_one)
    sent, forget_raw, value_raw = lax.optimization_barrier((sent, forget_raw, value_raw))
    new_state = updated_state(forget_raw, value_raw, lower_bound, state)
    ours = exchanged(sent, ("z", "y"))
    ours, new_state = lax.optimization_barrier((ours, new_state))
    other = flipped(ours, "tp", 1)
    theirs, mine, normed_own = mixer(at, ours, other, w_up, w_down)
    mlp = halved(mine, flipped(theirs, "tp", 1)).astype(bf16)
    mlp = exchanged(mlp, ("z", "y")).astype(f32).sum(axis=0)
    second = residual_scale * normed_own.astype(f32) + mlp
    total, squares = packed_total(
        (jnp.sum(second, axis=1), jnp.sum(second * second, axis=1)), ("z", "y", "tp")
    )
    result = finish_norm(second, total, squares, D, gain_two, bias_two).astype(bf16)
    return (result, new_state)


def solution(mesh):
    fine = Mesh(mesh.devices.reshape(4, 4, 4, 2), ("dp", "z", "y", "tp"))
    kv = ("z", "y")
    every = ("z", "y", "tp")
    placed = (
        P("dp", kv),
        P(("dp", "z", "y"), "tp", None, None),
        P(kv, "tp"),
        P(kv, "tp"),
        P(kv, "tp"),
        P(kv, "tp"),
        P("tp"),
        P(),
        P("tp", kv),
        P(every),
        P(every),
        P(None, every),
        P(every, None),
        P(every),
        P(every),
    )
    return jax.shard_map(
        per_device,
        mesh=fine,
        in_specs=placed,
        out_specs=(P("dp", every), P(("dp", "z", "y"), "tp", None, None)),
        check_vma=False,
    )
```

```python
import jax
import jax.numpy as jnp
from jax import lax
from jax.experimental import pallas as pl
from jax.experimental.pallas import tpu as pltpu
from jax.sharding import Mesh
from jax.sharding import PartitionSpec as P

D = 4096
STREAMS = ((True, 1), (True, 3), (False, 1), (False, 3))
epsilon = 0.1
residual_scale = 1.68
f32 = jnp.float32
bf16 = jnp.bfloat16


def dot(a, b):
    return jnp.dot(a, b, preferred_element_type=f32)


def flipped(value, axis, bits):
    return lax.ppermute(value, axis, [(i, i ^ bits) for i in range(lax.axis_size(axis))])


def exchanged(tiles, axis):
    return lax.all_to_all(tiles, axis, split_axis=0, concat_axis=0, tiled=True)


def of_all(value, axis):
    return exchanged(jnp.broadcast_to(value, (lax.axis_size(axis), *value.shape)), axis)


def relative(flip):
    return (0, 4 - flip, flip, 2)


def row_order(rows, outer, outer_flip, inner, inner_flip, outer_stride, inner_stride):
    own = rows // 16
    p = lax.broadcasted_iota(jnp.int32, (rows, 128), 0)
    c = lax.broadcasted_iota(jnp.int32, (rows, 128), 1)
    block = p >> (own.bit_length() - 1)

    def flip_of(i, flip):
        r = relative(flip)
        return jnp.where(i == 0, r[0], jnp.where(i == 1, r[1], jnp.where(i == 2, r[2], r[3])))

    o = jnp.bitwise_xor(outer, flip_of(block >> 2, outer_flip))
    i = jnp.bitwise_xor(inner, flip_of(block & 3, inner_flip))
    source = (o * outer_stride + i * inner_stride) * own + (p & (own - 1))
    order = [jnp.where(c + at == source, 1.0, 0.0) for at in range(0, rows, 128)]
    return jnp.concatenate(order, axis=1).astype(bf16)


def halved(kept, received):
    return kept + received.astype(f32)


def project_kernel(at_ref, tokens_hbm, *refs):
    weights, results = refs[:4], refs[4:12]
    tokens_ref, held, sems = refs[12:]
    copies = [pltpu.make_async_copy(tokens_hbm, tokens_ref, sems.at[4])]
    copies += [pltpu.make_async_copy(weights[i], held.at[i], sems.at[i]) for i in range(4)]
    for copy in copies:
        copy.start()
    rows = tokens_ref.shape[0]
    z, y = at_ref[1] >> 2, at_ref[1] & 3
    orders = []
    for z_first, flip in STREAMS:
        if z_first:
            orders.append(row_order(rows, z, flip, y, flip, 4, 1))
        else:
            orders.append(row_order(rows, y, flip, z, flip, 1, 4))
    copies[0].wait()
    for i in range(4):
        tokens = dot(orders[i], tokens_ref[...]).astype(bf16)
        copies[1 + i].wait()
        results[2 * i][...] = dot(tokens[rows // 2 :], held[i]).astype(bf16)
        results[2 * i + 1][...] = dot(tokens[: rows // 2], held[i])


def halve_kernel(kept_ref, arrived_ref, sent_ref, next_ref):
    rows = next_ref.shape[0]
    sent_ref[...] = halved(kept_ref[rows:], arrived_ref[rows:]).astype(bf16)
    next_ref[...] = halved(kept_ref[:rows], arrived_ref[:rows])


def to_halves(kernel, rows, width, name, *args):
    return pl.pallas_call(
        kernel,
        out_shape=(jax.ShapeDtypeStruct((rows, width), bf16), jax.ShapeDtypeStruct((rows, width), f32)),
        in_specs=in_vmem(len(args)),
        out_specs=tuple(in_vmem(2)),
        compiler_params=pltpu.CompilerParams(vmem_limit_bytes=4 << 20),
        cost_estimate=pl.CostEstimate(flops=rows << 16, bytes_accessed=rows << 14, transcendentals=0),
        name=name,
    )(*args)


def projected(at, tokens, weights):
    rows, width = tokens.shape[0] // 2, weights[0].shape[1]
    halves = (jax.ShapeDtypeStruct((rows, width), bf16), jax.ShapeDtypeStruct((rows, width), f32))
    return pl.pallas_call(
        project_kernel,
        out_shape=halves * 4,
        in_specs=[
            pl.BlockSpec(memory_space=pltpu.SMEM),
            *[pl.BlockSpec(memory_space=pltpu.HBM)] * 5,
        ],
        out_specs=tuple(in_vmem(8)),
        scratch_shapes=[
            pltpu.VMEM(tokens.shape, bf16),
            pltpu.VMEM((4, *weights[0].shape), bf16),
            pltpu.SemaphoreType.DMA((5,)),
        ],
        compiler_params=pltpu.CompilerParams(vmem_limit_bytes=12 << 20),
        cost_estimate=pl.CostEstimate(flops=1 << 30, bytes_accessed=1 << 23, transcendentals=0),
        name="project",
    )(at, in_hbm(tokens), *map(in_hbm, weights))


def scattered_sum(sent, kept, first, flip_first, second, flip_second):
    least = kept.shape[0] // 8
    steps = ((first, flip_first), (first, 4 - flip_first), (second, flip_second), (second, 4 - flip_second))
    for axis, flip in steps:
        arrived = flipped(sent, axis, flip)
        rows = kept.shape[0]
        if rows > least:
            sent, kept = to_halves(halve_kernel, rows // 2, kept.shape[1], "halve", kept, arrived)
    return kept, arrived


def packed_total(arrays, axis):
    line = jnp.stack(arrays)
    got = of_all(line[None], axis).sum(axis=0)[0]
    return got[0], got[1]


def finish_norm(values, total, squares, width, gain, bias):
    center = total[:, None] / width
    spread = squares[:, None] / width - center * center
    return (values - center) * lax.rsqrt(spread + epsilon) * gain + bias


def rounded(kept_ref, arrived_ref):
    return halved(kept_ref[...], arrived_ref[...]).astype(bf16).astype(f32)


def gates(forget_raw, bound):
    rest = 1.0 - bound
    return bound + rest * jax.nn.sigmoid(forget_raw), rest * jax.nn.sigmoid(-forget_raw)


def pieces(value):
    high = value.astype(bf16)
    rest = value - high.astype(f32)
    middle = rest.astype(bf16)
    return high, middle, (rest - middle.astype(f32)).astype(bf16)


def spread(stacked, chooser):
    return dot(stacked, chooser)


def choosers(rows, lanes):
    k = lax.broadcasted_iota(jnp.int32, (rows, rows * lanes), 0)
    n = lax.broadcasted_iota(jnp.int32, (rows, rows * lanes), 1)
    one = jnp.where(k == n // lanes, 1.0, 0.0).astype(bf16)
    return jnp.concatenate([one] * 3, axis=0)


def by_pairs(value, wide):
    return jnp.concatenate([value[:, at : at + wide] for at in range(0, value.shape[1], wide)], axis=0)


def read_kernel(
    q_kept, q_ref, f_kept, f_ref, bound_ref, state_hbm, reads_ref, stacked, state_ref, choose_ref, sems
):
    slots, rows, _, size = state_ref.shape[:4]
    wide = 2 * size
    pairs = stacked.shape[0]

    def fetched(pair):
        slot = pair % slots
        return pltpu.make_async_copy(state_hbm.at[:, pl.ds(2 * pair, 2)], state_ref.at[slot], sems.at[slot])

    for pair in range(slots):
        fetched(pair).start()
    choose_ref[...] = choosers(rows, wide)
    query = rounded(q_kept, q_ref)
    forget, _ = gates(rounded(f_kept, f_ref), bound_ref[...])
    scaled = jnp.concatenate(pieces(forget * query * jax.nn.sigmoid(query)), axis=0)
    for pair in range(pairs):
        stacked[pair] = jnp.transpose(scaled[:, pair * wide : (pair + 1) * wide])

    def body(pair, carry):
        fetched(pair).wait()
        slot = pair % slots
        for two in range(rows // 2):
            at = slice(2 * two * wide, 2 * (two + 1) * wide)
            columns = spread(stacked[pair], choose_ref[:, at])
            for b in range(2):
                folded = []
                for half in range(2):
                    column = columns[half * size : (half + 1) * size, b * wide : b * wide + size]
                    product = state_ref[slot, 2 * two + b, half] * column
                    folded.append(jnp.sum(product.reshape(size // 8, 8, size), axis=0))
                total = jnp.sum(jnp.concatenate(folded, axis=1), axis=0, keepdims=True)
                reads_ref[pair, 2 * two + b : 2 * two + b + 1, :] = total

        @pl.when(pair + slots < pairs)
        def _():
            fetched(pair + slots).start()

        return carry

    lax.fori_loop(0, pairs, body, 0)


def head_sums(value, size):
    wide = value.shape[1]
    a = lax.broadcasted_iota(jnp.int32, (wide, wide), 0) // size
    b = lax.broadcasted_iota(jnp.int32, (wide, wide), 1) // size
    ones = jnp.where(a == b, 1.0, 0.0).astype(bf16)
    return sum(dot(piece, ones) for piece in pieces(value))


def mix_kernel(
    q_kept, q_ref, f_kept, f_ref, v_kept, v_ref, g_kept, g_ref, bound_ref, gain_ref, reads_ref, mix_ref
):
    pairs, rows, wide = reads_ref.shape
    query = rounded(q_kept, q_ref)
    query = query * jax.nn.sigmoid(query)
    _, keyvec = gates(rounded(f_kept, f_ref), bound_ref[...])
    gate = rounded(g_kept, g_ref)
    gate = by_pairs(gate * jax.nn.sigmoid(gate), wide)
    gain = jnp.concatenate([gain_ref[...]] * 2, axis=1)
    agreement = head_sums(by_pairs(keyvec * query, wide), wide // 2)
    read = reads_ref[...].reshape(pairs * rows, wide) + agreement * by_pairs(rounded(v_kept, v_ref), wide)
    power = head_sums(read * read, wide // 2) * (2.0 / wide)
    mix = (read * lax.rsqrt(power + epsilon) * gain * gate).astype(bf16)
    for pair in range(pairs):
        for i in range(mix_ref.shape[0]):
            mix_ref[i, :, pair * wide : (pair + 1) * wide] = mix[pair * rows : (pair + 1) * rows]


def state_kernel(
    f_kept,
    f_ref,
    v_kept,
    v_ref,
    bound_ref,
    state_ref,
    out_ref,
    forgets,
    keys,
    values,
    old,
    ready,
    choose_ref,
    old_sems,
    sems,
):
    rows, heads, size = state_ref.shape[:3]
    wide = 2 * size
    pairs = heads // 2
    slots = ready.shape[0]

    def fetched(pair):
        slot = pair % slots
        return pltpu.make_async_copy(state_ref.at[:, pl.ds(2 * pair, 2)], old.at[slot], old_sems.at[slot])

    for slot in range(slots):
        fetched(slot).start()
    choose_ref[...] = choosers(rows, wide)
    forget, keyvec = gates(rounded(f_kept, f_ref), bound_ref[...])
    forget = jnp.concatenate(pieces(forget), axis=0)
    keyvec = jnp.concatenate(pieces(keyvec), axis=0)
    value = rounded(v_kept, v_ref)
    for pair in range(heads // 2):
        own = slice(pair * wide, (pair + 1) * wide)
        forgets[pair] = jnp.transpose(forget[:, own])
        keys[pair] = jnp.transpose(keyvec[:, own])
    for head in range(heads):
        values[head] = value[:, head * size : (head + 1) * size]

    def copied(pair):
        slot = pair % slots
        return pltpu.make_async_copy(ready.at[slot], out_ref.at[:, pl.ds(2 * pair, 2)], sems.at[slot])

    def body(pair, carry):
        @pl.when(pair >= slots)
        def _():
            copied(pair - slots).wait()

        fetched(pair).wait()
        slot = pair % slots
        for two in range(rows // 2):
            at = slice(2 * two * wide, 2 * (two + 1) * wide)
            kept = spread(forgets[pair], choose_ref[:, at])
            added = spread(keys[pair], choose_ref[:, at])
            for half in range(2):
                for b in range(2):
                    part = (slice(half * size, (half + 1) * size), slice(b * wide, b * wide + size))
                    row = 2 * two + b
                    ready[slot, row, half] = (
                        kept[part] * old[slot, row, half]
                        + added[part] * values[2 * pair + half, row : row + 1, :]
                    )
        copied(pair).start()

        @pl.when(pair + slots < pairs)
        def _():
            fetched(pair + slots).start()

        return carry

    lax.fori_loop(0, pairs, body, 0)
    for slot in range(slots):
        copied(pairs - slots + slot).wait()


def out_kernel(at_ref, mix_ref, weight_ref, theirs_ref, mine_ref):
    size = mine_ref.shape[1]
    both = dot(mix_ref[...], weight_ref[...])
    left, right = both[:, :size], both[:, size:]
    theirs_ref[...] = jnp.where(at_ref[0] == 0, right, left)
    mine_ref[...] = jnp.where(at_ref[0] == 0, left, right)


def message_kernel(at_ref, mine_ref, arrived_ref, tokens_ref, gain_ref, bias_ref, out_ref):
    rows, size = mine_ref.shape
    tokens = tokens_ref[...].astype(f32)
    tokens = jnp.where(at_ref[0] == 0, tokens[:, :size], tokens[:, size:])
    first = residual_scale * tokens + (mine_ref[...] + arrived_ref[...])
    center = jnp.mean(first, axis=1, keepdims=True)
    first = first - center
    power = jnp.sum(first * first, axis=1, keepdims=True)
    lane = lax.broadcasted_iota(jnp.int32, (rows, size), 1)
    turned = jnp.where(lane == 0, center, jnp.where(lane == 1, power, 0.0))
    turned = [jnp.transpose(turned[r : r + size])[0:8] for r in range(0, rows, size)]
    centers = pieces(jnp.concatenate([v[0:1] for v in turned], axis=0))
    powers = pieces(jnp.concatenate([v[1:2] for v in turned], axis=0))
    tail = [p.astype(f32) for p in (*centers, *powers[:2], *pieces(gain_ref[...]), *pieces(bias_ref[...]))]
    tail = jnp.concatenate(tail, axis=0).astype(bf16)
    first = first.astype(bf16)
    for i in range(out_ref.shape[0]):
        out_ref[i, :rows] = first
        out_ref[i, rows:] = tail


def mlp_kernel(
    at_ref,
    ours_ref,
    other_ref,
    up_hbm,
    down_hbm,
    theirs_ref,
    mine_ref,
    own_ref,
    joined,
    shifts,
    up_ref,
    down_ref,
    sems,
):
    up_copy = pltpu.make_async_copy(up_hbm, up_ref, sems.at[0])
    down_copy = pltpu.make_async_copy(down_hbm, down_ref, sems.at[1])
    up_copy.start()
    t, kv = at_ref[0], at_ref[1]
    blocks, rows, size = ours_ref.shape
    rows -= 16
    tails = []
    for ref in (ours_ref, other_ref):
        for k in range(blocks):
            tails.append(ref[k, rows:].astype(f32))
    centers = [v[0:2] + v[2:4] + v[4:6] for v in tails]
    center = sum(centers) * (1.0 / len(centers))
    centers = [c - center for c in centers]
    power = sum(v[6:8] + v[8:10] for v in tails) + size * sum(c * c for c in centers)
    scale = lax.rsqrt(power * (1.0 / (size * len(tails))) + epsilon)
    wanted = [*(c * scale for c in centers)]
    lines = [jnp.concatenate([v[r : r + 1] for v in wanted], axis=0) for r in range(rows // size)]
    lines = jnp.concatenate(lines, axis=1)
    shifts[...] = jnp.transpose(jnp.concatenate(pieces(lines), axis=0))
    factor = jnp.concatenate(
        [jnp.transpose(jnp.broadcast_to(scale[r : r + 1], (size, size))) for r in range(rows // size)], axis=0
    )
    piece_of = lax.broadcasted_iota(jnp.int32, (6 * blocks, size), 0) % (2 * blocks)
    for side, ref in enumerate((ours_ref, other_ref)):
        if side == 1:
            down_copy.start()
        for k in range(blocks):
            block = side * blocks + k
            shift = spread(shifts[...], jnp.where(piece_of == block, 1.0, 0.0).astype(bf16))
            v = tails[block]
            gain = v[10:11] + v[11:12] + v[12:13]
            bias = v[13:14] + v[14:15] + v[15:16]
            value = (ref[k, :rows].astype(f32) * factor + shift) * gain + bias
            to = 2 * k + (t if side == 0 else 1 - t)
            joined[:, pl.ds(pl.multiple_of(to * size, size), size)] = value.astype(bf16)
    own_ref[...] = joined[:, pl.ds(pl.multiple_of((2 * kv + t) * size, size), size)]
    up_copy.wait()
    upper = dot(joined[...], up_ref[...])
    hidden = jnp.square(jnp.maximum(upper, 0.0)).astype(bf16)
    down_copy.wait()
    for k in range(blocks):
        both = dot(hidden, down_ref[:, 2 * k * size : 2 * (k + 1) * size])
        left, right = both[:, :size], both[:, size:]
        theirs_ref[k] = jnp.where(t == 0, right, left).astype(bf16)
        mine_ref[k] = jnp.where(t == 0, left, right)


def in_hbm(value):
    return pltpu.with_memory_space_constraint(value, pltpu.HBM)


def in_vmem(n):
    return [pl.BlockSpec(memory_space=pltpu.VMEM)] * n


def in_hbm(value):
    return pltpu.with_memory_space_constraint(value, pltpu.HBM)


def head_reads(query, forget, bound, state):
    rows, heads, size = state.shape[:3]
    return pl.pallas_call(
        read_kernel,
        out_shape=jax.ShapeDtypeStruct((heads // 2, rows, 2 * size), f32),
        in_specs=[*in_vmem(5), pl.BlockSpec(memory_space=pltpu.HBM)],
        out_specs=in_vmem(1)[0],
        scratch_shapes=[
            pltpu.VMEM((heads // 2, 2 * size, 3 * rows), bf16),
            pltpu.VMEM((5, rows, 2, size, size), f32),
            pltpu.VMEM((3 * rows, 2 * rows * size), bf16),
            pltpu.SemaphoreType.DMA((5,)),
        ],
        cost_estimate=pl.CostEstimate(flops=1 << 26, bytes_accessed=1 << 23, transcendentals=0),
        compiler_params=pltpu.CompilerParams(vmem_limit_bytes=9 << 20),
        name="heads_read",
    )(*query, *forget, bound[None], in_hbm(state))


def mixed_heads(query, forget, value, gate, bound, head_gain, reads):
    pairs, rows, wide = reads.shape
    return pl.pallas_call(
        mix_kernel,
        out_shape=jax.ShapeDtypeStruct((16, rows, pairs * wide), bf16),
        in_specs=in_vmem(11),
        out_specs=in_vmem(1)[0],
        compiler_params=pltpu.CompilerParams(vmem_limit_bytes=6 << 20),
        name="heads_mix",
    )(*query, *forget, *value, *gate, bound[None], head_gain[None], reads)


def updated_state(forget, value, bound, state):
    rows, heads, size = state.shape[:3]
    slots = 4
    block = pltpu.VMEM((slots, rows, 2, size, size), f32)
    return pl.pallas_call(
        state_kernel,
        out_shape=jax.ShapeDtypeStruct(state.shape, f32),
        in_specs=[*in_vmem(5), pl.BlockSpec(memory_space=pltpu.HBM)],
        out_specs=pl.BlockSpec(memory_space=pltpu.HBM),
        scratch_shapes=[
            pltpu.VMEM((heads // 2, 2 * size, 3 * rows), bf16),
            pltpu.VMEM((heads // 2, 2 * size, 3 * rows), bf16),
            pltpu.VMEM((heads, rows, size), f32),
            block,
            block,
            pltpu.VMEM((3 * rows, 2 * rows * size), bf16),
            pltpu.SemaphoreType.DMA((slots,)),
            pltpu.SemaphoreType.DMA((slots,)),
        ],
        cost_estimate=pl.CostEstimate(flops=1 << 27, bytes_accessed=1 << 25, transcendentals=0),
        compiler_params=pltpu.CompilerParams(vmem_limit_bytes=16 << 20),
        name="state_update",
    )(*forget, *value, bound[None], in_hbm(state))


def out_halves(at, mixout, w_out):
    half = jax.ShapeDtypeStruct((mixout.shape[0], w_out.shape[1] // 2), f32)
    return pl.pallas_call(
        out_kernel,
        out_shape=(half, half),
        in_specs=[pl.BlockSpec(memory_space=pltpu.SMEM), *in_vmem(2)],
        out_specs=tuple(in_vmem(2)),
        cost_estimate=pl.CostEstimate(flops=1 << 28, bytes_accessed=1 << 21, transcendentals=0),
        compiler_params=pltpu.CompilerParams(vmem_limit_bytes=4 << 20),
        name="out_halves",
    )(at, mixout, w_out)


def message(at, mine, arrived, tokens, gain, bias):
    rows, size = mine.shape
    return pl.pallas_call(
        message_kernel,
        out_shape=jax.ShapeDtypeStruct((16, rows + 16, size), bf16),
        in_specs=[pl.BlockSpec(memory_space=pltpu.SMEM), *in_vmem(5)],
        out_specs=in_vmem(1)[0],
        compiler_params=pltpu.CompilerParams(vmem_limit_bytes=4 << 20),
        name="first_message",
    )(at, mine, arrived, tokens, gain[None], bias[None])


def mixer(at, ours, other, w_up, w_down):
    blocks, rows, size = ours.shape
    rows -= 16
    shape = (blocks, rows, size)
    return pl.pallas_call(
        mlp_kernel,
        out_shape=(
            jax.ShapeDtypeStruct(shape, bf16),
            jax.ShapeDtypeStruct(shape, f32),
            jax.ShapeDtypeStruct((rows, size), bf16),
        ),
        in_specs=[
            pl.BlockSpec(memory_space=pltpu.SMEM),
            *in_vmem(2),
            *[pl.BlockSpec(memory_space=pltpu.HBM)] * 2,
        ],
        out_specs=tuple(in_vmem(3)),
        scratch_shapes=[
            pltpu.VMEM((rows, 2 * blocks * size), bf16),
            pltpu.VMEM((rows, 6 * blocks), bf16),
            pltpu.VMEM(w_up.shape, bf16),
            pltpu.VMEM(w_down.shape, bf16),
            pltpu.SemaphoreType.DMA((2,)),
        ],
        cost_estimate=pl.CostEstimate(flops=1 << 31, bytes_accessed=1 << 23, transcendentals=0),
        compiler_params=pltpu.CompilerParams(vmem_limit_bytes=28 << 20),
        name="channel_mixer",
    )(at, ours, other, in_hbm(w_up), in_hbm(w_down))


def per_device(
    tokens,
    state,
    w_query,
    w_forget,
    w_input,
    w_gate,
    lower_bound,
    head_gain,
    w_out,
    gain_one,
    bias_one,
    w_up,
    w_down,
    gain_two,
    bias_two,
):
    z, y, t = lax.axis_index("z"), lax.axis_index("y"), lax.axis_index("tp")
    rows = tokens.shape[0]
    rows_own = rows // 16
    width = w_query.shape[1]

    at = jnp.stack([t, 4 * z + y])
    halves = projected(at, tokens, (w_query, w_forget, w_input, w_gate))
    streams = []
    sent = halves[0::2]
    for i, (z_first, flip) in enumerate(STREAMS):
        axes = ("z", flip, "y", flip) if z_first else ("y", flip, "z", flip)
        streams.append(scattered_sum(sent[i], halves[2 * i + 1], *axes))
    query_raw, forget_raw, value_raw, gate_raw = streams
    reads = head_reads(query_raw, forget_raw, lower_bound, state)
    mixout = mixed_heads(query_raw, forget_raw, value_raw, gate_raw, lower_bound, head_gain, reads)
    columns = w_out.shape[1] // 2
    mixout = exchanged(mixout, ("z", "y")).reshape(rows, width)
    theirs, mine = out_halves(at, mixout, w_out)
    arrived = flipped(theirs, "tp", 1)
    sent = message(at, mine, arrived, tokens, gain_one, bias_one)
    sent, forget_raw, value_raw = lax.optimization_barrier((sent, forget_raw, value_raw))
    new_state = updated_state(forget_raw, value_raw, lower_bound, state)
    ours = exchanged(sent, ("z", "y"))
    ours, new_state = lax.optimization_barrier((ours, new_state))
    other = flipped(ours, "tp", 1)
    theirs, mine, normed_own = mixer(at, ours, other, w_up, w_down)
    mlp = halved(mine, flipped(theirs, "tp", 1)).astype(bf16)
    mlp = exchanged(mlp, ("z", "y")).astype(f32).sum(axis=0)
    second = residual_scale * normed_own.astype(f32) + mlp
    total, squares = packed_total(
        (jnp.sum(second, axis=1), jnp.sum(second * second, axis=1)), ("z", "y", "tp")
    )
    result = finish_norm(second, total, squares, D, gain_two, bias_two).astype(bf16)
    return (result, new_state)


def solution(mesh):
    fine = Mesh(mesh.devices.reshape(4, 4, 4, 2), ("dp", "z", "y", "tp"))
    kv = ("z", "y")
    every = ("z", "y", "tp")
    placed = (
        P("dp", kv),
        P(("dp", "z", "y"), "tp", None, None),
        P(kv, "tp"),
        P(kv, "tp"),
        P(kv, "tp"),
        P(kv, "tp"),
        P("tp"),
        P(),
        P("tp", kv),
        P(every),
        P(every),
        P(None, every),
        P(every, None),
        P(every),
        P(every),
    )
    return jax.shard_map(
        per_device,
        mesh=fine,
        in_specs=placed,
        out_specs=(P("dp", every), P(("dp", "z", "y"), "tp", None, None)),
        check_vma=False,
    )
```

```python
import functools

import jax
import jax.numpy as jnp
from jax import lax
from jax.experimental import pallas as pl
from jax.experimental.pallas import tpu as pltpu
from jax.sharding import Mesh
from jax.sharding import PartitionSpec as P

D = 4096
STREAMS = ((True, 1), (True, 3), (False, 1), (False, 3))
epsilon = 0.1
residual_scale = 1.68
f32 = jnp.float32
bf16 = jnp.bfloat16


def dot(a, b):
    return jnp.dot(a, b, preferred_element_type=f32)


def flipped(value, axis, bits):
    return lax.ppermute(value, axis, [(i, i ^ bits) for i in range(lax.axis_size(axis))])


def exchanged(tiles, axis):
    return lax.all_to_all(tiles, axis, split_axis=0, concat_axis=0, tiled=True)


def of_all(value, axis):
    return exchanged(jnp.broadcast_to(value, (lax.axis_size(axis), *value.shape)), axis)


def relative(flip):
    return (0, 4 - flip, flip, 2)


def row_order(rows, start, outer, outer_flip, inner, inner_flip, outer_stride, inner_stride):
    own = rows // 16
    p = lax.broadcasted_iota(jnp.int32, (rows // 2, 128), 0) + start
    c = lax.broadcasted_iota(jnp.int32, (rows // 2, 128), 1)
    block = p >> (own.bit_length() - 1)

    def flip_of(i, flip):
        r = relative(flip)
        return jnp.where(i == 0, r[0], jnp.where(i == 1, r[1], jnp.where(i == 2, r[2], r[3])))

    o = jnp.bitwise_xor(outer, flip_of(block >> 2, outer_flip))
    i = jnp.bitwise_xor(inner, flip_of(block & 3, inner_flip))
    source = (o * outer_stride + i * inner_stride) * own + (p & (own - 1))
    order = [jnp.where(c + at == source, 1.0, 0.0) for at in range(0, rows, 128)]
    return jnp.concatenate(order, axis=1).astype(bf16)


def halved(kept, received):
    return kept + received.astype(f32)


def project_kernel(start, at_ref, tokens_hbm, *refs):
    weights, results = refs[:4], refs[4:8]
    tokens_ref, held, sems = refs[8:]
    copies = [pltpu.make_async_copy(tokens_hbm, tokens_ref, sems.at[4])]
    copies += [pltpu.make_async_copy(weights[i], held.at[i], sems.at[i]) for i in range(4)]
    for copy in copies:
        copy.start()
    rows = tokens_ref.shape[0]
    z, y = at_ref[1] >> 2, at_ref[1] & 3
    orders = []
    for z_first, flip in STREAMS:
        if z_first:
            orders.append(row_order(rows, start, z, flip, y, flip, 4, 1))
        else:
            orders.append(row_order(rows, start, y, flip, z, flip, 1, 4))
    copies[0].wait()
    for i in range(4):
        tokens = dot(orders[i], tokens_ref[...]).astype(bf16)
        copies[1 + i].wait()
        results[i][...] = dot(tokens, held[i]).astype(results[i].dtype)


def halve_kernel(kept_ref, arrived_ref, sent_ref, next_ref):
    rows = next_ref.shape[0]
    sent_ref[...] = halved(kept_ref[rows:], arrived_ref[rows:]).astype(bf16)
    next_ref[...] = halved(kept_ref[:rows], arrived_ref[:rows])


def to_halves(kernel, rows, width, name, *args):
    return pl.pallas_call(
        kernel,
        out_shape=(jax.ShapeDtypeStruct((rows, width), bf16), jax.ShapeDtypeStruct((rows, width), f32)),
        in_specs=in_vmem(len(args)),
        out_specs=tuple(in_vmem(2)),
        compiler_params=pltpu.CompilerParams(vmem_limit_bytes=4 << 20),
        cost_estimate=pl.CostEstimate(flops=rows << 16, bytes_accessed=rows << 14, transcendentals=0),
        name=name,
    )(*args)


def projected(start, dtype, at, tokens, weights):
    rows, width = tokens.shape[0] // 2, weights[0].shape[1]
    return pl.pallas_call(
        functools.partial(project_kernel, start),
        out_shape=(jax.ShapeDtypeStruct((rows, width), dtype),) * 4,
        in_specs=[
            pl.BlockSpec(memory_space=pltpu.SMEM),
            *[pl.BlockSpec(memory_space=pltpu.HBM)] * 5,
        ],
        out_specs=tuple(in_vmem(4)),
        scratch_shapes=[
            pltpu.VMEM(tokens.shape, bf16),
            pltpu.VMEM((4, *weights[0].shape), bf16),
            pltpu.SemaphoreType.DMA((5,)),
        ],
        compiler_params=pltpu.CompilerParams(vmem_limit_bytes=12 << 20),
        cost_estimate=pl.CostEstimate(flops=1 << 30, bytes_accessed=1 << 23, transcendentals=0),
        name="project",
    )(at, in_hbm(tokens), *map(in_hbm, weights))


def scattered_sum(sent, kept, first, flip_first, second, flip_second):
    least = kept.shape[0] // 8
    steps = ((first, flip_first), (first, 4 - flip_first), (second, flip_second), (second, 4 - flip_second))
    for axis, flip in steps:
        arrived = flipped(sent, axis, flip)
        rows = kept.shape[0]
        if rows > least:
            sent, kept = to_halves(halve_kernel, rows // 2, kept.shape[1], "halve", kept, arrived)
    return kept, arrived


def packed_total(arrays, axis):
    line = jnp.stack(arrays)
    got = of_all(line[None], axis).sum(axis=0)[0]
    return got[0], got[1]


def finish_norm(values, total, squares, width, gain, bias):
    center = total[:, None] / width
    spread = squares[:, None] / width - center * center
    return (values - center) * lax.rsqrt(spread + epsilon) * gain + bias


def rounded(kept_ref, arrived_ref):
    return halved(kept_ref[...], arrived_ref[...]).astype(bf16).astype(f32)


def gates(forget_raw, bound):
    rest = 1.0 - bound
    return bound + rest * jax.nn.sigmoid(forget_raw), rest * jax.nn.sigmoid(-forget_raw)


def pieces(value):
    high = value.astype(bf16)
    rest = value - high.astype(f32)
    middle = rest.astype(bf16)
    return high, middle, (rest - middle.astype(f32)).astype(bf16)


def spread(stacked, chooser):
    return dot(stacked, chooser)


def choosers(rows, lanes):
    k = lax.broadcasted_iota(jnp.int32, (rows, rows * lanes), 0)
    n = lax.broadcasted_iota(jnp.int32, (rows, rows * lanes), 1)
    one = jnp.where(k == n // lanes, 1.0, 0.0).astype(bf16)
    return jnp.concatenate([one] * 3, axis=0)


def by_pairs(value, wide):
    return jnp.concatenate([value[:, at : at + wide] for at in range(0, value.shape[1], wide)], axis=0)


def read_kernel(
    q_kept, q_ref, f_kept, f_ref, bound_ref, state_hbm, reads_ref, stacked, state_ref, choose_ref, sems
):
    slots, rows, _, size = state_ref.shape[:4]
    wide = 2 * size
    pairs = stacked.shape[0]

    def fetched(pair):
        slot = pair % slots
        return pltpu.make_async_copy(state_hbm.at[:, pl.ds(2 * pair, 2)], state_ref.at[slot], sems.at[slot])

    for pair in range(slots):
        fetched(pair).start()
    choose_ref[...] = choosers(rows, wide)
    query = rounded(q_kept, q_ref)
    forget, _ = gates(rounded(f_kept, f_ref), bound_ref[...])
    scaled = jnp.concatenate(pieces(forget * query * jax.nn.sigmoid(query)), axis=0)
    for pair in range(pairs):
        stacked[pair] = jnp.transpose(scaled[:, pair * wide : (pair + 1) * wide])

    def body(pair, carry):
        fetched(pair).wait()
        slot = pair % slots
        for two in range(rows // 2):
            at = slice(2 * two * wide, 2 * (two + 1) * wide)
            columns = spread(stacked[pair], choose_ref[:, at])
            for b in range(2):
                folded = []
                for half in range(2):
                    column = columns[half * size : (half + 1) * size, b * wide : b * wide + size]
                    product = state_ref[slot, 2 * two + b, half] * column
                    folded.append(jnp.sum(product.reshape(size // 8, 8, size), axis=0))
                total = jnp.sum(jnp.concatenate(folded, axis=1), axis=0, keepdims=True)
                reads_ref[pair, 2 * two + b : 2 * two + b + 1, :] = total

        @pl.when(pair + slots < pairs)
        def _():
            fetched(pair + slots).start()

        return carry

    lax.fori_loop(0, pairs, body, 0)


def head_sums(value, size):
    wide = value.shape[1]
    a = lax.broadcasted_iota(jnp.int32, (wide, wide), 0) // size
    b = lax.broadcasted_iota(jnp.int32, (wide, wide), 1) // size
    ones = jnp.where(a == b, 1.0, 0.0).astype(bf16)
    return sum(dot(piece, ones) for piece in pieces(value))


def mix_kernel(
    q_kept, q_ref, f_kept, f_ref, v_kept, v_ref, g_kept, g_ref, bound_ref, gain_ref, reads_ref, mix_ref
):
    pairs, rows, wide = reads_ref.shape
    query = rounded(q_kept, q_ref)
    query = query * jax.nn.sigmoid(query)
    _, keyvec = gates(rounded(f_kept, f_ref), bound_ref[...])
    gate = rounded(g_kept, g_ref)
    gate = by_pairs(gate * jax.nn.sigmoid(gate), wide)
    gain = jnp.concatenate([gain_ref[...]] * 2, axis=1)
    agreement = head_sums(by_pairs(keyvec * query, wide), wide // 2)
    read = reads_ref[...].reshape(pairs * rows, wide) + agreement * by_pairs(rounded(v_kept, v_ref), wide)
    power = head_sums(read * read, wide // 2) * (2.0 / wide)
    mix = (read * lax.rsqrt(power + epsilon) * gain * gate).astype(bf16)
    for pair in range(pairs):
        for i in range(mix_ref.shape[0]):
            mix_ref[i, :, pair * wide : (pair + 1) * wide] = mix[pair * rows : (pair + 1) * rows]


def state_kernel(
    f_kept,
    f_ref,
    v_kept,
    v_ref,
    bound_ref,
    state_ref,
    out_ref,
    forgets,
    keys,
    values,
    old,
    ready,
    choose_ref,
    old_sems,
    sems,
):
    rows, heads, size = state_ref.shape[:3]
    wide = 2 * size
    pairs = heads // 2
    slots = ready.shape[0]

    def fetched(pair):
        slot = pair % slots
        return pltpu.make_async_copy(state_ref.at[:, pl.ds(2 * pair, 2)], old.at[slot], old_sems.at[slot])

    for slot in range(slots):
        fetched(slot).start()
    choose_ref[...] = choosers(rows, wide)
    forget, keyvec = gates(rounded(f_kept, f_ref), bound_ref[...])
    forget = jnp.concatenate(pieces(forget), axis=0)
    keyvec = jnp.concatenate(pieces(keyvec), axis=0)
    value = rounded(v_kept, v_ref)
    for pair in range(heads // 2):
        own = slice(pair * wide, (pair + 1) * wide)
        forgets[pair] = jnp.transpose(forget[:, own])
        keys[pair] = jnp.transpose(keyvec[:, own])
    for head in range(heads):
        values[head] = value[:, head * size : (head + 1) * size]

    def copied(pair):
        slot = pair % slots
        return pltpu.make_async_copy(ready.at[slot], out_ref.at[:, pl.ds(2 * pair, 2)], sems.at[slot])

    def body(pair, carry):
        @pl.when(pair >= slots)
        def _():
            copied(pair - slots).wait()

        fetched(pair).wait()
        slot = pair % slots
        for two in range(rows // 2):
            at = slice(2 * two * wide, 2 * (two + 1) * wide)
            kept = spread(forgets[pair], choose_ref[:, at])
            added = spread(keys[pair], choose_ref[:, at])
            for half in range(2):
                for b in range(2):
                    part = (slice(half * size, (half + 1) * size), slice(b * wide, b * wide + size))
                    row = 2 * two + b
                    ready[slot, row, half] = (
                        kept[part] * old[slot, row, half]
                        + added[part] * values[2 * pair + half, row : row + 1, :]
                    )
        copied(pair).start()

        @pl.when(pair + slots < pairs)
        def _():
            fetched(pair + slots).start()

        return carry

    lax.fori_loop(0, pairs, body, 0)
    for slot in range(slots):
        copied(pairs - slots + slot).wait()


def out_kernel(at_ref, mix_ref, weight_ref, theirs_ref, mine_ref):
    size = mine_ref.shape[1]
    both = dot(mix_ref[...], weight_ref[...])
    left, right = both[:, :size], both[:, size:]
    theirs_ref[...] = jnp.where(at_ref[0] == 0, right, left)
    mine_ref[...] = jnp.where(at_ref[0] == 0, left, right)


def message_kernel(at_ref, mine_ref, arrived_ref, tokens_ref, gain_ref, bias_ref, out_ref):
    rows, size = mine_ref.shape
    tokens = tokens_ref[...].astype(f32)
    tokens = jnp.where(at_ref[0] == 0, tokens[:, :size], tokens[:, size:])
    first = residual_scale * tokens + (mine_ref[...] + arrived_ref[...])
    center = jnp.mean(first, axis=1, keepdims=True)
    first = first - center
    power = jnp.sum(first * first, axis=1, keepdims=True)
    lane = lax.broadcasted_iota(jnp.int32, (rows, size), 1)
    turned = jnp.where(lane == 0, center, jnp.where(lane == 1, power, 0.0))
    turned = [jnp.transpose(turned[r : r + size])[0:8] for r in range(0, rows, size)]
    centers = pieces(jnp.concatenate([v[0:1] for v in turned], axis=0))
    powers = pieces(jnp.concatenate([v[1:2] for v in turned], axis=0))
    tail = [p.astype(f32) for p in (*centers, *powers[:2], *pieces(gain_ref[...]), *pieces(bias_ref[...]))]
    tail = jnp.concatenate(tail, axis=0).astype(bf16)
    first = first.astype(bf16)
    for i in range(out_ref.shape[0]):
        out_ref[i, :rows] = first
        out_ref[i, rows:] = tail


def mlp_kernel(
    at_ref,
    ours_ref,
    other_ref,
    up_hbm,
    down_hbm,
    theirs_ref,
    mine_ref,
    own_ref,
    joined,
    shifts,
    up_ref,
    down_ref,
    sems,
):
    up_copy = pltpu.make_async_copy(up_hbm, up_ref, sems.at[0])
    down_copy = pltpu.make_async_copy(down_hbm, down_ref, sems.at[1])
    up_copy.start()
    t, kv = at_ref[0], at_ref[1]
    blocks, rows, size = ours_ref.shape
    rows -= 16
    tails = []
    for ref in (ours_ref, other_ref):
        for k in range(blocks):
            tails.append(ref[k, rows:].astype(f32))
    centers = [v[0:2] + v[2:4] + v[4:6] for v in tails]
    center = sum(centers) * (1.0 / len(centers))
    centers = [c - center for c in centers]
    power = sum(v[6:8] + v[8:10] for v in tails) + size * sum(c * c for c in centers)
    scale = lax.rsqrt(power * (1.0 / (size * len(tails))) + epsilon)
    wanted = [*(c * scale for c in centers)]
    lines = [jnp.concatenate([v[r : r + 1] for v in wanted], axis=0) for r in range(rows // size)]
    lines = jnp.concatenate(lines, axis=1)
    shifts[...] = jnp.transpose(jnp.concatenate(pieces(lines), axis=0))
    factor = jnp.concatenate(
        [jnp.transpose(jnp.broadcast_to(scale[r : r + 1], (size, size))) for r in range(rows // size)], axis=0
    )
    piece_of = lax.broadcasted_iota(jnp.int32, (6 * blocks, size), 0) % (2 * blocks)
    for side, ref in enumerate((ours_ref, other_ref)):
        if side == 1:
            down_copy.start()
        for k in range(blocks):
            block = side * blocks + k
            shift = spread(shifts[...], jnp.where(piece_of == block, 1.0, 0.0).astype(bf16))
            v = tails[block]
            gain = v[10:11] + v[11:12] + v[12:13]
            bias = v[13:14] + v[14:15] + v[15:16]
            value = (ref[k, :rows].astype(f32) * factor + shift) * gain + bias
            to = 2 * k + (t if side == 0 else 1 - t)
            joined[:, pl.ds(pl.multiple_of(to * size, size), size)] = value.astype(bf16)
    own_ref[...] = joined[:, pl.ds(pl.multiple_of((2 * kv + t) * size, size), size)]
    up_copy.wait()
    upper = dot(joined[...], up_ref[...])
    hidden = jnp.square(jnp.maximum(upper, 0.0)).astype(bf16)
    down_copy.wait()
    for k in range(blocks):
        both = dot(hidden, down_ref[:, 2 * k * size : 2 * (k + 1) * size])
        left, right = both[:, :size], both[:, size:]
        theirs_ref[k] = jnp.where(t == 0, right, left).astype(bf16)
        mine_ref[k] = jnp.where(t == 0, left, right)


def in_hbm(value):
    return pltpu.with_memory_space_constraint(value, pltpu.HBM)


def in_vmem(n):
    return [pl.BlockSpec(memory_space=pltpu.VMEM)] * n


def in_hbm(value):
    return pltpu.with_memory_space_constraint(value, pltpu.HBM)


def head_reads(query, forget, bound, state):
    rows, heads, size = state.shape[:3]
    return pl.pallas_call(
        read_kernel,
        out_shape=jax.ShapeDtypeStruct((heads // 2, rows, 2 * size), f32),
        in_specs=[*in_vmem(5), pl.BlockSpec(memory_space=pltpu.HBM)],
        out_specs=in_vmem(1)[0],
        scratch_shapes=[
            pltpu.VMEM((heads // 2, 2 * size, 3 * rows), bf16),
            pltpu.VMEM((5, rows, 2, size, size), f32),
            pltpu.VMEM((3 * rows, 2 * rows * size), bf16),
            pltpu.SemaphoreType.DMA((5,)),
        ],
        cost_estimate=pl.CostEstimate(flops=1 << 26, bytes_accessed=1 << 23, transcendentals=0),
        compiler_params=pltpu.CompilerParams(vmem_limit_bytes=9 << 20),
        name="heads_read",
    )(*query, *forget, bound[None], in_hbm(state))


def mixed_heads(query, forget, value, gate, bound, head_gain, reads):
    pairs, rows, wide = reads.shape
    return pl.pallas_call(
        mix_kernel,
        out_shape=jax.ShapeDtypeStruct((16, rows, pairs * wide), bf16),
        in_specs=in_vmem(11),
        out_specs=in_vmem(1)[0],
        compiler_params=pltpu.CompilerParams(vmem_limit_bytes=6 << 20),
        name="heads_mix",
    )(*query, *forget, *value, *gate, bound[None], head_gain[None], reads)


def updated_state(forget, value, bound, state):
    rows, heads, size = state.shape[:3]
    slots = 4
    block = pltpu.VMEM((slots, rows, 2, size, size), f32)
    return pl.pallas_call(
        state_kernel,
        out_shape=jax.ShapeDtypeStruct(state.shape, f32),
        in_specs=[*in_vmem(5), pl.BlockSpec(memory_space=pltpu.HBM)],
        out_specs=pl.BlockSpec(memory_space=pltpu.HBM),
        scratch_shapes=[
            pltpu.VMEM((heads // 2, 2 * size, 3 * rows), bf16),
            pltpu.VMEM((heads // 2, 2 * size, 3 * rows), bf16),
            pltpu.VMEM((heads, rows, size), f32),
            block,
            block,
            pltpu.VMEM((3 * rows, 2 * rows * size), bf16),
            pltpu.SemaphoreType.DMA((slots,)),
            pltpu.SemaphoreType.DMA((slots,)),
        ],
        cost_estimate=pl.CostEstimate(flops=1 << 27, bytes_accessed=1 << 25, transcendentals=0),
        compiler_params=pltpu.CompilerParams(vmem_limit_bytes=16 << 20),
        name="state_update",
    )(*forget, *value, bound[None], in_hbm(state))


def out_halves(at, mixout, w_out):
    half = jax.ShapeDtypeStruct((mixout.shape[0], w_out.shape[1] // 2), f32)
    return pl.pallas_call(
        out_kernel,
        out_shape=(half, half),
        in_specs=[pl.BlockSpec(memory_space=pltpu.SMEM), *in_vmem(2)],
        out_specs=tuple(in_vmem(2)),
        cost_estimate=pl.CostEstimate(flops=1 << 28, bytes_accessed=1 << 21, transcendentals=0),
        compiler_params=pltpu.CompilerParams(vmem_limit_bytes=4 << 20),
        name="out_halves",
    )(at, mixout, w_out)


def message(at, mine, arrived, tokens, gain, bias):
    rows, size = mine.shape
    return pl.pallas_call(
        message_kernel,
        out_shape=jax.ShapeDtypeStruct((16, rows + 16, size), bf16),
        in_specs=[pl.BlockSpec(memory_space=pltpu.SMEM), *in_vmem(5)],
        out_specs=in_vmem(1)[0],
        compiler_params=pltpu.CompilerParams(vmem_limit_bytes=4 << 20),
        name="first_message",
    )(at, mine, arrived, tokens, gain[None], bias[None])


def mixer(at, ours, other, w_up, w_down):
    blocks, rows, size = ours.shape
    rows -= 16
    shape = (blocks, rows, size)
    return pl.pallas_call(
        mlp_kernel,
        out_shape=(
            jax.ShapeDtypeStruct(shape, bf16),
            jax.ShapeDtypeStruct(shape, f32),
            jax.ShapeDtypeStruct((rows, size), bf16),
        ),
        in_specs=[
            pl.BlockSpec(memory_space=pltpu.SMEM),
            *in_vmem(2),
            *[pl.BlockSpec(memory_space=pltpu.HBM)] * 2,
        ],
        out_specs=tuple(in_vmem(3)),
        scratch_shapes=[
            pltpu.VMEM((rows, 2 * blocks * size), bf16),
            pltpu.VMEM((rows, 6 * blocks), bf16),
            pltpu.VMEM(w_up.shape, bf16),
            pltpu.VMEM(w_down.shape, bf16),
            pltpu.SemaphoreType.DMA((2,)),
        ],
        cost_estimate=pl.CostEstimate(flops=1 << 31, bytes_accessed=1 << 23, transcendentals=0),
        compiler_params=pltpu.CompilerParams(vmem_limit_bytes=28 << 20),
        name="channel_mixer",
    )(at, ours, other, in_hbm(w_up), in_hbm(w_down))


def per_device(
    tokens,
    state,
    w_query,
    w_forget,
    w_input,
    w_gate,
    lower_bound,
    head_gain,
    w_out,
    gain_one,
    bias_one,
    w_up,
    w_down,
    gain_two,
    bias_two,
):
    z, y, t = lax.axis_index("z"), lax.axis_index("y"), lax.axis_index("tp")
    rows = tokens.shape[0]
    rows_own = rows // 16
    width = w_query.shape[1]

    at = jnp.stack([t, 4 * z + y])
    weights = (w_query, w_forget, w_input, w_gate)
    sent = projected(rows // 2, bf16, at, tokens, weights)
    at_kept, sent = lax.optimization_barrier((at, sent))
    kept = projected(0, f32, at_kept, tokens, weights)
    streams = []
    for i, (z_first, flip) in enumerate(STREAMS):
        axes = ("z", flip, "y", flip) if z_first else ("y", flip, "z", flip)
        streams.append(scattered_sum(sent[i], kept[i], *axes))
    query_raw, forget_raw, value_raw, gate_raw = streams
    reads = head_reads(query_raw, forget_raw, lower_bound, state)
    mixout = mixed_heads(query_raw, forget_raw, value_raw, gate_raw, lower_bound, head_gain, reads)
    columns = w_out.shape[1] // 2
    mixout = exchanged(mixout, ("z", "y")).reshape(rows, width)
    theirs, mine = out_halves(at, mixout, w_out)
    arrived = flipped(theirs, "tp", 1)
    sent = message(at, mine, arrived, tokens, gain_one, bias_one)
    sent, forget_raw, value_raw = lax.optimization_barrier((sent, forget_raw, value_raw))
    new_state = updated_state(forget_raw, value_raw, lower_bound, state)
    ours = exchanged(sent, ("z", "y"))
    ours, new_state = lax.optimization_barrier((ours, new_state))
    other = flipped(ours, "tp", 1)
    theirs, mine, normed_own = mixer(at, ours, other, w_up, w_down)
    mlp = halved(mine, flipped(theirs, "tp", 1)).astype(bf16)
    mlp = exchanged(mlp, ("z", "y")).astype(f32).sum(axis=0)
    second = residual_scale * normed_own.astype(f32) + mlp
    total, squares = packed_total(
        (jnp.sum(second, axis=1), jnp.sum(second * second, axis=1)), ("z", "y", "tp")
    )
    result = finish_norm(second, total, squares, D, gain_two, bias_two).astype(bf16)
    return (result, new_state)


def solution(mesh):
    fine = Mesh(mesh.devices.reshape(4, 4, 4, 2), ("dp", "z", "y", "tp"))
    kv = ("z", "y")
    every = ("z", "y", "tp")
    placed = (
        P("dp", kv),
        P(("dp", "z", "y"), "tp", None, None),
        P(kv, "tp"),
        P(kv, "tp"),
        P(kv, "tp"),
        P(kv, "tp"),
        P("tp"),
        P(),
        P("tp", kv),
        P(every),
        P(every),
        P(None, every),
        P(every, None),
        P(every),
        P(every),
    )
    return jax.shard_map(
        per_device,
        mesh=fine,
        in_specs=placed,
        out_specs=(P("dp", every), P(("dp", "z", "y"), "tp", None, None)),
        check_vma=False,
    )
```
